256 devices in a mesh: ep: 16 (over y, x), tp: 16 (over z, core).
Axes of the slice: x: 4, y: 4, z: 8, core: 2. Of those that a mesh axis runs over, the one named last changes fastest.
Arguments:
- stream: bfloat16 [131072, 1024], P(('ep', 'tp')), may hold values from -6 to 6
- norm_gain: float32 [1024], replicated, may hold values from 0.5 to 1.5
- gate_rows: bfloat16 [16, 1024, 1024], P('ep', 'tp'), may hold values from -0.1875 to 0.1875
- up_rows: bfloat16 [16, 1024, 1024], P('ep', 'tp'), may hold values from -0.1875 to 0.1875
- down_rows: bfloat16 [16, 1024, 1024], P('ep', 'tp'), may hold values from -0.1875 to 0.1875
- chosen: int32 [16, 16384], P('ep'), may hold values from 0 to 131071, as said below
- affinity: float32 [16, 16384], P('ep'), may hold values from 0.2 to 1
Outputs:
- mixed_out: bfloat16 [131072, 1024], P(('ep', 'tp'))
The draws below stay inside these ranges and needn't reach their ends.
Inputs may be any that keep to these rules, and one draw needn't show every extreme that they name: Each row of chosen names 16384 different token numbers in increasing order. Among the 512 consecutive token numbers of any one device, an expert reads at most 128, and for every expert some device holds exactly 128 of its tokens.
All inputs are finite; a program needn't handle non-finite values.
Results may differ from the reference program's by a relative error of at most 0.008.
Values may be sent and summed in bfloat16 or wider, within the bound.
No kernel may reach another device: no remote copies, remote signals or barrier semaphores. Data moves between devices by JAX's collectives and lax.ppermute only.
A program may use at most 64 MiB of HBM per device.

```python
import jax
import jax.numpy as jnp
from jax import lax

D = 1024
FF = 1024
TOK_DEV = 512
EXPERTS = 16
TOKENS = 131072
CAPACITY = 16384


def draw_chosen(key, part):
    blocks = TOKENS // TOK_DEV
    average = CAPACITY // blocks

    def one_expert(subkey):
        pair_key, offset_key, score_key = jax.random.split(subkey, 3)
        pairing = jax.random.permutation(pair_key, blocks)
        offsets = jax.random.randint(offset_key, (blocks // 2,), 0, average + 1)
        offsets = offsets.at[0].set(average)
        counts = jnp.zeros((blocks,), jnp.int32)
        counts = counts.at[pairing[0::2]].set(average + offsets)
        counts = counts.at[pairing[1::2]].set(average - offsets)
        scores = jax.random.randint(score_key, (blocks, TOK_DEV), 0, 1 << 20) * TOK_DEV
        scores = scores + jnp.arange(TOK_DEV, dtype=jnp.int32)[None, :]
        ranking = jnp.argsort(jnp.argsort(scores, axis=1), axis=1)
        member = (ranking < counts[:, None]).reshape(-1).astype(jnp.int32)
        return jnp.argsort(1 - member, stable=True)[:CAPACITY].astype(jnp.int32)
    expert_keys = jax.random.split(jax.random.fold_in(key, 11), EXPERTS)
    return jax.vmap(one_expert)(expert_keys)


def block_scale(stream_key, extent, shards, low, top_value):
    def one(axis_at, shards_of):
        steps = jax.random.uniform(jax.random.fold_in(jax.random.fold_in(stream_key, 6), axis_at), (shards_of,), jnp.float32, low / len(shards), top_value / len(shards))
        return jnp.repeat(jnp.exp(steps), extent[axis_at] // shards_of).reshape((-1,) + (1,) * (len(extent) - axis_at - 1))

    factor_of = one(*shards[0])
    for cut in shards[1:]:
        factor_of = factor_of * one(*cut)
    return factor_of


def bell_draw(rng, extent, spread, reach, cuts=(), kind=jnp.bfloat16):
    array = jax.random.normal(rng, extent, jnp.float32) * spread
    if len(cuts) > 0:
        array = block_scale(rng, extent, cuts, -0.22, 0.18) * array
    return jnp.clip(array, min=-reach, max=reach).astype(kind)


def setup_inputs(seed: int = 0) -> dict:
    key_list = jax.random.split(jax.random.key(seed), 8)
    return {
        "stream": bell_draw(key_list[0], (TOKENS, D), 1.0, 6.0, ((0, 256),)),
        "norm_gain": jnp.clip(1.0 + 0.1 * jax.random.normal(key_list[1], (D,), jnp.float32), 0.5, 1.5),
        "gate_rows": bell_draw(key_list[2], (EXPERTS, FF, D), D ** -0.5, 0.1875, ((0, 16), (1, 16))),
        "up_rows": bell_draw(key_list[3], (EXPERTS, FF, D), D ** -0.5, 0.1875, ((0, 16), (1, 16))),
        "down_rows": bell_draw(key_list[4], (EXPERTS, FF, D), FF ** -0.5, 0.1875, ((0, 16), (1, 16))),
        "chosen": draw_chosen(jax.random.fold_in(key_list[7], 71), 0),
        "affinity": jnp.clip(0.2 + 0.8 * jax.random.uniform(key_list[6], (EXPERTS, CAPACITY), jnp.float32) ** block_scale(key_list[6], (EXPERTS, CAPACITY), ((0, 16),), -0.2, 0.2), 0.2, 1.0),
    }


epsilon = 1e-06

def reference(stream, norm_gain, gate_rows, up_rows, down_rows, chosen, affinity):
    values = stream.astype(jnp.float32)
    inverse = lax.rsqrt(lax.optimization_barrier(jnp.mean(values * values, axis=-1, keepdims=True)) + epsilon)
    normed = (values * inverse * norm_gain).astype(jnp.bfloat16)

    def one_expert(running, pieces):
        gate_mat, up_mat, down_mat, picked, weights = pieces
        picked_rows = jnp.take(normed, picked, axis=0)
        gate_sum = jnp.dot(picked_rows, gate_mat.T, preferred_element_type=jnp.float32)
        up_sum = jnp.dot(picked_rows, up_mat.T, preferred_element_type=jnp.float32)
        hidden = (jax.nn.silu(gate_sum) * up_sum).astype(jnp.bfloat16)
        result = jnp.dot(hidden, down_mat, preferred_element_type=jnp.float32).astype(jnp.bfloat16)
        result = lax.optimization_barrier(result)
        weighted = result.astype(jnp.float32) * weights[:, None]
        return (running.at[picked].add(weighted), None)
    initial = jnp.zeros(stream.shape, jnp.float32)
    mixed_out, _ = lax.scan(one_expert, initial, (gate_rows, up_rows, down_rows, chosen, affinity))
    return mixed_out.astype(jnp.bfloat16)
```

```python
import functools

import jax
import jax.numpy as jnp
from jax import lax
from jax.experimental import pallas as pl
from jax.experimental.pallas import tpu as pltpu
from jax.sharding import PartitionSpec as P

epsilon = 1e-06
CHUNKS = 1


def windows_kernel(block, slots, bounds_ref, list_ref, affinity_ref, rows_ref, weights_ref):
    listed = list_ref[...]
    lines = listed.shape[0]
    lane = lax.broadcasted_iota(jnp.int32, (1, slots), 1)
    for j in range(rows_ref.shape[0]):
        bound = bounds_ref[j]
        start = jnp.sum((listed < bound).astype(jnp.int32))
        line, shift = start // slots, start % slots
        first = jnp.minimum(line, lines - 1)
        second = jnp.minimum(line + 1, lines - 1)
        back = lax.rem(slots - shift, slots)

        def window(ref):
            low = pltpu.roll(ref[pl.ds(first, 1), :], back, 1)
            high = pltpu.roll(ref[pl.ds(second, 1), :], back, 1)
            return jnp.where(lane < slots - shift, low, high)

        rows = window(list_ref) - bound
        rows_ref[pl.ds(j, 1), :] = jnp.where((rows >= 0) & (rows < block), rows, -1)
        weights_ref[pl.ds(j, 1), :] = window(affinity_ref)


def windows(bounds, listed, affinity, block, slots):
    count = bounds.shape[0]
    return pl.pallas_call(
        functools.partial(windows_kernel, block, slots),
        in_specs=[
            pl.BlockSpec(memory_space=pltpu.SMEM),
            pl.BlockSpec(memory_space=pltpu.VMEM),
            pl.BlockSpec(memory_space=pltpu.VMEM),
        ],
        out_shape=(
            jax.ShapeDtypeStruct((count, slots), jnp.int32),
            jax.ShapeDtypeStruct((count, slots), jnp.float32),
        ),
        cost_estimate=pl.CostEstimate(flops=8_000_000, bytes_accessed=150_000, transcendentals=0),
        name="windows",
    )(bounds, listed.reshape(-1, slots), affinity.reshape(-1, slots))


def norm_kernel(stream_ref, gain_ref, out_ref):
    values = stream_ref[...].astype(jnp.float32)
    inverse = lax.rsqrt(jnp.mean(values * values, axis=-1, keepdims=True) + epsilon)
    out_ref[...] = (values * inverse * gain_ref[...]).astype(jnp.bfloat16)


def normalize(stream, norm_gain):
    rows, features = stream.shape
    step = rows // 4
    return pl.pallas_call(
        norm_kernel,
        grid=(4,),
        in_specs=[
            pl.BlockSpec((step, features), lambda i: (i, 0)),
            pl.BlockSpec((1, features), lambda i: (0, 0)),
        ],
        out_specs=pl.BlockSpec((step, features), lambda i: (i, 0)),
        out_shape=jax.ShapeDtypeStruct((rows, features), jnp.bfloat16),
        cost_estimate=pl.CostEstimate(flops=3_000_000, bytes_accessed=2 << 20, transcendentals=512),
        name="normalize",
    )(stream, norm_gain.reshape(1, features))


def pick_kernel(rows_ref, normed_ref, out_ref):
    tokens = normed_ref.shape[0]
    token = lax.broadcasted_iota(jnp.int32, (tokens, rows_ref.shape[1]), 0)
    chosen = jnp.where(token == rows_ref[...], 1.0, 0.0).astype(jnp.bfloat16)
    out_ref[...] = lax.dot_general(
        chosen, normed_ref[...], (((0,), (0,)), ((), ())), preferred_element_type=jnp.float32
    ).astype(jnp.bfloat16)


def pick(rows, normed):
    total = rows.size
    tokens, features = normed.shape
    step = 512
    return pl.pallas_call(
        pick_kernel,
        grid=(total // step,),
        in_specs=[
            pl.BlockSpec((1, step), lambda i: (0, i)),
            pl.BlockSpec((tokens, features), lambda i: (0, 0)),
        ],
        out_specs=pl.BlockSpec((step, features), lambda i: (i, 0)),
        out_shape=jax.ShapeDtypeStruct((total, features), jnp.bfloat16),
        cost_estimate=pl.CostEstimate(
            flops=2 * total * tokens * features, bytes_accessed=2 * total * features, transcendentals=0
        ),
        name="pick",
    )(rows.reshape(1, total), normed)


def expert_kernel(inputs_ref, gate_ref, up_ref, down_ref, weights_ref, out_ref):
    inputs = inputs_ref[...]
    features = inputs.shape[1]
    gate = gate_ref[...].reshape(-1, features)
    up = up_ref[...].reshape(-1, features)
    down = down_ref[...].reshape(-1, features)
    last = (((1,), (1,)), ((), ()))
    gate_sum = lax.dot_general(inputs, gate, last, preferred_element_type=jnp.float32)
    up_sum = lax.dot_general(inputs, up, last, preferred_element_type=jnp.float32)
    hidden = (gate_sum / (1.0 + jnp.exp(-gate_sum)) * up_sum).astype(jnp.bfloat16)
    result = jnp.dot(hidden, down, preferred_element_type=jnp.float32)
    column = jnp.broadcast_to(weights_ref[...], (128, weights_ref.shape[1])).T[:, :1]
    out_ref[...] = (result * column).astype(jnp.bfloat16)


def expert(inputs, pieces, weights):
    total, features = inputs.shape
    count, _, piece_rows, _ = pieces.shape
    step = 256
    units = count * piece_rows

    def part(k):
        return pl.BlockSpec((count, 1, piece_rows, features), lambda i: (0, k, 0, 0))

    return pl.pallas_call(
        expert_kernel,
        grid=(total // step,),
        in_specs=[
            pl.BlockSpec((step, features), lambda i: (i, 0)),
            part(0),
            part(1),
            part(2),
            pl.BlockSpec((1, step), lambda i: (0, i)),
        ],
        out_specs=pl.BlockSpec((step, features), lambda i: (i, 0)),
        out_shape=jax.ShapeDtypeStruct((total, features), jnp.bfloat16),
        cost_estimate=pl.CostEstimate(
            flops=6 * total * units * features,
            bytes_accessed=6 * units * features + 4 * total * features,
            transcendentals=2 * total * units,
        ),
        compiler_params=pltpu.CompilerParams(vmem_limit_bytes=48 << 20),
        name="expert",
    )(inputs, pieces, pieces, pieces, weights.reshape(1, total))


def combine_kernel(rows_ref, returned_ref, out_ref, chosen_ref):
    @pl.when(pl.program_id(0) == 0)
    def _():
        token = lax.broadcasted_iota(jnp.int32, chosen_ref.shape, 0)
        chosen_ref[...] = jnp.where(token == rows_ref[...], 1.0, 0.0).astype(jnp.bfloat16)

    out_ref[...] = jnp.dot(
        chosen_ref[...], returned_ref[...], preferred_element_type=jnp.float32
    ).astype(jnp.bfloat16)


def combine(rows, returned, tokens):
    total, features = returned.shape
    step = 256
    return pl.pallas_call(
        combine_kernel,
        grid=(features // step,),
        in_specs=[
            pl.BlockSpec((1, total), lambda i: (0, 0)),
            pl.BlockSpec((total, step), lambda i: (0, i)),
        ],
        out_specs=pl.BlockSpec((tokens, step), lambda i: (0, i)),
        out_shape=jax.ShapeDtypeStruct((tokens, features), jnp.bfloat16),
        scratch_shapes=[pltpu.VMEM((tokens, total), jnp.bfloat16)],
        cost_estimate=pl.CostEstimate(
            flops=2 * total * tokens * features, bytes_accessed=2 * total * features, transcendentals=0
        ),
        name="combine",
    )(rows.reshape(1, total), returned)


def gather_pieces(own, tp_count):
    chips = tp_count // 2

    def along(by):
        return [(z * 2 + c, (z + by) % chips * 2 + c) for z in range(chips) for c in range(2)]

    held, right, left = [own], own, own
    for step in range(chips // 2):
        right = lax.ppermute(right, "tp", along(1))
        held.append(right)
        if step < chips // 2 - 1:
            left = lax.ppermute(left, "tp", along(-1))
            held.append(left)
    half = jnp.stack(held)
    other = lax.ppermute(half, "tp", [(j, j ^ 1) for j in range(tp_count)])
    return jnp.concatenate([half, other])


def per_device(stream, norm_gain, gate_rows, up_rows, down_rows, chosen, affinity):
    ep_count = lax.axis_size("ep")
    tp_count = lax.axis_size("tp")
    block, features = stream.shape
    slots = 4 * block // ep_count
    bounds = (jnp.arange(ep_count, dtype=jnp.int32) * tp_count + lax.axis_index("tp")) * block
    own_pieces = jnp.concatenate([gate_rows, up_rows, down_rows])
    pieces = gather_pieces(own_pieces, tp_count)
    rows_there, weights = windows(bounds, chosen, affinity, block, slots)
    rows_here = lax.all_to_all(rows_there, "ep", split_axis=0, concat_axis=0, tiled=True)
    normed = normalize(stream, norm_gain)
    size = slots // CHUNKS
    returned, rows_of = [], []
    for chunk in range(CHUNKS):
        cut = slice(chunk * size, (chunk + 1) * size)
        rows = rows_here[:, cut]
        outgoing = pick(rows, normed).reshape(ep_count, size, features)
        arrived = lax.all_to_all(outgoing, "ep", split_axis=0, concat_axis=0, tiled=True)
        produced = expert(arrived.reshape(-1, features), pieces, weights[:, cut])
        produced = produced.reshape(ep_count, size, features)
        back = lax.all_to_all(produced, "ep", split_axis=0, concat_axis=0, tiled=True)
        returned.append(back.reshape(-1, features))
        rows_of.append(rows.reshape(-1))
    return combine(jnp.concatenate(rows_of), jnp.concatenate(returned), block)


def solution(mesh):
    return jax.shard_map(
        per_device,
        mesh=mesh,
        in_specs=(
            P(("ep", "tp"), None),
            P(),
            P("ep", "tp", None),
            P("ep", "tp", None),
            P("ep", "tp", None),
            P("ep", None),
            P("ep", None),
        ),
        out_specs=P(("ep", "tp"), None),
        check_vma=False,
    )
```

```python
import functools

import jax
import jax.numpy as jnp
from jax import lax
from jax.experimental import pallas as pl
from jax.experimental.pallas import tpu as pltpu
from jax.sharding import PartitionSpec as P

epsilon = 1e-06


def windows_kernel(block, slots, bounds_ref, list_ref, affinity_ref, rows_ref, weights_ref):
    listed = list_ref[...]
    lines = listed.shape[0]
    lane = lax.broadcasted_iota(jnp.int32, (1, slots), 1)
    for j in range(rows_ref.shape[0]):
        bound = bounds_ref[j]
        start = jnp.sum((listed < bound).astype(jnp.int32))
        line, shift = start // slots, start % slots
        first = jnp.minimum(line, lines - 1)
        second = jnp.minimum(line + 1, lines - 1)
        back = lax.rem(slots - shift, slots)

        def window(ref):
            low = pltpu.roll(ref[pl.ds(first, 1), :], back, 1)
            high = pltpu.roll(ref[pl.ds(second, 1), :], back, 1)
            return jnp.where(lane < slots - shift, low, high)

        rows = window(list_ref) - bound
        rows_ref[pl.ds(j, 1), :] = jnp.where((rows >= 0) & (rows < block), rows, -1)
        weights_ref[pl.ds(j, 1), :] = window(affinity_ref)


def windows(bounds, listed, affinity, block, slots):
    count = bounds.shape[0]
    return pl.pallas_call(
        functools.partial(windows_kernel, block, slots),
        in_specs=[
            pl.BlockSpec(memory_space=pltpu.SMEM),
            pl.BlockSpec(memory_space=pltpu.VMEM),
            pl.BlockSpec(memory_space=pltpu.VMEM),
        ],
        out_shape=(
            jax.ShapeDtypeStruct((count, slots), jnp.int32),
            jax.ShapeDtypeStruct((count, slots), jnp.float32),
        ),
        cost_estimate=pl.CostEstimate(flops=8_000_000, bytes_accessed=150_000, transcendentals=0),
        name="windows",
    )(bounds, listed.reshape(-1, slots), affinity.reshape(-1, slots))


def prepare_kernel(stream_ref, gain_ref, gate_ref, up_ref, down_ref, normed_ref, piece_ref):
    values = stream_ref[...].astype(jnp.float32)
    inverse = lax.rsqrt(jnp.mean(values * values, axis=-1, keepdims=True) + epsilon)
    normed_ref[...] = (values * inverse * gain_ref[...]).astype(jnp.bfloat16)

    @pl.when(pl.program_id(0) == 0)
    def _():
        piece_ref[0:1] = gate_ref[...]
        piece_ref[1:2] = up_ref[...]
        piece_ref[2:3] = down_ref[...]


def prepare(stream, norm_gain, parts):
    rows, features = stream.shape
    step = rows // 2
    part = pl.BlockSpec(parts[0].shape, lambda i: (0, 0, 0))
    piece = (3, *parts[0].shape[1:])
    return pl.pallas_call(
        prepare_kernel,
        grid=(2,),
        in_specs=[
            pl.BlockSpec((step, features), lambda i: (i, 0)),
            pl.BlockSpec((1, features), lambda i: (0, 0)),
            part,
            part,
            part,
        ],
        out_specs=(
            pl.BlockSpec((step, features), lambda i: (i, 0)),
            pl.BlockSpec(piece, lambda i: (0, 0, 0)),
        ),
        out_shape=(
            jax.ShapeDtypeStruct((rows, features), jnp.bfloat16),
            jax.ShapeDtypeStruct(piece, jnp.bfloat16),
        ),
        cost_estimate=pl.CostEstimate(flops=3_000_000, bytes_accessed=3 << 20, transcendentals=512),
        name="prepare",
    )(stream, norm_gain.reshape(1, features), *parts)


def pick_kernel(rows_ref, normed_ref, out_ref):
    tokens = normed_ref.shape[0]
    columns = rows_ref[...].astype(jnp.float32).T
    token = lax.broadcasted_iota(jnp.int32, (columns.shape[0], tokens), 1).astype(jnp.float32)
    chosen = jnp.concatenate(
        [jnp.where(columns[:, e : e + 1] == token, 1.0, 0.0).astype(jnp.bfloat16) for e in range(columns.shape[1])]
    )
    out_ref[...] = jnp.dot(chosen, normed_ref[...], preferred_element_type=jnp.float32).astype(jnp.bfloat16)


def pick(rows, normed):
    count, slots = rows.shape
    tokens, features = normed.shape
    step = 8
    return pl.pallas_call(
        pick_kernel,
        grid=(count // step,),
        in_specs=[
            pl.BlockSpec((step, slots), lambda i: (i, 0)),
            pl.BlockSpec((tokens, features), lambda i: (0, 0)),
        ],
        out_specs=pl.BlockSpec((step * slots, features), lambda i: (i, 0)),
        out_shape=jax.ShapeDtypeStruct((count * slots, features), jnp.bfloat16),
        cost_estimate=pl.CostEstimate(
            flops=2 * count * slots * tokens * features, bytes_accessed=2 * count * slots * features, transcendentals=0
        ),
        name="pick",
    )(rows, normed)


def expert_kernel(inputs_ref, gate_ref, up_ref, down_ref, weights_ref, out_ref):
    inputs = inputs_ref[...]
    features = inputs.shape[1]
    gate = gate_ref[...].reshape(-1, features)
    up = up_ref[...].reshape(-1, features)
    down = down_ref[...].reshape(-1, features)
    last = (((1,), (1,)), ((), ()))
    gate_sum = lax.dot_general(inputs, gate, last, preferred_element_type=jnp.float32)
    up_sum = lax.dot_general(inputs, up, last, preferred_element_type=jnp.float32)
    hidden = (gate_sum / (1.0 + jnp.exp(-gate_sum)) * up_sum).astype(jnp.bfloat16)
    result = jnp.dot(hidden, down, preferred_element_type=jnp.float32)
    column = jnp.broadcast_to(weights_ref[...], (128, weights_ref.shape[1])).T[:, :1]
    out_ref[...] = (result * column).astype(jnp.bfloat16)


def expert(inputs, pieces, weights):
    total, features = inputs.shape
    count, _, piece_rows, _ = pieces.shape
    step = 256
    units = count * piece_rows

    def part(k):
        return pl.BlockSpec((count, 1, piece_rows, features), lambda i: (0, k, 0, 0))

    return pl.pallas_call(
        expert_kernel,
        grid=(total // step,),
        in_specs=[
            pl.BlockSpec((step, features), lambda i: (i, 0)),
            part(0),
            part(1),
            part(2),
            pl.BlockSpec((1, step), lambda i: (0, i)),
        ],
        out_specs=pl.BlockSpec((step, features), lambda i: (i, 0)),
        out_shape=jax.ShapeDtypeStruct((total, features), jnp.bfloat16),
        cost_estimate=pl.CostEstimate(
            flops=6 * total * units * features,
            bytes_accessed=6 * units * features + 4 * total * features,
            transcendentals=2 * total * units,
        ),
        compiler_params=pltpu.CompilerParams(vmem_limit_bytes=48 << 20),
        name="expert",
    )(inputs, pieces, pieces, pieces, weights.reshape(1, total))


def combine_kernel(rows_ref, returned_ref, out_ref, chosen_ref):
    @pl.when(pl.program_id(0) == 0)
    def _():
        count, slots = rows_ref.shape
        token = lax.broadcasted_iota(jnp.int32, (chosen_ref.shape[0], slots), 0)
        for e in range(count):
            chosen_ref[:, e * slots : (e + 1) * slots] = jnp.where(
                token == rows_ref[e : e + 1, :], 1.0, 0.0
            ).astype(jnp.bfloat16)

    out_ref[...] = jnp.dot(
        chosen_ref[...], returned_ref[...], preferred_element_type=jnp.float32
    ).astype(jnp.bfloat16)


def combine(rows, returned, tokens):
    total, features = returned.shape
    step = 256
    return pl.pallas_call(
        combine_kernel,
        grid=(features // step,),
        in_specs=[
            pl.BlockSpec(rows.shape, lambda i: (0, 0)),
            pl.BlockSpec((total, step), lambda i: (0, i)),
        ],
        out_specs=pl.BlockSpec((tokens, step), lambda i: (0, i)),
        out_shape=jax.ShapeDtypeStruct((tokens, features), jnp.bfloat16),
        scratch_shapes=[pltpu.VMEM((tokens, total), jnp.bfloat16)],
        cost_estimate=pl.CostEstimate(
            flops=2 * total * tokens * features, bytes_accessed=2 * total * features, transcendentals=0
        ),
        name="combine",
    )(rows, returned)


def gather_pieces(own, tp_count):
    chips = tp_count // 2

    def along(by):
        return [(z * 2 + c, (z + by) % chips * 2 + c) for z in range(chips) for c in range(2)]

    held, right, left = [own], own, own
    for step in range(chips // 2):
        right = lax.ppermute(right, "tp", along(1))
        held.append(right)
        if step < chips // 2 - 1:
            left = lax.ppermute(left, "tp", along(-1))
            held.append(left)
    half = jnp.stack(held)
    other = lax.ppermute(half, "tp", [(j, j ^ 1) for j in range(tp_count)])
    return jnp.concatenate([half, other])


def layer(stream, norm_gain, gate_rows, up_rows, down_rows, chosen, affinity):
    ep_count = lax.axis_size("ep")
    tp_count = lax.axis_size("tp")
    block, features = stream.shape
    slots = 4 * block // ep_count
    bounds = (jnp.arange(ep_count, dtype=jnp.int32) * tp_count + lax.axis_index("tp")) * block
    rows_there, weights = windows(bounds, chosen, affinity, block, slots)
    rows_here = lax.all_to_all(rows_there, "ep", split_axis=0, concat_axis=0, tiled=True)
    normed, own = prepare(stream, norm_gain, (gate_rows, up_rows, down_rows))
    pieces = gather_pieces(own, tp_count)
    outgoing = pick(rows_here, normed).reshape(ep_count, slots, features)
    arrived = lax.all_to_all(outgoing, "ep", split_axis=0, concat_axis=0, tiled=True)
    produced = expert(arrived.reshape(-1, features), pieces, weights)
    produced = produced.reshape(ep_count, slots, features)
    returned = lax.all_to_all(produced, "ep", split_axis=0, concat_axis=0, tiled=True)
    return combine(rows_here, returned.reshape(-1, features), block)


def solution(mesh):
    return jax.shard_map(
        layer,
        mesh=mesh,
        in_specs=(
            P(("ep", "tp"), None),
            P(),
            P("ep", "tp", None),
            P("ep", "tp", None),
            P("ep", "tp", None),
            P("ep", None),
            P("ep", None),
        ),
        out_specs=P(("ep", "tp"), None),
        check_vma=False,
    )
```

```python
import functools

import jax
import jax.numpy as jnp
from jax import lax
from jax.experimental import pallas as pl
from jax.experimental.pallas import tpu as pltpu
from jax.sharding import PartitionSpec as P

epsilon = 1e-06
SIDE = 4
SMEM = pl.BlockSpec(memory_space=pltpu.SMEM)
VMEM = pl.BlockSpec(memory_space=pltpu.VMEM)


def wrap(value):
    return lax.rem(value + SIDE, SIDE)


def windows_kernel(block, slots, bounds_ref, list_ref, affinity_ref, rows_ref, weights_ref):
    listed = list_ref[...]
    lines = listed.shape[0]
    lane = lax.broadcasted_iota(jnp.int32, (1, slots), 1)
    for j in range(weights_ref.shape[0]):
        y, x = divmod(j, SIDE)
        bound = bounds_ref[j]
        start = jnp.sum((listed < bound).astype(jnp.int32))
        line, shift = start // slots, start % slots
        first = jnp.minimum(line, lines - 1)
        second = jnp.minimum(line + 1, lines - 1)
        back = lax.rem(slots - shift, slots)

        def window(ref):
            low = pltpu.roll(ref[pl.ds(first, 1), :], back, 1)
            high = pltpu.roll(ref[pl.ds(second, 1), :], back, 1)
            return jnp.where(lane < slots - shift, low, high)

        rows = window(list_ref) - bound
        rows = jnp.where((rows >= 0) & (rows < block), rows, -1)
        for t in range(SIDE):
            rows_ref[y * SIDE + (x + t) % SIDE, t : t + 1, :] = rows
            rows_ref[(y + t) % SIDE * SIDE + x, SIDE + t : SIDE + t + 1, :] = rows
        weights_ref[j : j + 1, :] = window(affinity_ref)


def windows(bounds, listed, affinity, block, slots):
    count = bounds.shape[0]
    return pl.pallas_call(
        functools.partial(windows_kernel, block, slots),
        in_specs=[SMEM, VMEM, VMEM],
        out_shape=(
            jax.ShapeDtypeStruct((count, 2 * SIDE, slots), jnp.int32),
            jax.ShapeDtypeStruct((count, slots), jnp.float32),
        ),
        cost_estimate=pl.CostEstimate(flops=8_000_000, bytes_accessed=150_000, transcendentals=0),
        name="windows",
    )(bounds, listed.reshape(-1, slots), affinity.reshape(-1, slots))


def prepare_kernel(stream_ref, gain_ref, gate_ref, up_ref, down_ref, low_ref, high_ref, piece_ref):
    values = stream_ref[...].astype(jnp.float32)
    inverse = lax.rsqrt(jnp.mean(values * values, axis=-1, keepdims=True) + epsilon)
    normed = (values * inverse * gain_ref[...]).astype(jnp.bfloat16)
    half = low_ref.shape[1]
    low_ref[...] = normed[:, :half]
    high_ref[...] = normed[:, half:]

    @pl.when(pl.program_id(0) == 0)
    def _():
        piece_ref[0:1] = gate_ref[...]
        piece_ref[1:2] = up_ref[...]
        piece_ref[2:3] = down_ref[...]


def prepare(stream, norm_gain, parts):
    rows, features = stream.shape
    step, half = rows // 2, features // 2
    part = pl.BlockSpec(parts[0].shape, lambda i: (0, 0, 0))
    piece = (3, *parts[0].shape[1:])
    return pl.pallas_call(
        prepare_kernel,
        grid=(2,),
        in_specs=[
            pl.BlockSpec((step, features), lambda i: (i, 0)),
            pl.BlockSpec((1, features), lambda i: (0, 0)),
            part,
            part,
            part,
        ],
        out_specs=(
            pl.BlockSpec((step, half), lambda i: (i, 0)),
            pl.BlockSpec((step, half), lambda i: (i, 0)),
            pl.BlockSpec(piece, lambda i: (0, 0, 0)),
        ),
        out_shape=(
            jax.ShapeDtypeStruct((rows, half), jnp.bfloat16),
            jax.ShapeDtypeStruct((rows, half), jnp.bfloat16),
            jax.ShapeDtypeStruct(piece, jnp.bfloat16),
        ),
        cost_estimate=pl.CostEstimate(flops=3_000_000, bytes_accessed=3 << 20, transcendentals=512),
        name="prepare",
    )(stream, norm_gain.reshape(1, features), *parts)


def pick_kernel(along_y, place_ref, rows_ref, *refs):
    sources, outs = refs[:SIDE], refs[SIDE:]
    y, x = place_ref[0], place_ref[1]
    tokens, slots = sources[0].shape[0], rows_ref.shape[2]
    token = lax.broadcasted_iota(jnp.int32, (slots, tokens), 1).astype(jnp.float32)
    columns = []
    for d in range(SIDE):
        e = wrap(y + d) * SIDE + x if along_y else y * SIDE + wrap(x + d)
        columns.append(rows_ref[e].astype(jnp.float32).T)
    for t in range(SIDE):
        k = t if along_y else SIDE + t
        chosen = jnp.concatenate(
            [jnp.where(column[:, k : k + 1] == token, 1.0, 0.0).astype(jnp.bfloat16) for column in columns]
        )
        rows = jnp.dot(chosen, sources[t][...], preferred_element_type=jnp.float32).astype(jnp.bfloat16)
        for d in range(SIDE):
            outs[d][t * slots : (t + 1) * slots, :] = rows[d * slots : (d + 1) * slots, :]


def pick(along_y, place, rows, sources):
    tokens, half = sources[0].shape
    slots = rows.shape[2]
    return pl.pallas_call(
        functools.partial(pick_kernel, along_y),
        in_specs=[SMEM] + [VMEM] * (1 + SIDE),
        out_shape=[jax.ShapeDtypeStruct((SIDE * slots, half), jnp.bfloat16)] * SIDE,
        cost_estimate=pl.CostEstimate(
            flops=2 * SIDE * SIDE * slots * tokens * half, bytes_accessed=4 << 20, transcendentals=0
        ),
        name="pick_y" if along_y else "pick_x",
    )(place, rows, *sources)


def expert_kernel(pieces, place_ref, weights_ref, *refs):
    low, high = refs[:SIDE], refs[SIDE : 2 * SIDE]
    piece_refs = refs[2 * SIDE : 2 * SIDE + pieces]
    out_ref, inputs_ref, gate_ref, up_ref, down_ref = refs[2 * SIDE + pieces :]
    y, x = place_ref[0], place_ref[1]
    slots, half = out_ref.shape[1], low[0].shape[1]
    for k, piece in enumerate(piece_refs):
        width = piece.shape[1]
        gate_ref[k * width : (k + 1) * width, :] = piece[0]
        up_ref[k * width : (k + 1) * width, :] = piece[1]
        down_ref[k * width : (k + 1) * width, :] = piece[2]
    for a in range(SIDE):
        inputs_ref[a * SIDE * slots : (a + 1) * SIDE * slots, :half] = low[a][...]
        for b in range(SIDE):
            at = (a * SIDE + b) * slots
            inputs_ref[at : at + slots, half:] = high[b][a * slots : (a + 1) * slots, :]
    last = (((1,), (1,)), ((), ()))
    together = 2

    def step(i, carry):
        inputs = inputs_ref[pl.ds(pl.multiple_of(i * together * slots, together * slots), together * slots), :]
        gate_sum = lax.dot_general(inputs, gate_ref[...], last, preferred_element_type=jnp.float32)
        up_sum = lax.dot_general(inputs, up_ref[...], last, preferred_element_type=jnp.float32)
        hidden = (gate_sum / (1.0 + jnp.exp(-gate_sum)) * up_sum).astype(jnp.bfloat16)
        result = jnp.dot(hidden, down_ref[...], preferred_element_type=jnp.float32)
        for k in range(together):
            at = i * together + k
            back = wrap(y - at // SIDE) * SIDE + wrap(x - lax.rem(at, SIDE))
            line = weights_ref[pl.ds(back, 1), :]
            column = jnp.broadcast_to(line, (slots, slots)).T[:, :1]
            out_ref[back] = (result[k * slots : (k + 1) * slots] * column).astype(jnp.bfloat16)
        return carry

    lax.fori_loop(0, SIDE * SIDE // together, step, 0)


def expert(place, weights, low, high, pieces):
    slots, half = weights.shape[1], low[0].shape[1]
    features, units = 2 * half, len(pieces) * pieces[0].shape[1]
    total = SIDE * SIDE * slots
    return pl.pallas_call(
        functools.partial(expert_kernel, len(pieces)),
        in_specs=[SMEM] + [VMEM] * (1 + len(low) + len(high) + len(pieces)),
        out_shape=jax.ShapeDtypeStruct((SIDE * SIDE, slots, features), jnp.bfloat16),
        scratch_shapes=[
            pltpu.VMEM((total, features), jnp.bfloat16),
            pltpu.VMEM((units, features), jnp.bfloat16),
            pltpu.VMEM((units, features), jnp.bfloat16),
            pltpu.VMEM((units, features), jnp.bfloat16),
        ],
        cost_estimate=pl.CostEstimate(
            flops=6 * total * units * features,
            bytes_accessed=6 * units * features + 4 * total * features,
            transcendentals=2 * total * units,
        ),
        compiler_params=pltpu.CompilerParams(vmem_limit_bytes=48 << 20),
        name="expert",
    )(place, weights, *low, *high, *pieces)


def combine_kernel(rows_ref, returned_ref, out_ref, chosen_ref):
    @pl.when(pl.program_id(0) == 0)
    def _():
        count, _, slots = rows_ref.shape
        token = lax.broadcasted_iota(jnp.int32, (chosen_ref.shape[0], slots), 0)
        for e in range(count):
            chosen_ref[:, e * slots : (e + 1) * slots] = jnp.where(token == rows_ref[e, 0:1, :], 1.0, 0.0).astype(
                jnp.bfloat16
            )

    out_ref[...] = jnp.dot(chosen_ref[...], returned_ref[...], preferred_element_type=jnp.float32).astype(jnp.bfloat16)


def combine(rows, returned, tokens):
    total, features = returned.shape
    step = 256
    return pl.pallas_call(
        combine_kernel,
        grid=(features // step,),
        in_specs=[
            pl.BlockSpec(rows.shape, lambda i: (0, 0, 0)),
            pl.BlockSpec((total, step), lambda i: (0, i)),
        ],
        out_specs=pl.BlockSpec((tokens, step), lambda i: (0, i)),
        out_shape=jax.ShapeDtypeStruct((tokens, features), jnp.bfloat16),
        scratch_shapes=[pltpu.VMEM((tokens, total), jnp.bfloat16)],
        cost_estimate=pl.CostEstimate(
            flops=2 * total * tokens * features, bytes_accessed=2 * total * features, transcendentals=0
        ),
        name="combine",
    )(rows, returned)


def over_plane(array, by_y, by_x):
    places = [(y, x) for y in range(SIDE) for x in range(SIDE)]
    return lax.ppermute(
        array, "ep", [(y * SIDE + x, (y + by_y) % SIDE * SIDE + (x + by_x) % SIDE) for y, x in places]
    )


def along_z(array, by, tp_count):
    chips = tp_count // 2
    return lax.ppermute(array, "tp", [(z * 2 + c, (z + by) % chips * 2 + c) for z in range(chips) for c in range(2)])


def other_core(array, tp_count):
    return lax.ppermute(array, "tp", [(j, j ^ 1) for j in range(tp_count)])


def layer(stream, norm_gain, gate_rows, up_rows, down_rows, chosen, affinity):
    ep_count = lax.axis_size("ep")
    tp_count = lax.axis_size("tp")
    block, features = stream.shape
    slots = 4 * block // ep_count
    ep_index = lax.axis_index("ep").astype(jnp.int32)
    place = jnp.stack([ep_index // SIDE, ep_index % SIDE])
    bounds = (jnp.arange(ep_count, dtype=jnp.int32) * tp_count + lax.axis_index("tp")) * block
    low, high, own = prepare(stream, norm_gain, (gate_rows, up_rows, down_rows))
    near = {by: along_z(own, by, tp_count) for by in (1, -1, 2, -2)}
    lows = [low] + [over_plane(low, 0, t) for t in range(1, SIDE)]
    highs = [high] + [over_plane(high, t, 0) for t in range(1, SIDE)]
    rows_there, weights = windows(bounds, chosen, affinity, block, slots)
    rows_here = lax.all_to_all(rows_there, "ep", split_axis=0, concat_axis=0, tiled=True)
    far = [along_z(near[2], 1, tp_count), along_z(near[-2], -1, tp_count), along_z(near[2], 2, tp_count)]
    held = [own, *near.values(), *far]
    pieces = held + [other_core(piece, tp_count) for piece in held]
    picked_low = pick(True, place, rows_here, lows)
    picked_high = pick(False, place, rows_here, highs)
    arrived_low = [picked_low[0]] + [over_plane(picked_low[d], d, 0) for d in range(1, SIDE)]
    arrived_high = [picked_high[0]] + [over_plane(picked_high[d], 0, d) for d in range(1, SIDE)]
    produced = expert(place, weights, arrived_low, arrived_high, pieces)
    returned = lax.all_to_all(produced, "ep", split_axis=0, concat_axis=0, tiled=True)
    return combine(rows_here, returned.reshape(-1, features), block)


def solution(mesh):
    return jax.shard_map(
        layer,
        mesh=mesh,
        in_specs=(
            P(("ep", "tp"), None),
            P(),
            P("ep", "tp", None),
            P("ep", "tp", None),
            P("ep", "tp", None),
            P("ep", None),
            P("ep", None),
        ),
        out_specs=P(("ep", "tp"), None),
        check_vma=False,
    )
```

```python
import functools

import jax
import jax.numpy as jnp
from jax import lax
from jax.experimental import pallas as pl
from jax.experimental.pallas import tpu as pltpu
from jax.sharding import PartitionSpec as P

epsilon = 1e-06
SIDE = 4
SMEM = pl.BlockSpec(memory_space=pltpu.SMEM)
VMEM = pl.BlockSpec(memory_space=pltpu.VMEM)


def wrap(value):
    return lax.rem(value + SIDE, SIDE)


def windows_kernel(block, slots, bounds_ref, list_ref, affinity_ref, rows_ref, weights_ref):
    listed = list_ref[...]
    lines = listed.shape[0]
    lane = lax.broadcasted_iota(jnp.int32, (1, slots), 1)
    for j in range(weights_ref.shape[0]):
        y, x = divmod(j, SIDE)
        bound = bounds_ref[j]
        start = jnp.sum((listed < bound).astype(jnp.int32))
        line, shift = start // slots, start % slots
        first = jnp.minimum(line, lines - 1)
        second = jnp.minimum(line + 1, lines - 1)
        back = lax.rem(slots - shift, slots)

        def window(ref):
            low = pltpu.roll(ref[pl.ds(first, 1), :], back, 1)
            high = pltpu.roll(ref[pl.ds(second, 1), :], back, 1)
            return jnp.where(lane < slots - shift, low, high)

        rows = window(list_ref) - bound
        rows = jnp.where((rows >= 0) & (rows < block), rows, -1)
        for t in range(SIDE):
            rows_ref[y * SIDE + (x + t) % SIDE, t : t + 1, :] = rows
            rows_ref[(y + t) % SIDE * SIDE + x, SIDE + t : SIDE + t + 1, :] = rows
        weights_ref[j : j + 1, :] = window(affinity_ref)


def windows(bounds, listed, affinity, block, slots):
    count = bounds.shape[0]
    return pl.pallas_call(
        functools.partial(windows_kernel, block, slots),
        in_specs=[SMEM, VMEM, VMEM],
        out_shape=(
            jax.ShapeDtypeStruct((count, 2 * SIDE, slots), jnp.int32),
            jax.ShapeDtypeStruct((count, slots), jnp.float32),
        ),
        cost_estimate=pl.CostEstimate(flops=8_000_000, bytes_accessed=150_000, transcendentals=0),
        name="windows",
    )(bounds, listed.reshape(-1, slots), affinity.reshape(-1, slots))


def prepare_kernel(stream_ref, gain_ref, gate_ref, up_ref, down_ref, low_ref, high_ref, piece_ref):
    values = stream_ref[...].astype(jnp.float32)
    inverse = lax.rsqrt(jnp.mean(values * values, axis=-1, keepdims=True) + epsilon)
    normed = (values * inverse * gain_ref[...]).astype(jnp.bfloat16)
    half = low_ref.shape[1]
    low_ref[...] = normed[:, :half]
    high_ref[...] = normed[:, half:]

    @pl.when(pl.program_id(0) == 0)
    def _():
        piece_ref[0:1] = gate_ref[...]
        piece_ref[1:2] = up_ref[...]
        piece_ref[2:3] = down_ref[...]


def prepare(stream, norm_gain, parts):
    rows, features = stream.shape
    step, half = rows // 2, features // 2
    part = pl.BlockSpec(parts[0].shape, lambda i: (0, 0, 0))
    piece = (3, *parts[0].shape[1:])
    return pl.pallas_call(
        prepare_kernel,
        grid=(2,),
        in_specs=[
            pl.BlockSpec((step, features), lambda i: (i, 0)),
            pl.BlockSpec((1, features), lambda i: (0, 0)),
            part,
            part,
            part,
        ],
        out_specs=(
            pl.BlockSpec((step, half), lambda i: (i, 0)),
            pl.BlockSpec((step, half), lambda i: (i, 0)),
            pl.BlockSpec(piece, lambda i: (0, 0, 0)),
        ),
        out_shape=(
            jax.ShapeDtypeStruct((rows, half), jnp.bfloat16),
            jax.ShapeDtypeStruct((rows, half), jnp.bfloat16),
            jax.ShapeDtypeStruct(piece, jnp.bfloat16),
        ),
        cost_estimate=pl.CostEstimate(flops=3_000_000, bytes_accessed=3 << 20, transcendentals=512),
        name="prepare",
    )(stream, norm_gain.reshape(1, features), *parts)


def pick_kernel(along_y, place_ref, rows_ref, *refs):
    sources, outs = refs[:SIDE], refs[SIDE:]
    y, x = place_ref[0], place_ref[1]
    tokens, slots = sources[0].shape[0], rows_ref.shape[2]
    token = lax.broadcasted_iota(jnp.int32, (slots, tokens), 1).astype(jnp.float32)
    columns = []
    for d in range(SIDE):
        e = wrap(y + d) * SIDE + x if along_y else y * SIDE + wrap(x + d)
        columns.append(rows_ref[e].astype(jnp.float32).T)
    for t in range(SIDE):
        k = t if along_y else SIDE + t
        chosen = jnp.concatenate(
            [jnp.where(column[:, k : k + 1] == token, 1.0, 0.0).astype(jnp.bfloat16) for column in columns]
        )
        rows = jnp.dot(chosen, sources[t][...], preferred_element_type=jnp.float32).astype(jnp.bfloat16)
        for d in range(SIDE):
            outs[d][t * slots : (t + 1) * slots, :] = rows[d * slots : (d + 1) * slots, :]


def pick(along_y, place, rows, sources):
    tokens, half = sources[0].shape
    slots = rows.shape[2]
    return pl.pallas_call(
        functools.partial(pick_kernel, along_y),
        in_specs=[SMEM] + [VMEM] * (1 + SIDE),
        out_shape=[jax.ShapeDtypeStruct((SIDE * slots, half), jnp.bfloat16)] * SIDE,
        cost_estimate=pl.CostEstimate(
            flops=2 * SIDE * SIDE * slots * tokens * half, bytes_accessed=4 << 20, transcendentals=0
        ),
        compiler_params=pltpu.CompilerParams(vmem_limit_bytes=12 << 20),
        name="pick_y" if along_y else "pick_x",
    )(place, rows, *sources)


def assemble_kernel(*refs):
    pieces, outs = refs[:-3], refs[-3:]
    width = pieces[0].shape[1]
    for k, piece in enumerate(pieces):
        for j, out in enumerate(outs):
            out[k * width : (k + 1) * width, :] = piece[j]


def assemble(pieces):
    shape = jax.ShapeDtypeStruct((len(pieces) * pieces[0].shape[1], pieces[0].shape[2]), jnp.bfloat16)
    return pl.pallas_call(
        assemble_kernel,
        in_specs=[VMEM] * len(pieces),
        out_shape=[shape] * 3,
        cost_estimate=pl.CostEstimate(flops=1_000_000, bytes_accessed=12 << 20, transcendentals=0),
        compiler_params=pltpu.CompilerParams(vmem_limit_bytes=16 << 20),
        name="assemble",
    )(*pieces)


def expert_kernel(place_ref, weights_ref, gate_ref, up_ref, down_ref, *refs):
    low, high = refs[:SIDE], refs[SIDE : 2 * SIDE]
    out_ref, inputs_ref = refs[2 * SIDE :]
    y, x = place_ref[0], place_ref[1]
    slots, half = out_ref.shape[1], low[0].shape[1]
    a = pl.program_id(0)
    for k in range(SIDE):

        @pl.when(a == k)
        def _():
            inputs_ref[:, :half] = low[k][...]

        inputs_ref[k * slots : (k + 1) * slots, half:] = high[k][pl.ds(pl.multiple_of(a * slots, slots), slots), :]
    last = (((1,), (1,)), ((), ()))
    inputs = inputs_ref[...]
    units = gate_ref.shape[0]
    width = units // 4
    hidden = []
    for f in range(0, units, width):
        gate_sum = lax.dot_general(inputs, gate_ref[f : f + width, :], last, preferred_element_type=jnp.float32)
        up_sum = lax.dot_general(inputs, up_ref[f : f + width, :], last, preferred_element_type=jnp.float32)
        hidden.append((gate_sum / (1.0 + jnp.exp(-gate_sum)) * up_sum).astype(jnp.bfloat16))
    result = jnp.dot(jnp.concatenate(hidden, 1), down_ref[...], preferred_element_type=jnp.float32)
    for b in range(SIDE):
        back = wrap(x - b)
        line = weights_ref[pl.ds(wrap(y - a) * SIDE + back, 1), :]
        column = jnp.broadcast_to(line, (slots, slots)).T[:, :1]
        out_ref[back] = (result[b * slots : (b + 1) * slots] * column).astype(jnp.bfloat16)


def expert(place, weights, low, high, gate, up, down):
    slots, half = weights.shape[1], low[0].shape[1]
    features, units = 2 * half, gate.shape[0]
    total = SIDE * SIDE * slots
    whole = pl.BlockSpec(memory_space=pltpu.VMEM)
    return pl.pallas_call(
        expert_kernel,
        grid_spec=pltpu.PrefetchScalarGridSpec(
            num_scalar_prefetch=1,
            grid=(SIDE,),
            in_specs=[whole] * (4 + len(low) + len(high)),
            out_specs=pl.BlockSpec((SIDE, slots, features), lambda a, place_ref: (wrap(place_ref[0] - a), 0, 0)),
            scratch_shapes=[pltpu.VMEM((SIDE * slots, features), jnp.bfloat16)],
        ),
        out_shape=jax.ShapeDtypeStruct((SIDE * SIDE, slots, features), jnp.bfloat16),
        cost_estimate=pl.CostEstimate(
            flops=6 * total * units * features,
            bytes_accessed=6 * units * features + 4 * total * features,
            transcendentals=2 * total * units,
        ),
        compiler_params=pltpu.CompilerParams(vmem_limit_bytes=36 << 20),
        name="expert",
    )(place, weights, gate, up, down, *low, *high)


def combine_kernel(rows_ref, returned_ref, out_ref, chosen_ref):
    @pl.when(pl.program_id(0) == 0)
    def _():
        count, _, slots = rows_ref.shape
        token = lax.broadcasted_iota(jnp.int32, (chosen_ref.shape[0], slots), 0)
        for e in range(count):
            chosen_ref[:, e * slots : (e + 1) * slots] = jnp.where(token == rows_ref[e, 0:1, :], 1.0, 0.0).astype(
                jnp.bfloat16
            )

    out_ref[...] = jnp.dot(chosen_ref[...], returned_ref[...], preferred_element_type=jnp.float32).astype(jnp.bfloat16)


def combine(rows, returned, tokens):
    total, features = returned.shape
    step = 256
    return pl.pallas_call(
        combine_kernel,
        grid=(features // step,),
        in_specs=[
            pl.BlockSpec(rows.shape, lambda i: (0, 0, 0)),
            pl.BlockSpec((total, step), lambda i: (0, i)),
        ],
        out_specs=pl.BlockSpec((tokens, step), lambda i: (0, i)),
        out_shape=jax.ShapeDtypeStruct((tokens, features), jnp.bfloat16),
        scratch_shapes=[pltpu.VMEM((tokens, total), jnp.bfloat16)],
        cost_estimate=pl.CostEstimate(
            flops=2 * total * tokens * features, bytes_accessed=2 * total * features, transcendentals=0
        ),
        compiler_params=pltpu.CompilerParams(vmem_limit_bytes=16 << 20),
        name="combine",
    )(rows, returned)


def over_plane(array, by_y, by_x):
    places = [(y, x) for y in range(SIDE) for x in range(SIDE)]
    return lax.ppermute(
        array, "ep", [(y * SIDE + x, (y + by_y) % SIDE * SIDE + (x + by_x) % SIDE) for y, x in places]
    )


def along_z(array, by, tp_count):
    chips = tp_count // 2
    return lax.ppermute(array, "tp", [(z * 2 + c, (z + by) % chips * 2 + c) for z in range(chips) for c in range(2)])


def other_core(array, tp_count):
    return lax.ppermute(array, "tp", [(j, j ^ 1) for j in range(tp_count)])


def layer(stream, norm_gain, gate_rows, up_rows, down_rows, chosen, affinity):
    ep_count = lax.axis_size("ep")
    tp_count = lax.axis_size("tp")
    block, features = stream.shape
    slots = 4 * block // ep_count
    ep_index = lax.axis_index("ep").astype(jnp.int32)
    place = jnp.stack([ep_index // SIDE, ep_index % SIDE])
    bounds = (jnp.arange(ep_count, dtype=jnp.int32) * tp_count + lax.axis_index("tp")) * block
    low, high, own = prepare(stream, norm_gain, (gate_rows, up_rows, down_rows))
    lows = [low] + [over_plane(low, 0, t) for t in range(1, SIDE)]
    highs = [high] + [over_plane(high, t, 0) for t in range(1, SIDE)]
    rows_there, weights = windows(bounds, chosen, affinity, block, slots)
    rows_here = lax.all_to_all(rows_there, "ep", split_axis=0, concat_axis=0, tiled=True)
    near = {by: along_z(own, by, tp_count) for by in (1, -1, 2, -2)}
    picked_low = pick(True, place, rows_here, lows)
    arrived_low = [picked_low[0]] + [over_plane(picked_low[d], d, 0) for d in range(1, SIDE)]
    picked_high = pick(False, place, rows_here, highs)
    arrived_high = [picked_high[0]] + [over_plane(picked_high[d], 0, d) for d in range(1, SIDE)]
    far = [along_z(near[2], 1, tp_count), along_z(near[-2], -1, tp_count), along_z(near[2], 2, tp_count)]
    held = [own, *near.values(), *far]
    pieces = held + [other_core(piece, tp_count) for piece in held]
    produced = expert(place, weights, arrived_low, arrived_high, *assemble(pieces))
    returned = lax.all_to_all(produced, "ep", split_axis=0, concat_axis=0, tiled=True)
    return combine(rows_here, returned.reshape(-1, features), block)


def solution(mesh):
    return jax.shard_map(
        layer,
        mesh=mesh,
        in_specs=(
            P(("ep", "tp"), None),
            P(),
            P("ep", "tp", None),
            P("ep", "tp", None),
            P("ep", "tp", None),
            P("ep", None),
            P("ep", None),
        ),
        out_specs=P(("ep", "tp"), None),
        check_vma=False,
    )
```

```python
import functools

import jax
import jax.numpy as jnp
from jax import lax
from jax.experimental import pallas as pl
from jax.experimental.pallas import tpu as pltpu
from jax.sharding import PartitionSpec as P

epsilon = 1e-06
SIDE = 4
SMEM = pl.BlockSpec(memory_space=pltpu.SMEM)
VMEM = pl.BlockSpec(memory_space=pltpu.VMEM)


def wrap(value):
    return lax.rem(value + SIDE, SIDE)


def windows_kernel(block, slots, bounds_ref, list_ref, affinity_ref, rows_ref, weights_ref):
    listed = list_ref[...]
    lines = listed.shape[0]
    lane = lax.broadcasted_iota(jnp.int32, (1, slots), 1)
    for j in range(weights_ref.shape[0]):
        y, x = divmod(j, SIDE)
        bound = bounds_ref[j]
        start = jnp.sum((listed < bound).astype(jnp.int32))
        line, shift = start // slots, start % slots
        first = jnp.minimum(line, lines - 1)
        second = jnp.minimum(line + 1, lines - 1)
        back = lax.rem(slots - shift, slots)

        def window(ref):
            low = pltpu.roll(ref[pl.ds(first, 1), :], back, 1)
            high = pltpu.roll(ref[pl.ds(second, 1), :], back, 1)
            return jnp.where(lane < slots - shift, low, high)

        rows = window(list_ref) - bound
        rows = jnp.where((rows >= 0) & (rows < block), rows, -1)
        for t in range(SIDE):
            rows_ref[y * SIDE + (x + t) % SIDE, t : t + 1, :] = rows
            rows_ref[(y + t) % SIDE * SIDE + x, SIDE + t : SIDE + t + 1, :] = rows
        weights_ref[j : j + 1, :] = window(affinity_ref)


def windows(bounds, listed, affinity, block, slots):
    count = bounds.shape[0]
    return pl.pallas_call(
        functools.partial(windows_kernel, block, slots),
        in_specs=[SMEM, VMEM, VMEM],
        out_shape=(
            jax.ShapeDtypeStruct((count, 2 * SIDE, slots), jnp.int32),
            jax.ShapeDtypeStruct((count, slots), jnp.float32),
        ),
        cost_estimate=pl.CostEstimate(flops=8_000_000, bytes_accessed=150_000, transcendentals=0),
        name="windows",
    )(bounds, listed.reshape(-1, slots), affinity.reshape(-1, slots))


def prepare_kernel(stream_ref, gain_ref, gate_ref, up_ref, down_ref, low_ref, high_ref, piece_ref):
    values = stream_ref[...].astype(jnp.float32)
    inverse = lax.rsqrt(jnp.mean(values * values, axis=-1, keepdims=True) + epsilon)
    normed = (values * inverse * gain_ref[...]).astype(jnp.bfloat16)
    half = low_ref.shape[1]
    low_ref[...] = normed[:, :half]
    high_ref[...] = normed[:, half:]

    @pl.when(pl.program_id(0) == 0)
    def _():
        piece_ref[0:1] = gate_ref[...]
        piece_ref[1:2] = up_ref[...]
        piece_ref[2:3] = down_ref[...]


def prepare(stream, norm_gain, parts):
    rows, features = stream.shape
    step, half = rows // 2, features // 2
    part = pl.BlockSpec(parts[0].shape, lambda i: (0, 0, 0))
    piece = (3, *parts[0].shape[1:])
    return pl.pallas_call(
        prepare_kernel,
        grid=(2,),
        in_specs=[
            pl.BlockSpec((step, features), lambda i: (i, 0)),
            pl.BlockSpec((1, features), lambda i: (0, 0)),
            part,
            part,
            part,
        ],
        out_specs=(
            pl.BlockSpec((step, half), lambda i: (i, 0)),
            pl.BlockSpec((step, half), lambda i: (i, 0)),
            pl.BlockSpec(piece, lambda i: (0, 0, 0)),
        ),
        out_shape=(
            jax.ShapeDtypeStruct((rows, half), jnp.bfloat16),
            jax.ShapeDtypeStruct((rows, half), jnp.bfloat16),
            jax.ShapeDtypeStruct(piece, jnp.bfloat16),
        ),
        cost_estimate=pl.CostEstimate(flops=3_000_000, bytes_accessed=3 << 20, transcendentals=512),
        name="prepare",
    )(stream, norm_gain.reshape(1, features), *parts)


def pick_kernel(along_y, place_ref, rows_ref, *refs):
    sources, outs = refs[:SIDE], refs[SIDE:]
    y, x = place_ref[0], place_ref[1]
    tokens, slots = sources[0].shape[0], rows_ref.shape[2]
    token = lax.broadcasted_iota(jnp.int32, (slots, tokens), 1).astype(jnp.float32)
    columns = []
    for d in range(SIDE):
        e = wrap(y + d) * SIDE + x if along_y else y * SIDE + wrap(x + d)
        columns.append(rows_ref[e].astype(jnp.float32).T)
    for t in range(SIDE):
        k = t if along_y else SIDE + t
        chosen = jnp.concatenate(
            [jnp.where(column[:, k : k + 1] == token, 1.0, 0.0).astype(jnp.bfloat16) for column in columns]
        )
        rows = jnp.dot(chosen, sources[t][...], preferred_element_type=jnp.float32).astype(jnp.bfloat16)
        for d in range(SIDE):
            outs[d][t * slots : (t + 1) * slots, :] = rows[d * slots : (d + 1) * slots, :]


def pick(along_y, place, rows, sources):
    tokens, half = sources[0].shape
    slots = rows.shape[2]
    return pl.pallas_call(
        functools.partial(pick_kernel, along_y),
        in_specs=[SMEM] + [VMEM] * (1 + SIDE),
        out_shape=[jax.ShapeDtypeStruct((SIDE * slots, half), jnp.bfloat16)] * SIDE,
        cost_estimate=pl.CostEstimate(
            flops=2 * SIDE * SIDE * slots * tokens * half, bytes_accessed=4 << 20, transcendentals=0
        ),
        compiler_params=pltpu.CompilerParams(vmem_limit_bytes=12 << 20),
        name="pick_y" if along_y else "pick_x",
    )(place, rows, *sources)


def assemble_kernel(*refs):
    pieces, outs = refs[:-3], refs[-3:]
    at = 0
    for piece in pieces:
        width = piece.shape[1]
        for j, out in enumerate(outs):
            out[at : at + width, :] = piece[j]
        at += width


def assemble(pieces):
    shape = jax.ShapeDtypeStruct((sum(piece.shape[1] for piece in pieces), pieces[0].shape[2]), jnp.bfloat16)
    return pl.pallas_call(
        assemble_kernel,
        in_specs=[VMEM] * len(pieces),
        out_shape=[shape] * 3,
        cost_estimate=pl.CostEstimate(flops=1_000_000, bytes_accessed=12 << 20, transcendentals=0),
        compiler_params=pltpu.CompilerParams(vmem_limit_bytes=16 << 20),
        name="assemble",
    )(*pieces)


def expert_kernel(place_ref, weights_ref, gate_ref, up_ref, down_ref, *refs):
    low, high = refs[:SIDE], refs[SIDE : 2 * SIDE]
    out_ref, inputs_ref = refs[2 * SIDE :]
    y, x = place_ref[0], place_ref[1]
    slots, half = out_ref.shape[1], low[0].shape[1]
    a = pl.program_id(0)
    for k in range(SIDE):

        @pl.when(a == k)
        def _():
            inputs_ref[:, :half] = low[k][...]

        inputs_ref[k * slots : (k + 1) * slots, half:] = high[k][pl.ds(pl.multiple_of(a * slots, slots), slots), :]
    last = (((1,), (1,)), ((), ()))
    inputs = inputs_ref[...]
    units = gate_ref.shape[0]
    width = units // 4
    hidden = []
    for f in range(0, units, width):
        gate_sum = lax.dot_general(inputs, gate_ref[f : f + width, :], last, preferred_element_type=jnp.float32)
        up_sum = lax.dot_general(inputs, up_ref[f : f + width, :], last, preferred_element_type=jnp.float32)
        hidden.append((gate_sum / (1.0 + jnp.exp(-gate_sum)) * up_sum).astype(jnp.bfloat16))
    result = jnp.dot(jnp.concatenate(hidden, 1), down_ref[...], preferred_element_type=jnp.float32)
    for b in range(SIDE):
        back = wrap(x - b)
        line = weights_ref[pl.ds(wrap(y - a) * SIDE + back, 1), :]
        column = jnp.broadcast_to(line, (slots, slots)).T[:, :1]
        out_ref[back] = (result[b * slots : (b + 1) * slots] * column).astype(jnp.bfloat16)


def expert(place, weights, low, high, gate, up, down):
    slots, half = weights.shape[1], low[0].shape[1]
    features, units = 2 * half, gate.shape[0]
    total = SIDE * SIDE * slots
    whole = pl.BlockSpec(memory_space=pltpu.VMEM)
    return pl.pallas_call(
        expert_kernel,
        grid_spec=pltpu.PrefetchScalarGridSpec(
            num_scalar_prefetch=1,
            grid=(SIDE,),
            in_specs=[whole] * (4 + len(low) + len(high)),
            out_specs=pl.BlockSpec((SIDE, slots, features), lambda a, place_ref: (wrap(place_ref[0] - a), 0, 0)),
            scratch_shapes=[pltpu.VMEM((SIDE * slots, features), jnp.bfloat16)],
        ),
        out_shape=jax.ShapeDtypeStruct((SIDE * SIDE, slots, features), jnp.bfloat16),
        cost_estimate=pl.CostEstimate(
            flops=6 * total * units * features,
            bytes_accessed=6 * units * features + 4 * total * features,
            transcendentals=2 * total * units,
        ),
        compiler_params=pltpu.CompilerParams(vmem_limit_bytes=36 << 20),
        name="expert",
    )(place, weights, gate, up, down, *low, *high)


def combine_kernel(rows_ref, returned_ref, out_ref, chosen_ref):
    @pl.when(pl.program_id(0) == 0)
    def _():
        count, _, slots = rows_ref.shape
        token = lax.broadcasted_iota(jnp.int32, (chosen_ref.shape[0], slots), 0)
        for e in range(count):
            chosen_ref[:, e * slots : (e + 1) * slots] = jnp.where(token == rows_ref[e, 0:1, :], 1.0, 0.0).astype(
                jnp.bfloat16
            )

    out_ref[...] = jnp.dot(chosen_ref[...], returned_ref[...], preferred_element_type=jnp.float32).astype(jnp.bfloat16)


def combine(rows, returned, tokens):
    total, features = returned.shape
    step = 256
    return pl.pallas_call(
        combine_kernel,
        grid=(features // step,),
        in_specs=[
            pl.BlockSpec(rows.shape, lambda i: (0, 0, 0)),
            pl.BlockSpec((total, step), lambda i: (0, i)),
        ],
        out_specs=pl.BlockSpec((tokens, step), lambda i: (0, i)),
        out_shape=jax.ShapeDtypeStruct((tokens, features), jnp.bfloat16),
        scratch_shapes=[pltpu.VMEM((tokens, total), jnp.bfloat16)],
        cost_estimate=pl.CostEstimate(
            flops=2 * total * tokens * features, bytes_accessed=2 * total * features, transcendentals=0
        ),
        compiler_params=pltpu.CompilerParams(vmem_limit_bytes=16 << 20),
        name="combine",
    )(rows, returned)


def over_plane(array, by_y, by_x):
    places = [(y, x) for y in range(SIDE) for x in range(SIDE)]
    return lax.ppermute(
        array, "ep", [(y * SIDE + x, (y + by_y) % SIDE * SIDE + (x + by_x) % SIDE) for y, x in places]
    )


def along_z(array, by, tp_count):
    chips = tp_count // 2
    return lax.ppermute(array, "tp", [(z * 2 + c, (z + by) % chips * 2 + c) for z in range(chips) for c in range(2)])


def other_core(array, tp_count):
    return lax.ppermute(array, "tp", [(j, j ^ 1) for j in range(tp_count)])


def layer(stream, norm_gain, gate_rows, up_rows, down_rows, chosen, affinity):
    ep_count = lax.axis_size("ep")
    tp_count = lax.axis_size("tp")
    block, features = stream.shape
    slots = 4 * block // ep_count
    ep_index = lax.axis_index("ep").astype(jnp.int32)
    place = jnp.stack([ep_index // SIDE, ep_index % SIDE])
    bounds = (jnp.arange(ep_count, dtype=jnp.int32) * tp_count + lax.axis_index("tp")) * block
    low, high, own = prepare(stream, norm_gain, (gate_rows, up_rows, down_rows))
    lows = [low] + [over_plane(low, 0, t) for t in range(1, SIDE)]
    highs = [high] + [over_plane(high, t, 0) for t in range(1, SIDE)]
    ahead, behind = along_z(own, 1, tp_count), along_z(own, -1, tp_count)
    rows_there, weights = windows(bounds, chosen, affinity, block, slots)
    rows_here = lax.all_to_all(rows_there, "ep", split_axis=0, concat_axis=0, tiled=True)
    ahead2, behind2 = along_z(ahead, 1, tp_count), along_z(behind, -1, tp_count)
    picked_low = pick(True, place, rows_here, lows)
    arrived_low = [picked_low[0]] + [over_plane(picked_low[d], d, 0) for d in range(1, SIDE)]
    picked_high = pick(False, place, rows_here, highs)
    arrived_high = [picked_high[0]] + [over_plane(picked_high[d], 0, d) for d in range(1, SIDE)]
    cut = own.shape[1] // 2
    far = [
        along_z(ahead2[:, :cut], 2, tp_count),
        along_z(behind2[:, cut:], -2, tp_count),
        along_z(ahead2, 1, tp_count),
        along_z(behind2, -1, tp_count),
    ]
    held = [own, ahead, behind, ahead2, behind2, *far]
    pieces = held + [other_core(piece, tp_count) for piece in held]
    produced = expert(place, weights, arrived_low, arrived_high, *assemble(pieces))
    returned = lax.all_to_all(produced, "ep", split_axis=0, concat_axis=0, tiled=True)
    return combine(rows_here, returned.reshape(-1, features), block)


def solution(mesh):
    return jax.shard_map(
        layer,
        mesh=mesh,
        in_specs=(
            P(("ep", "tp"), None),
            P(),
            P("ep", "tp", None),
            P("ep", "tp", None),
            P("ep", "tp", None),
            P("ep", None),
            P("ep", None),
        ),
        out_specs=P(("ep", "tp"), None),
        check_vma=False,
    )
```

```python
import functools

import jax
import jax.numpy as jnp
from jax import lax
from jax.experimental import pallas as pl
from jax.experimental.pallas import tpu as pltpu
from jax.sharding import PartitionSpec as P

epsilon = 1e-06
SIDE = 4
SMEM = pl.BlockSpec(memory_space=pltpu.SMEM)
VMEM = pl.BlockSpec(memory_space=pltpu.VMEM)


def wrap(value):
    return lax.rem(value + SIDE, SIDE)


def windows_kernel(block, slots, bounds_ref, list_ref, affinity_ref, rows_ref, weights_ref):
    listed = list_ref[...]
    lines = listed.shape[0]
    lane = lax.broadcasted_iota(jnp.int32, (1, slots), 1)
    for j in range(weights_ref.shape[0]):
        y, x = divmod(j, SIDE)
        bound = bounds_ref[j]
        start = jnp.sum((listed < bound).astype(jnp.int32))
        line, shift = start // slots, start % slots
        first = jnp.minimum(line, lines - 1)
        second = jnp.minimum(line + 1, lines - 1)
        back = lax.rem(slots - shift, slots)

        def window(ref):
            low = pltpu.roll(ref[pl.ds(first, 1), :], back, 1)
            high = pltpu.roll(ref[pl.ds(second, 1), :], back, 1)
            return jnp.where(lane < slots - shift, low, high)

        rows = window(list_ref) - bound
        rows = jnp.where((rows >= 0) & (rows < block), rows, -1)
        for t in range(SIDE):
            rows_ref[y * SIDE + (x + t) % SIDE, t : t + 1, :] = rows
            rows_ref[(y + t) % SIDE * SIDE + x, SIDE + t : SIDE + t + 1, :] = rows
        weights_ref[j : j + 1, :] = window(affinity_ref)


def windows(bounds, listed, affinity, block, slots):
    count = bounds.shape[0]
    return pl.pallas_call(
        functools.partial(windows_kernel, block, slots),
        in_specs=[SMEM, VMEM, VMEM],
        out_shape=(
            jax.ShapeDtypeStruct((count, 2 * SIDE, slots), jnp.int32),
            jax.ShapeDtypeStruct((count, slots), jnp.float32),
        ),
        cost_estimate=pl.CostEstimate(flops=8_000_000, bytes_accessed=150_000, transcendentals=0),
        name="windows",
    )(bounds, listed.reshape(-1, slots), affinity.reshape(-1, slots))


def prepare_kernel(stream_ref, gain_ref, gate_ref, up_ref, down_ref, low_ref, high_ref, piece_ref):
    values = stream_ref[...].astype(jnp.float32)
    inverse = lax.rsqrt(jnp.mean(values * values, axis=-1, keepdims=True) + epsilon)
    normed = (values * inverse * gain_ref[...]).astype(jnp.bfloat16)
    half = low_ref.shape[1]
    low_ref[...] = normed[:, :half]
    high_ref[...] = normed[:, half:]

    @pl.when(pl.program_id(0) == 0)
    def _():
        piece_ref[0:1] = gate_ref[...]
        piece_ref[1:2] = up_ref[...]
        piece_ref[2:3] = down_ref[...]


def prepare(stream, norm_gain, parts):
    rows, features = stream.shape
    step, half = rows // 2, features // 2
    part = pl.BlockSpec(parts[0].shape, lambda i: (0, 0, 0))
    piece = (3, *parts[0].shape[1:])
    return pl.pallas_call(
        prepare_kernel,
        grid=(2,),
        in_specs=[
            pl.BlockSpec((step, features), lambda i: (i, 0)),
            pl.BlockSpec((1, features), lambda i: (0, 0)),
            part,
            part,
            part,
        ],
        out_specs=(
            pl.BlockSpec((step, half), lambda i: (i, 0)),
            pl.BlockSpec((step, half), lambda i: (i, 0)),
            pl.BlockSpec(piece, lambda i: (0, 0, 0)),
        ),
        out_shape=(
            jax.ShapeDtypeStruct((rows, half), jnp.bfloat16),
            jax.ShapeDtypeStruct((rows, half), jnp.bfloat16),
            jax.ShapeDtypeStruct(piece, jnp.bfloat16),
        ),
        cost_estimate=pl.CostEstimate(flops=3_000_000, bytes_accessed=3 << 20, transcendentals=512),
        name="prepare",
    )(stream, norm_gain.reshape(1, features), *parts)


def pick_kernel(along_y, place_ref, rows_ref, *refs):
    sources, outs = refs[:SIDE], refs[SIDE:]
    y, x = place_ref[0], place_ref[1]
    tokens, slots = sources[0].shape[0], rows_ref.shape[2]
    token = lax.broadcasted_iota(jnp.int32, (slots, tokens), 1).astype(jnp.float32)
    columns = []
    for d in range(SIDE):
        e = wrap(y + d) * SIDE + x if along_y else y * SIDE + wrap(x + d)
        columns.append(rows_ref[e].astype(jnp.float32).T)
    for t in range(SIDE):
        k = t if along_y else SIDE + t
        chosen = jnp.concatenate(
            [jnp.where(column[:, k : k + 1] == token, 1.0, 0.0).astype(jnp.bfloat16) for column in columns]
        )
        rows = jnp.dot(chosen, sources[t][...], preferred_element_type=jnp.float32).astype(jnp.bfloat16)
        for d in range(SIDE):
            outs[d][t * slots : (t + 1) * slots, :] = rows[d * slots : (d + 1) * slots, :]


def pick(along_y, place, rows, sources):
    tokens, half = sources[0].shape
    slots = rows.shape[2]
    return pl.pallas_call(
        functools.partial(pick_kernel, along_y),
        in_specs=[SMEM] + [VMEM] * (1 + SIDE),
        out_shape=[jax.ShapeDtypeStruct((SIDE * slots, half), jnp.bfloat16)] * SIDE,
        cost_estimate=pl.CostEstimate(
            flops=2 * SIDE * SIDE * slots * tokens * half, bytes_accessed=4 << 20, transcendentals=0
        ),
        compiler_params=pltpu.CompilerParams(vmem_limit_bytes=12 << 20),
        name="pick_y" if along_y else "pick_x",
    )(place, rows, *sources)


def assemble_kernel(*refs):
    pieces, outs = refs[:-3], refs[-3:]
    at = 0
    for piece in pieces:
        width = piece.shape[1]
        for j, out in enumerate(outs):
            out[at : at + width, :] = piece[j]
        at += width


def assemble(pieces):
    shape = jax.ShapeDtypeStruct((sum(piece.shape[1] for piece in pieces), pieces[0].shape[2]), jnp.bfloat16)
    return pl.pallas_call(
        assemble_kernel,
        in_specs=[VMEM] * len(pieces),
        out_shape=[shape] * 3,
        cost_estimate=pl.CostEstimate(flops=1_000_000, bytes_accessed=12 << 20, transcendentals=0),
        compiler_params=pltpu.CompilerParams(vmem_limit_bytes=16 << 20),
        name="assemble",
    )(*pieces)


STEPS = (
    ((2, 0), (2, 1), (2, 2), (2, 3)),
    ((0, 2), (1, 2), (3, 2), (1, 1)),
    ((1, 0), (1, 3), (0, 1), (3, 1)),
    ((3, 0), (3, 3), (0, 3), (0, 0)),
)
FINISHED = (
    (("low", 2),),
    (("high", 2),),
    (("low", 1), ("high", 1)),
    (("low", 3), ("high", 3), ("low", 0), ("high", 0)),
)


def members(piece):
    half, fixed = piece
    return [(fixed, k) if half == "low" else (k, fixed) for k in range(SIDE)]


def expert_kernel(number, names, place_ref, weights_ref, gate_ref, up_ref, down_ref, *refs):
    inputs_ref, result_ref = refs[-2:]
    ref = dict(zip(names, refs))
    blocks = STEPS[number]
    y, x = place_ref[0], place_ref[1]
    slots, half = weights_ref.shape[1], ref["in", "low", blocks[0][0]].shape[1]
    for k, (a, b) in enumerate(blocks):
        inputs_ref[k * slots : (k + 1) * slots, :half] = ref["in", "low", a][b * slots : (b + 1) * slots, :]
        inputs_ref[k * slots : (k + 1) * slots, half:] = ref["in", "high", b][a * slots : (a + 1) * slots, :]
    last = (((1,), (1,)), ((), ()))
    units = gate_ref.shape[0]
    width, rows = units // 4, inputs_ref.shape[0] // 2

    def work(i, carry):
        at = pl.ds(pl.multiple_of(i * rows, rows), rows)
        inputs = inputs_ref[at, :]
        hidden = []
        for f in range(0, units, width):
            gate_sum = lax.dot_general(inputs, gate_ref[f : f + width, :], last, preferred_element_type=jnp.float32)
            up_sum = lax.dot_general(inputs, up_ref[f : f + width, :], last, preferred_element_type=jnp.float32)
            hidden.append((gate_sum / (1.0 + jnp.exp(-gate_sum)) * up_sum).astype(jnp.bfloat16))
        result_ref[at, :] = jnp.dot(jnp.concatenate(hidden, 1), down_ref[...], preferred_element_type=jnp.float32)
        return carry

    lax.fori_loop(0, 2, work, 0)
    made = {}
    for k, (a, b) in enumerate(blocks):
        line = weights_ref[pl.ds(wrap(y - a) * SIDE + wrap(x - b), 1), :]
        column = jnp.broadcast_to(line, (slots, slots)).T[:, :1]
        made[a, b] = (result_ref[k * slots : (k + 1) * slots, :] * column).astype(jnp.bfloat16)

    def part(block, which):
        if block in made:
            return made[block][:, :half] if which == "low" else made[block][:, half:]
        step = next(n for n in range(number) if block in STEPS[n])
        k = STEPS[step].index(block)
        return ref["made", which, step][k * slots : (k + 1) * slots, :]

    for name in names:
        if name[0] == "out":
            for k, block in enumerate(members(name[1:])):
                ref[name][k * slots : (k + 1) * slots, :] = part(block, name[1])
        if name == ("made", name[1], number):
            for k, block in enumerate(blocks):
                ref[name][k * slots : (k + 1) * slots, :] = part(block, name[1])


def expert(number, place, weights, projections, low, high, made):
    slots, half = weights.shape[1], low[0].shape[1]
    features, units = 2 * half, projections[0].shape[0]
    total = SIDE * slots
    blocks = STEPS[number]
    inputs = {("in", "low", a): low[a] for a, _ in blocks}
    inputs.update({("in", "high", b): high[b] for _, b in blocks})
    for piece in FINISHED[number]:
        for block in members(piece):
            step = next(n for n in range(len(STEPS)) if block in STEPS[n])
            if step < number:
                inputs["made", piece[0], step] = made[piece[0], step]
    outs = [("out", *piece) for piece in FINISHED[number]]
    for which in ("low", "high"):
        later = [
            piece
            for done in FINISHED[number + 1 :]
            for piece in done
            if piece[0] == which and any(block in blocks for block in members(piece))
        ]
        if later:
            outs.append(("made", which, number))
    results = pl.pallas_call(
        functools.partial(expert_kernel, number, [*inputs, *outs]),
        in_specs=[SMEM] + [VMEM] * (4 + len(inputs)),
        out_shape=[jax.ShapeDtypeStruct((total, half), jnp.bfloat16)] * len(outs),
        scratch_shapes=[pltpu.VMEM((total, features), jnp.bfloat16), pltpu.VMEM((total, features), jnp.float32)],
        cost_estimate=pl.CostEstimate(
            flops=6 * total * units * features, bytes_accessed=4 * total * features, transcendentals=2 * total * units
        ),
        compiler_params=pltpu.CompilerParams(vmem_limit_bytes=28 << 20),
    )(place, weights, *projections, *inputs.values())
    results = dict(zip(outs, results))
    made.update({name[1:]: array for name, array in results.items() if name[0] == "made"})
    return {name[1:]: array for name, array in results.items() if name[0] == "out"}


def relay_kernel(along_y, place_ref, rows_ref, *refs):
    pieces, outs = refs[:SIDE], refs[SIDE:]
    y, x = place_ref[0], place_ref[1]
    tokens, slots = outs[0].shape[0], rows_ref.shape[2]
    token = lax.broadcasted_iota(jnp.int32, (tokens, slots), 0)
    lists = []
    for d in range(SIDE):
        lists.append(rows_ref[wrap(y + d) * SIDE + x if along_y else y * SIDE + wrap(x + d)])
    for t in range(SIDE):
        k = t if along_y else SIDE + t
        chosen = jnp.concatenate(
            [jnp.where(token == rows[k : k + 1, :], 1.0, 0.0).astype(jnp.bfloat16) for rows in lists], 1
        )
        rows = jnp.concatenate([piece[t * slots : (t + 1) * slots, :] for piece in pieces])
        outs[t][...] = jnp.dot(chosen, rows, preferred_element_type=jnp.float32).astype(jnp.bfloat16)


def relay(along_y, place, rows, pieces, tokens):
    total, half = pieces[0].shape
    return pl.pallas_call(
        functools.partial(relay_kernel, along_y),
        in_specs=[SMEM] + [VMEM] * (1 + SIDE),
        out_shape=[jax.ShapeDtypeStruct((tokens, half), jnp.bfloat16)] * SIDE,
        cost_estimate=pl.CostEstimate(
            flops=2 * SIDE * total * tokens * half, bytes_accessed=4 << 20, transcendentals=0
        ),
        compiler_params=pltpu.CompilerParams(vmem_limit_bytes=12 << 20),
        name="relay_y" if along_y else "relay_x",
    )(place, rows, *pieces)


def add_kernel(*refs):
    out_ref = refs[-1]
    half = refs[0].shape[1]
    for n, parts in enumerate((refs[:SIDE], refs[SIDE : 2 * SIDE])):
        total = parts[0][...].astype(jnp.float32)
        for part in parts[1:]:
            total = total + part[...].astype(jnp.float32)
        out_ref[:, n * half : (n + 1) * half] = total.astype(jnp.bfloat16)


def add(lows, highs):
    tokens, half = lows[0].shape
    step = tokens // 4
    return pl.pallas_call(
        add_kernel,
        grid=(4,),
        in_specs=[pl.BlockSpec((step, half), lambda i: (i, 0))] * (2 * SIDE),
        out_specs=pl.BlockSpec((step, 2 * half), lambda i: (i, 0)),
        out_shape=jax.ShapeDtypeStruct((tokens, 2 * half), jnp.bfloat16),
        cost_estimate=pl.CostEstimate(flops=4_000_000, bytes_accessed=5 << 20, transcendentals=0),
        compiler_params=pltpu.CompilerParams(vmem_limit_bytes=12 << 20),
        name="add",
    )(*lows, *highs)


def over_plane(array, by_y, by_x):
    places = [(y, x) for y in range(SIDE) for x in range(SIDE)]
    return lax.ppermute(
        array, "ep", [(y * SIDE + x, (y + by_y) % SIDE * SIDE + (x + by_x) % SIDE) for y, x in places]
    )


def along_z(array, by, tp_count):
    chips = tp_count // 2
    return lax.ppermute(array, "tp", [(z * 2 + c, (z + by) % chips * 2 + c) for z in range(chips) for c in range(2)])


def other_core(array, tp_count):
    return lax.ppermute(array, "tp", [(j, j ^ 1) for j in range(tp_count)])


def layer(stream, norm_gain, gate_rows, up_rows, down_rows, chosen, affinity):
    ep_count = lax.axis_size("ep")
    tp_count = lax.axis_size("tp")
    block, _ = stream.shape
    slots = 4 * block // ep_count
    ep_index = lax.axis_index("ep").astype(jnp.int32)
    place = jnp.stack([ep_index // SIDE, ep_index % SIDE])
    bounds = (jnp.arange(ep_count, dtype=jnp.int32) * tp_count + lax.axis_index("tp")) * block
    low, high, own = prepare(stream, norm_gain, (gate_rows, up_rows, down_rows))
    lows = [low] + [over_plane(low, 0, t) for t in range(1, SIDE)]
    highs = [high] + [over_plane(high, t, 0) for t in range(1, SIDE)]
    ahead, behind = along_z(own, 1, tp_count), along_z(own, -1, tp_count)
    rows_there, weights = windows(bounds, chosen, affinity, block, slots)
    rows_here = lax.all_to_all(rows_there, "ep", split_axis=0, concat_axis=0, tiled=True)
    ahead2, behind2 = along_z(ahead, 1, tp_count), along_z(behind, -1, tp_count)
    picked_low = pick(True, place, rows_here, lows)
    arrived_low = [picked_low[0]] + [over_plane(picked_low[d], d, 0) for d in range(1, SIDE)]
    picked_high = pick(False, place, rows_here, highs)
    arrived_high = [picked_high[0]] + [over_plane(picked_high[d], 0, d) for d in range(1, SIDE)]
    cut = own.shape[1] // 2
    far = [
        along_z(ahead2[:, :cut], 2, tp_count),
        along_z(behind2[:, cut:], -2, tp_count),
        along_z(ahead2, 1, tp_count),
        along_z(behind2, -1, tp_count),
    ]
    held = [own, ahead, behind, ahead2, behind2, *far]
    pieces = held + [other_core(piece, tp_count) for piece in held]
    projections = assemble(pieces)
    made, back = {}, {}
    for number in range(len(STEPS)):
        finished = expert(number, place, weights, projections, arrived_low, arrived_high, made)
        for (half, by), piece in finished.items():
            if by == 0:
                back[half, by] = piece
            elif half == "low":
                back[half, by] = over_plane(piece, -by, 0)
            else:
                back[half, by] = over_plane(piece, 0, -by)
    sums_low = relay(True, place, rows_here, [back["low", d] for d in range(SIDE)], block)
    sums_low = [sums_low[0]] + [over_plane(sums_low[t], 0, -t) for t in range(1, SIDE)]
    sums_high = relay(False, place, rows_here, [back["high", d] for d in range(SIDE)], block)
    sums_high = [sums_high[0]] + [over_plane(sums_high[t], -t, 0) for t in range(1, SIDE)]
    return add(sums_low, sums_high)


def solution(mesh):
    return jax.shard_map(
        layer,
        mesh=mesh,
        in_specs=(
            P(("ep", "tp"), None),
            P(),
            P("ep", "tp", None),
            P("ep", "tp", None),
            P("ep", "tp", None),
            P("ep", None),
            P("ep", None),
        ),
        out_specs=P(("ep", "tp"), None),
        check_vma=False,
    )
```

```python
import functools

import jax
import jax.numpy as jnp
from jax import lax
from jax.experimental import pallas as pl
from jax.experimental.pallas import tpu as pltpu
from jax.sharding import PartitionSpec as P

epsilon = 1e-06
SIDE = 4
SMEM = pl.BlockSpec(memory_space=pltpu.SMEM)
VMEM = pl.BlockSpec(memory_space=pltpu.VMEM)


def wrap(value):
    return lax.rem(value + SIDE, SIDE)


def windows_kernel(block, slots, bounds_ref, list_ref, affinity_ref, rows_ref, weights_ref):
    listed = list_ref[...]
    lines = listed.shape[0]
    lane = lax.broadcasted_iota(jnp.int32, (1, slots), 1)
    for j in range(weights_ref.shape[0]):
        y, x = divmod(j, SIDE)
        bound = bounds_ref[j]
        start = jnp.sum((listed < bound).astype(jnp.int32))
        line, shift = start // slots, start % slots
        first = jnp.minimum(line, lines - 1)
        second = jnp.minimum(line + 1, lines - 1)
        back = lax.rem(slots - shift, slots)

        def window(ref):
            low = pltpu.roll(ref[pl.ds(first, 1), :], back, 1)
            high = pltpu.roll(ref[pl.ds(second, 1), :], back, 1)
            return jnp.where(lane < slots - shift, low, high)

        rows = window(list_ref) - bound
        rows = jnp.where((rows >= 0) & (rows < block), rows, -1)
        for t in range(SIDE):
            rows_ref[y * SIDE + (x + t) % SIDE, t : t + 1, :] = rows
            rows_ref[(y + t) % SIDE * SIDE + x, SIDE + t : SIDE + t + 1, :] = rows
        weights_ref[j : j + 1, :] = window(affinity_ref)


def windows(bounds, listed, affinity, block, slots):
    count = bounds.shape[0]
    return pl.pallas_call(
        functools.partial(windows_kernel, block, slots),
        in_specs=[SMEM, VMEM, VMEM],
        out_shape=(
            jax.ShapeDtypeStruct((count, 2 * SIDE, slots), jnp.int32),
            jax.ShapeDtypeStruct((count, slots), jnp.float32),
        ),
        cost_estimate=pl.CostEstimate(flops=8_000_000, bytes_accessed=150_000, transcendentals=0),
        name="windows",
    )(bounds, listed.reshape(-1, slots), affinity.reshape(-1, slots))


def prepare_kernel(stream_ref, gain_ref, gate_ref, up_ref, down_ref, low_ref, high_ref, piece_ref):
    values = stream_ref[...].astype(jnp.float32)
    inverse = lax.rsqrt(jnp.mean(values * values, axis=-1, keepdims=True) + epsilon)
    normed = (values * inverse * gain_ref[...]).astype(jnp.bfloat16)
    half = low_ref.shape[1]
    low_ref[...] = normed[:, :half]
    high_ref[...] = normed[:, half:]

    @pl.when(pl.program_id(0) == 0)
    def _():
        piece_ref[0:1] = gate_ref[...]
        piece_ref[1:2] = up_ref[...]
        piece_ref[2:3] = down_ref[...]


def prepare(stream, norm_gain, parts):
    rows, features = stream.shape
    step, half = rows // 2, features // 2
    part = pl.BlockSpec(parts[0].shape, lambda i: (0, 0, 0))
    piece = (3, *parts[0].shape[1:])
    return pl.pallas_call(
        prepare_kernel,
        grid=(2,),
        in_specs=[
            pl.BlockSpec((step, features), lambda i: (i, 0)),
            pl.BlockSpec((1, features), lambda i: (0, 0)),
            part,
            part,
            part,
        ],
        out_specs=(
            pl.BlockSpec((step, half), lambda i: (i, 0)),
            pl.BlockSpec((step, half), lambda i: (i, 0)),
            pl.BlockSpec(piece, lambda i: (0, 0, 0)),
        ),
        out_shape=(
            jax.ShapeDtypeStruct((rows, half), jnp.bfloat16),
            jax.ShapeDtypeStruct((rows, half), jnp.bfloat16),
            jax.ShapeDtypeStruct(piece, jnp.bfloat16),
        ),
        cost_estimate=pl.CostEstimate(flops=3_000_000, bytes_accessed=3 << 20, transcendentals=512),
        name="prepare",
    )(stream, norm_gain.reshape(1, features), *parts)


def pick_kernel(along_y, place_ref, rows_ref, *refs):
    sources, outs = refs[:SIDE], refs[SIDE:]
    y, x = place_ref[0], place_ref[1]
    tokens, slots = sources[0].shape[0], rows_ref.shape[2]
    token = lax.broadcasted_iota(jnp.int32, (slots, tokens), 1).astype(jnp.float32)
    columns = []
    for d in range(SIDE):
        e = wrap(y + d) * SIDE + x if along_y else y * SIDE + wrap(x + d)
        columns.append(rows_ref[e].astype(jnp.float32).T)
    for t in range(SIDE):
        k = t if along_y else SIDE + t
        chosen = jnp.concatenate(
            [jnp.where(column[:, k : k + 1] == token, 1.0, 0.0).astype(jnp.bfloat16) for column in columns]
        )
        rows = jnp.dot(chosen, sources[t][...], preferred_element_type=jnp.float32).astype(jnp.bfloat16)
        for d in range(SIDE):
            outs[d][t * slots : (t + 1) * slots, :] = rows[d * slots : (d + 1) * slots, :]


def pick(along_y, place, rows, sources):
    tokens, half = sources[0].shape
    slots = rows.shape[2]
    return pl.pallas_call(
        functools.partial(pick_kernel, along_y),
        in_specs=[SMEM] + [VMEM] * (1 + SIDE),
        out_shape=[jax.ShapeDtypeStruct((SIDE * slots, half), jnp.bfloat16)] * SIDE,
        cost_estimate=pl.CostEstimate(
            flops=2 * SIDE * SIDE * slots * tokens * half, bytes_accessed=4 << 20, transcendentals=0
        ),
        compiler_params=pltpu.CompilerParams(vmem_limit_bytes=12 << 20),
        name="pick_y" if along_y else "pick_x",
    )(place, rows, *sources)


def stack_kernel(*refs):
    out_ref, at = refs[-1], 0
    for piece in refs[:-1]:
        width = piece.shape[1]
        out_ref[:, at : at + width, :] = piece[...]
        at += width


def stack(pieces):
    return pl.pallas_call(
        stack_kernel,
        in_specs=[VMEM] * len(pieces),
        out_shape=jax.ShapeDtypeStruct(
            (3, sum(piece.shape[1] for piece in pieces), pieces[0].shape[2]), jnp.bfloat16
        ),
        cost_estimate=pl.CostEstimate(flops=1_000_000, bytes_accessed=4 << 20, transcendentals=0),
        compiler_params=pltpu.CompilerParams(vmem_limit_bytes=8 << 20),
    )(*pieces)


def assemble_kernel(*refs):
    pieces, outs = refs[:-3], refs[-3:]
    at = 0
    for piece in pieces:
        width = piece.shape[1]
        for j, out in enumerate(outs):
            out[at : at + width, :] = piece[j]
        at += width


def assemble(pieces):
    shape = jax.ShapeDtypeStruct((sum(piece.shape[1] for piece in pieces), pieces[0].shape[2]), jnp.bfloat16)
    return pl.pallas_call(
        assemble_kernel,
        in_specs=[VMEM] * len(pieces),
        out_shape=[shape] * 3,
        cost_estimate=pl.CostEstimate(flops=1_000_000, bytes_accessed=12 << 20, transcendentals=0),
        compiler_params=pltpu.CompilerParams(vmem_limit_bytes=16 << 20),
        name="assemble",
    )(*pieces)


STEPS = (
    ((2, 0), (2, 1), (2, 2), (2, 3), (0, 2), (1, 2), (3, 2), (1, 1)),
    ((1, 0), (1, 3), (0, 1), (3, 1), (3, 0), (3, 3), (0, 3), (0, 0)),
)
FINISHED = (
    (("low", 2), ("high", 2)),
    (("low", 1), ("high", 1), ("low", 3), ("high", 3), ("low", 0), ("high", 0)),
)


def members(piece):
    half, fixed = piece
    return [(fixed, k) if half == "low" else (k, fixed) for k in range(SIDE)]


def expert_kernel(number, names, place_ref, weights_ref, gate_ref, up_ref, down_ref, *refs):
    inputs_ref, result_ref, columns_ref = refs[-3:]
    ref = dict(zip(names, refs))
    blocks = STEPS[number]
    y, x = place_ref[0], place_ref[1]
    slots, half = weights_ref.shape[1], ref["in", "low", blocks[0][0]].shape[1]
    for k, (a, b) in enumerate(blocks):
        at = slice(k * slots, (k + 1) * slots)
        inputs_ref[at, :half] = ref["in", "low", a][b * slots : (b + 1) * slots, :]
        inputs_ref[at, half:] = ref["in", "high", b][a * slots : (a + 1) * slots, :]
        line = weights_ref[pl.ds(wrap(y - a) * SIDE + wrap(x - b), 1), :]
        columns_ref[at, :] = jnp.broadcast_to(line, (slots, slots)).T
    last = (((1,), (1,)), ((), ()))
    units = gate_ref.shape[0]
    width, rows = units // 4, SIDE * slots

    def work(i, carry):
        at = pl.ds(pl.multiple_of(i * rows, rows), rows)
        inputs = inputs_ref[at, :]
        hidden = []
        for f in range(0, units, width):
            gate_sum = lax.dot_general(inputs, gate_ref[f : f + width, :], last, preferred_element_type=jnp.float32)
            up_sum = lax.dot_general(inputs, up_ref[f : f + width, :], last, preferred_element_type=jnp.float32)
            hidden.append((gate_sum / (1.0 + jnp.exp(-gate_sum)) * up_sum).astype(jnp.bfloat16))
        result = jnp.dot(jnp.concatenate(hidden, 1), down_ref[...], preferred_element_type=jnp.float32)
        result_ref[at, :] = (result * columns_ref[at, :][:, :1]).astype(jnp.bfloat16)
        return carry

    lax.fori_loop(0, len(blocks) // SIDE, work, 0)

    def part(block, which):
        if block in blocks:
            k = blocks.index(block)
            cut = slice(0, half) if which == "low" else slice(half, 2 * half)
            return result_ref[k * slots : (k + 1) * slots, cut]
        step = next(n for n in range(number) if block in STEPS[n])
        k = STEPS[step].index(block)
        return ref["made", which, step][k * slots : (k + 1) * slots, :]

    for name in names:
        if name[0] == "out":
            for k, block in enumerate(members(name[1:])):
                ref[name][k * slots : (k + 1) * slots, :] = part(block, name[1])
        if name == ("made", name[1], number):
            for k, block in enumerate(blocks):
                ref[name][k * slots : (k + 1) * slots, :] = part(block, name[1])


def expert(number, place, weights, projections, low, high, made):
    slots, half = weights.shape[1], low[0].shape[1]
    features, units = 2 * half, projections[0].shape[0]
    piece_rows = SIDE * slots
    blocks = STEPS[number]
    total = len(blocks) * slots
    inputs = {("in", "low", a): low[a] for a, _ in blocks}
    inputs.update({("in", "high", b): high[b] for _, b in blocks})
    for piece in FINISHED[number]:
        for block in members(piece):
            step = next(n for n in range(len(STEPS)) if block in STEPS[n])
            if step < number:
                inputs["made", piece[0], step] = made[piece[0], step]
    outs = [("out", *piece) for piece in FINISHED[number]]
    for which in ("low", "high"):
        later = [
            piece
            for done in FINISHED[number + 1 :]
            for piece in done
            if piece[0] == which and any(block in blocks for block in members(piece))
        ]
        if later:
            outs.append(("made", which, number))
    shapes = [(piece_rows if name[0] == "out" else total, half) for name in outs]
    results = pl.pallas_call(
        functools.partial(expert_kernel, number, [*inputs, *outs]),
        in_specs=[SMEM] + [VMEM] * (4 + len(inputs)),
        out_shape=[jax.ShapeDtypeStruct(shape, jnp.bfloat16) for shape in shapes],
        scratch_shapes=[
            pltpu.VMEM((total, features), jnp.bfloat16),
            pltpu.VMEM((total, features), jnp.bfloat16),
            pltpu.VMEM((total, slots), jnp.float32),
        ],
        cost_estimate=pl.CostEstimate(
            flops=6 * total * units * features, bytes_accessed=4 * total * features, transcendentals=2 * total * units
        ),
        compiler_params=pltpu.CompilerParams(vmem_limit_bytes=28 << 20),
    )(place, weights, *projections, *inputs.values())
    results = dict(zip(outs, results))
    made.update({name[1:]: array for name, array in results.items() if name[0] == "made"})
    return {name[1:]: array for name, array in results.items() if name[0] == "out"}


def relay_kernel(along_y, place_ref, rows_ref, *refs):
    pieces, outs = refs[:SIDE], refs[SIDE:]
    y, x = place_ref[0], place_ref[1]
    tokens, slots = outs[0].shape[0], rows_ref.shape[2]
    step = tokens // 2
    token = lax.broadcasted_iota(jnp.int32, (step, slots), 0)
    lists = []
    for d in range(SIDE):
        lists.append(rows_ref[wrap(y + d) * SIDE + x if along_y else y * SIDE + wrap(x + d)])

    def work(i, carry):
        for t in range(SIDE):
            k = t if along_y else SIDE + t
            chosen = jnp.concatenate(
                [jnp.where(token + i * step == rows[k : k + 1, :], 1.0, 0.0).astype(jnp.bfloat16) for rows in lists], 1
            )
            rows = jnp.concatenate([piece[t * slots : (t + 1) * slots, :] for piece in pieces])
            total = jnp.dot(chosen, rows, preferred_element_type=jnp.float32)
            outs[t][pl.ds(pl.multiple_of(i * step, step), step), :] = total.astype(jnp.bfloat16)
        return carry

    lax.fori_loop(0, 2, work, 0)


def relay(along_y, place, rows, pieces, tokens):
    total, half = pieces[0].shape
    return pl.pallas_call(
        functools.partial(relay_kernel, along_y),
        in_specs=[SMEM] + [VMEM] * (1 + SIDE),
        out_shape=[jax.ShapeDtypeStruct((tokens, half), jnp.bfloat16)] * SIDE,
        cost_estimate=pl.CostEstimate(
            flops=2 * SIDE * total * tokens * half, bytes_accessed=4 << 20, transcendentals=0
        ),
        compiler_params=pltpu.CompilerParams(vmem_limit_bytes=12 << 20),
        name="relay_y" if along_y else "relay_x",
    )(place, rows, *pieces)


def add_kernel(*refs):
    out_ref = refs[-1]
    half = refs[0].shape[1]
    for n, parts in enumerate((refs[:SIDE], refs[SIDE : 2 * SIDE])):
        total = parts[0][...].astype(jnp.float32)
        for part in parts[1:]:
            total = total + part[...].astype(jnp.float32)
        out_ref[:, n * half : (n + 1) * half] = total.astype(jnp.bfloat16)


def add(lows, highs):
    tokens, half = lows[0].shape
    step = tokens // 4
    return pl.pallas_call(
        add_kernel,
        grid=(4,),
        in_specs=[pl.BlockSpec((step, half), lambda i: (i, 0))] * (2 * SIDE),
        out_specs=pl.BlockSpec((step, 2 * half), lambda i: (i, 0)),
        out_shape=jax.ShapeDtypeStruct((tokens, 2 * half), jnp.bfloat16),
        cost_estimate=pl.CostEstimate(flops=4_000_000, bytes_accessed=5 << 20, transcendentals=0),
        compiler_params=pltpu.CompilerParams(vmem_limit_bytes=12 << 20),
        name="add",
    )(*lows, *highs)


def over_plane(array, by_y, by_x):
    places = [(y, x) for y in range(SIDE) for x in range(SIDE)]
    return lax.ppermute(
        array, "ep", [(y * SIDE + x, (y + by_y) % SIDE * SIDE + (x + by_x) % SIDE) for y, x in places]
    )


def along_z(array, by, tp_count):
    chips = tp_count // 2
    return lax.ppermute(array, "tp", [(z * 2 + c, (z + by) % chips * 2 + c) for z in range(chips) for c in range(2)])


def other_core(array, tp_count):
    return lax.ppermute(array, "tp", [(j, j ^ 1) for j in range(tp_count)])


def layer(stream, norm_gain, gate_rows, up_rows, down_rows, chosen, affinity):
    ep_count = lax.axis_size("ep")
    tp_count = lax.axis_size("tp")
    block, _ = stream.shape
    slots = 4 * block // ep_count
    ep_index = lax.axis_index("ep").astype(jnp.int32)
    place = jnp.stack([ep_index // SIDE, ep_index % SIDE])
    bounds = (jnp.arange(ep_count, dtype=jnp.int32) * tp_count + lax.axis_index("tp")) * block
    low, high, own = prepare(stream, norm_gain, (gate_rows, up_rows, down_rows))
    lows = [low] + [over_plane(low, 0, t) for t in range(1, SIDE)]
    highs = [high] + [over_plane(high, t, 0) for t in range(1, SIDE)]
    ahead, behind = along_z(own, 1, tp_count), along_z(own, -1, tp_count)
    rows_there, weights = windows(bounds, chosen, affinity, block, slots)
    rows_here = lax.all_to_all(rows_there, "ep", split_axis=0, concat_axis=0, tiled=True)
    ahead2, behind2 = along_z(ahead, 1, tp_count), along_z(behind, -1, tp_count)
    picked_low = pick(True, place, rows_here, lows)
    arrived_low = [picked_low[0]] + [over_plane(picked_low[d], d, 0) for d in range(1, SIDE)]
    picked_high = pick(False, place, rows_here, highs)
    arrived_high = [picked_high[0]] + [over_plane(picked_high[d], 0, d) for d in range(1, SIDE)]
    cut = own.shape[1] // 2
    far = [
        along_z(ahead2[:, :cut], 2, tp_count),
        along_z(behind2[:, cut:], -2, tp_count),
        along_z(ahead2, 1, tp_count),
        along_z(behind2, -1, tp_count),
    ]
    early = stack([own, ahead, behind, ahead2, behind2])
    late = stack(far)
    pieces = [early, late, other_core(early, tp_count), other_core(late, tp_count)]
    projections = assemble(pieces)
    made, back = {}, {}
    for number in range(len(STEPS)):
        finished = expert(number, place, weights, projections, arrived_low, arrived_high, made)
        for (half, by), piece in finished.items():
            if by == 0:
                back[half, by] = piece
            elif half == "low":
                back[half, by] = over_plane(piece, -by, 0)
            else:
                back[half, by] = over_plane(piece, 0, -by)
    sums_low = relay(True, place, rows_here, [back["low", d] for d in range(SIDE)], block)
    sums_low = [sums_low[0]] + [over_plane(sums_low[t], 0, -t) for t in range(1, SIDE)]
    sums_high = relay(False, place, rows_here, [back["high", d] for d in range(SIDE)], block)
    sums_high = [sums_high[0]] + [over_plane(sums_high[t], -t, 0) for t in range(1, SIDE)]
    return add(sums_low, sums_high)


def solution(mesh):
    return jax.shard_map(
        layer,
        mesh=mesh,
        in_specs=(
            P(("ep", "tp"), None),
            P(),
            P("ep", "tp", None),
            P("ep", "tp", None),
            P("ep", "tp", None),
            P("ep", None),
            P("ep", None),
        ),
        out_specs=P(("ep", "tp"), None),
        check_vma=False,
    )
```

```python
import functools

import jax
import jax.numpy as jnp
from jax import lax
from jax.experimental import pallas as pl
from jax.experimental.pallas import tpu as pltpu
from jax.sharding import PartitionSpec as P

epsilon = 1e-06
SIDE = 4
SMEM = pl.BlockSpec(memory_space=pltpu.SMEM)
VMEM = pl.BlockSpec(memory_space=pltpu.VMEM)


def wrap(value):
    return lax.rem(value + SIDE, SIDE)


def windows_kernel(block, slots, bounds_ref, list_ref, affinity_ref, rows_ref, weights_ref):
    listed = list_ref[...]
    lines = listed.shape[0]
    lane = lax.broadcasted_iota(jnp.int32, (1, slots), 1)

    def cut(j, carry):
        y, x = j // SIDE, lax.rem(j, SIDE)
        bound = bounds_ref[j]
        start = jnp.sum((listed < bound).astype(jnp.int32))
        line, shift = start // slots, start % slots
        first = jnp.minimum(line, lines - 1)
        second = jnp.minimum(line + 1, lines - 1)
        back = lax.rem(slots - shift, slots)

        def window(ref):
            low = pltpu.roll(ref[pl.ds(first, 1), :], back, 1)
            high = pltpu.roll(ref[pl.ds(second, 1), :], back, 1)
            return jnp.where(lane < slots - shift, low, high)

        rows = window(list_ref) - bound
        rows = jnp.where((rows >= 0) & (rows < block), rows, -1)
        for t in range(SIDE):
            rows_ref[y * SIDE + wrap(x + t - SIDE), t : t + 1, :] = rows
            rows_ref[wrap(y + t - SIDE) * SIDE + x, SIDE + t : SIDE + t + 1, :] = rows
        weights_ref[pl.ds(j, 1), :] = window(affinity_ref)
        return carry

    lax.fori_loop(0, weights_ref.shape[0], cut, 0, unroll=4)


def windows(bounds, listed, affinity, block, slots):
    count = bounds.shape[0]
    return pl.pallas_call(
        functools.partial(windows_kernel, block, slots),
        in_specs=[SMEM, VMEM, VMEM],
        out_shape=(
            jax.ShapeDtypeStruct((count, 2 * SIDE, slots), jnp.int32),
            jax.ShapeDtypeStruct((count, slots), jnp.float32),
        ),
        cost_estimate=pl.CostEstimate(flops=8_000_000, bytes_accessed=150_000, transcendentals=0),
        name="windows",
    )(bounds, listed.reshape(-1, slots), affinity.reshape(-1, slots))


def prepare_kernel(stream_ref, gain_ref, gate_ref, up_ref, down_ref, low_ref, high_ref, piece_ref):
    values = stream_ref[...].astype(jnp.float32)
    inverse = lax.rsqrt(jnp.mean(values * values, axis=-1, keepdims=True) + epsilon)
    normed = (values * inverse * gain_ref[...]).astype(jnp.bfloat16)
    half = low_ref.shape[1]
    low_ref[...] = normed[:, :half]
    high_ref[...] = normed[:, half:]

    @pl.when(pl.program_id(0) == 0)
    def _():
        piece_ref[0:1] = gate_ref[...]
        piece_ref[1:2] = up_ref[...]
        piece_ref[2:3] = down_ref[...]


def prepare(stream, norm_gain, parts):
    rows, features = stream.shape
    step, half = rows // 2, features // 2
    part = pl.BlockSpec(parts[0].shape, lambda i: (0, 0, 0))
    piece = (3, *parts[0].shape[1:])
    return pl.pallas_call(
        prepare_kernel,
        grid=(2,),
        in_specs=[
            pl.BlockSpec((step, features), lambda i: (i, 0)),
            pl.BlockSpec((1, features), lambda i: (0, 0)),
            part,
            part,
            part,
        ],
        out_specs=(
            pl.BlockSpec((step, half), lambda i: (i, 0)),
            pl.BlockSpec((step, half), lambda i: (i, 0)),
            pl.BlockSpec(piece, lambda i: (0, 0, 0)),
        ),
        out_shape=(
            jax.ShapeDtypeStruct((rows, half), jnp.bfloat16),
            jax.ShapeDtypeStruct((rows, half), jnp.bfloat16),
            jax.ShapeDtypeStruct(piece, jnp.bfloat16),
        ),
        cost_estimate=pl.CostEstimate(flops=3_000_000, bytes_accessed=3 << 20, transcendentals=512),
        name="prepare",
    )(stream, norm_gain.reshape(1, features), *parts)


def pick_kernel(along_y, place_ref, rows_ref, own_ref, after_ref, top_ref, bottom_ref, before_ref, *refs):
    outs = refs[:SIDE]
    across_ref, chosen_ref = refs[SIDE:]
    y, x = place_ref[0], place_ref[1]
    tokens, half = own_ref.shape
    slots = rows_ref.shape[2]
    across_ref[: tokens // 2, :] = top_ref[...]
    across_ref[tokens // 2 :, :] = bottom_ref[...]
    token = lax.broadcasted_iota(jnp.int32, (slots, tokens), 1).astype(jnp.float32)
    for d in range(SIDE):
        e = wrap(y + d) * SIDE + x if along_y else y * SIDE + wrap(x + d)
        column = rows_ref[e].astype(jnp.float32).T
        for t in range(SIDE):
            k = t if along_y else SIDE + t
            chosen_ref[t, d * slots : (d + 1) * slots, :] = jnp.where(column[:, k : k + 1] == token, 1.0, 0.0).astype(
                jnp.bfloat16
            )
    step = half // 2

    def work(i, carry):
        at = pl.ds(pl.multiple_of(i * step, step), step)
        for t, source in enumerate((own_ref, after_ref, across_ref, before_ref)):
            rows = jnp.dot(chosen_ref[t], source[:, at], preferred_element_type=jnp.float32).astype(jnp.bfloat16)
            for d in range(SIDE):
                outs[d][t * slots : (t + 1) * slots, at] = rows[d * slots : (d + 1) * slots, :]
        return carry

    lax.fori_loop(0, 2, work, 0)


def pick(along_y, place, rows, sources):
    tokens, half = sources[0].shape
    slots = rows.shape[2]
    return pl.pallas_call(
        functools.partial(pick_kernel, along_y),
        in_specs=[SMEM] + [VMEM] * 6,
        out_shape=[jax.ShapeDtypeStruct((SIDE * slots, half), jnp.bfloat16)] * SIDE,
        scratch_shapes=[
            pltpu.VMEM((tokens, half), jnp.bfloat16),
            pltpu.VMEM((SIDE, SIDE * slots, tokens), jnp.bfloat16),
        ],
        cost_estimate=pl.CostEstimate(
            flops=2 * SIDE * SIDE * slots * tokens * half, bytes_accessed=4 << 20, transcendentals=0
        ),
        compiler_params=pltpu.CompilerParams(vmem_limit_bytes=14 << 20),
        name="pick_y" if along_y else "pick_x",
    )(place, rows, *sources)


def stack_kernel(*refs):
    out_ref, at = refs[-1], 0
    for piece in refs[:-1]:
        width = piece.shape[1]
        out_ref[:, at : at + width, :] = piece[...]
        at += width


def stack(pieces):
    return pl.pallas_call(
        stack_kernel,
        in_specs=[VMEM] * len(pieces),
        out_shape=jax.ShapeDtypeStruct(
            (3, sum(piece.shape[1] for piece in pieces), pieces[0].shape[2]), jnp.bfloat16
        ),
        cost_estimate=pl.CostEstimate(flops=1_000_000, bytes_accessed=4 << 20, transcendentals=0),
        compiler_params=pltpu.CompilerParams(vmem_limit_bytes=8 << 20),
    )(*pieces)


def assemble_kernel(*refs):
    pieces, outs = refs[:-3], refs[-3:]
    step = 64
    at = 0
    for piece in pieces:
        width = piece.shape[1]
        for j, out in enumerate(outs):

            def move(i, carry, piece=piece, out=out, j=j, at=at):
                rows = pl.multiple_of(i * step, step)
                out[pl.ds(at + rows, step), :] = piece[j, pl.ds(rows, step), :]
                return carry

            lax.fori_loop(0, width // step, move, 0)
        at += width


def assemble(pieces):
    shape = jax.ShapeDtypeStruct((sum(piece.shape[1] for piece in pieces), pieces[0].shape[2]), jnp.bfloat16)
    return pl.pallas_call(
        assemble_kernel,
        in_specs=[VMEM] * len(pieces),
        out_shape=[shape] * 3,
        cost_estimate=pl.CostEstimate(flops=1_000_000, bytes_accessed=12 << 20, transcendentals=0),
        compiler_params=pltpu.CompilerParams(vmem_limit_bytes=16 << 20),
        name="assemble",
    )(*pieces)


STEPS = (
    ((2, 0), (2, 1), (2, 2), (2, 3), (0, 2), (1, 2), (3, 2), (1, 1)),
    ((1, 0), (1, 3), (0, 1), (3, 1), (3, 0), (3, 3), (0, 3), (0, 0)),
)
FINISHED = (
    (("low", 2), ("high", 2)),
    (("low", 1), ("high", 1), ("low", 3), ("high", 3), ("low", 0), ("high", 0)),
)


def members(piece):
    half, fixed = piece
    return [(fixed, k) if half == "low" else (k, fixed) for k in range(SIDE)]


def expert_kernel(number, names, place_ref, weights_ref, gate_ref, up_ref, down_ref, *refs):
    inputs_ref, result_ref, columns_ref = refs[-3:]
    ref = dict(zip(names, refs))
    blocks = STEPS[number]
    y, x = place_ref[0], place_ref[1]
    slots, half = weights_ref.shape[1], ref["in", "low", blocks[0][0]].shape[1]
    for k, (a, b) in enumerate(blocks):
        at = slice(k * slots, (k + 1) * slots)
        inputs_ref[at, :half] = ref["in", "low", a][b * slots : (b + 1) * slots, :]
        inputs_ref[at, half:] = ref["in", "high", b][a * slots : (a + 1) * slots, :]
        line = weights_ref[pl.ds(wrap(y - a) * SIDE + wrap(x - b), 1), :]
        columns_ref[at, :] = jnp.broadcast_to(line, (slots, slots)).T
    last = (((1,), (1,)), ((), ()))
    units = gate_ref.shape[0]
    width, rows = units // 4, SIDE * slots

    def work(i, carry):
        at = pl.ds(pl.multiple_of(i * rows, rows), rows)
        inputs = inputs_ref[at, :]
        hidden = []
        for f in range(0, units, width):
            gate_sum = lax.dot_general(inputs, gate_ref[f : f + width, :], last, preferred_element_type=jnp.float32)
            up_sum = lax.dot_general(inputs, up_ref[f : f + width, :], last, preferred_element_type=jnp.float32)
            hidden.append((gate_sum / (1.0 + jnp.exp(-gate_sum)) * up_sum).astype(jnp.bfloat16))
        result = jnp.dot(jnp.concatenate(hidden, 1), down_ref[...], preferred_element_type=jnp.float32)
        result_ref[at, :] = (result * columns_ref[at, :][:, :1]).astype(jnp.bfloat16)
        return carry

    lax.fori_loop(0, len(blocks) // SIDE, work, 0)

    def part(block, which):
        if block in blocks:
            k = blocks.index(block)
            cut = slice(0, half) if which == "low" else slice(half, 2 * half)
            return result_ref[k * slots : (k + 1) * slots, cut]
        step = next(n for n in range(number) if block in STEPS[n])
        k = STEPS[step].index(block)
        return ref["made", which, step][k * slots : (k + 1) * slots, :]

    for name in names:
        if name[0] == "out":
            for k, block in enumerate(members(name[1:])):
                ref[name][k * slots : (k + 1) * slots, :] = part(block, name[1])
        if name == ("made", name[1], number):
            for k, block in enumerate(blocks):
                ref[name][k * slots : (k + 1) * slots, :] = part(block, name[1])


def expert(number, place, weights, projections, low, high, made):
    slots, half = weights.shape[1], low[0].shape[1]
    features, units = 2 * half, projections[0].shape[0]
    piece_rows = SIDE * slots
    blocks = STEPS[number]
    total = len(blocks) * slots
    inputs = {("in", "low", a): low[a] for a, _ in blocks}
    inputs.update({("in", "high", b): high[b] for _, b in blocks})
    for piece in FINISHED[number]:
        for block in members(piece):
            step = next(n for n in range(len(STEPS)) if block in STEPS[n])
            if step < number:
                inputs["made", piece[0], step] = made[piece[0], step]
    outs = [("out", *piece) for piece in FINISHED[number]]
    for which in ("low", "high"):
        later = [
            piece
            for done in FINISHED[number + 1 :]
            for piece in done
            if piece[0] == which and any(block in blocks for block in members(piece))
        ]
        if later:
            outs.append(("made", which, number))
    shapes = [(piece_rows if name[0] == "out" else total, half) for name in outs]
    results = pl.pallas_call(
        functools.partial(expert_kernel, number, [*inputs, *outs]),
        in_specs=[SMEM] + [VMEM] * (4 + len(inputs)),
        out_shape=[jax.ShapeDtypeStruct(shape, jnp.bfloat16) for shape in shapes],
        scratch_shapes=[
            pltpu.VMEM((total, features), jnp.bfloat16),
            pltpu.VMEM((total, features), jnp.bfloat16),
            pltpu.VMEM((total, slots), jnp.float32),
        ],
        cost_estimate=pl.CostEstimate(
            flops=6 * total * units * features, bytes_accessed=4 * total * features, transcendentals=2 * total * units
        ),
        compiler_params=pltpu.CompilerParams(vmem_limit_bytes=28 << 20),
    )(place, weights, *projections, *inputs.values())
    results = dict(zip(outs, results))
    made.update({name[1:]: array for name, array in results.items() if name[0] == "made"})
    return {name[1:]: array for name, array in results.items() if name[0] == "out"}


def relay_kernel(along_y, place_ref, rows_ref, *refs):
    pieces, outs = refs[:SIDE], refs[SIDE:]
    y, x = place_ref[0], place_ref[1]
    tokens, slots = outs[0].shape[0], rows_ref.shape[2]
    step = tokens // 2
    token = lax.broadcasted_iota(jnp.int32, (step, slots), 0)
    lists = []
    for d in range(SIDE):
        lists.append(rows_ref[wrap(y + d) * SIDE + x if along_y else y * SIDE + wrap(x + d)])

    def work(i, carry):
        for t in range(SIDE):
            k = t if along_y else SIDE + t
            chosen = jnp.concatenate(
                [jnp.where(token + i * step == rows[k : k + 1, :], 1.0, 0.0).astype(jnp.bfloat16) for rows in lists], 1
            )
            rows = jnp.concatenate([piece[t * slots : (t + 1) * slots, :] for piece in pieces])
            total = jnp.dot(chosen, rows, preferred_element_type=jnp.float32)
            outs[t][pl.ds(pl.multiple_of(i * step, step), step), :] = total.astype(jnp.bfloat16)
        return carry

    lax.fori_loop(0, 2, work, 0)


def relay(along_y, place, rows, pieces, tokens):
    total, half = pieces[0].shape
    return pl.pallas_call(
        functools.partial(relay_kernel, along_y),
        in_specs=[SMEM] + [VMEM] * (1 + SIDE),
        out_shape=[jax.ShapeDtypeStruct((tokens, half), jnp.bfloat16)] * SIDE,
        cost_estimate=pl.CostEstimate(
            flops=2 * SIDE * total * tokens * half, bytes_accessed=4 << 20, transcendentals=0
        ),
        compiler_params=pltpu.CompilerParams(vmem_limit_bytes=12 << 20),
        name="relay_y" if along_y else "relay_x",
    )(place, rows, *pieces)


def add_kernel(*refs):
    out_ref = refs[-1]
    half = refs[0].shape[1]
    for n, parts in enumerate((refs[:SIDE], refs[SIDE : 2 * SIDE])):
        total = parts[0][...].astype(jnp.float32)
        for part in parts[1:]:
            total = total + part[...].astype(jnp.float32)
        out_ref[:, n * half : (n + 1) * half] = total.astype(jnp.bfloat16)


def add(lows, highs):
    tokens, half = lows[0].shape
    step = tokens // 4
    return pl.pallas_call(
        add_kernel,
        grid=(4,),
        in_specs=[pl.BlockSpec((step, half), lambda i: (i, 0))] * (2 * SIDE),
        out_specs=pl.BlockSpec((step, 2 * half), lambda i: (i, 0)),
        out_shape=jax.ShapeDtypeStruct((tokens, 2 * half), jnp.bfloat16),
        cost_estimate=pl.CostEstimate(flops=4_000_000, bytes_accessed=5 << 20, transcendentals=0),
        compiler_params=pltpu.CompilerParams(vmem_limit_bytes=12 << 20),
        name="add",
    )(*lows, *highs)


def over_plane(array, by_y, by_x):
    places = [(y, x) for y in range(SIDE) for x in range(SIDE)]
    return lax.ppermute(
        array, "ep", [(y * SIDE + x, (y + by_y) % SIDE * SIDE + (x + by_x) % SIDE) for y, x in places]
    )


def along_z(array, by, tp_count):
    chips = tp_count // 2
    return lax.ppermute(array, "tp", [(z * 2 + c, (z + by) % chips * 2 + c) for z in range(chips) for c in range(2)])


def other_core(array, tp_count):
    return lax.ppermute(array, "tp", [(j, j ^ 1) for j in range(tp_count)])


def layer(stream, norm_gain, gate_rows, up_rows, down_rows, chosen, affinity):
    ep_count = lax.axis_size("ep")
    tp_count = lax.axis_size("tp")
    block, _ = stream.shape
    slots = 4 * block // ep_count
    ep_index = lax.axis_index("ep").astype(jnp.int32)
    place = jnp.stack([ep_index // SIDE, ep_index % SIDE])
    bounds = (jnp.arange(ep_count, dtype=jnp.int32) * tp_count + lax.axis_index("tp")) * block
    low, high, own = prepare(stream, norm_gain, (gate_rows, up_rows, down_rows))
    left, right = over_plane(low, 0, 1), over_plane(low, 0, -1)
    down, up = over_plane(high, 1, 0), over_plane(high, -1, 0)
    ahead, behind = along_z(own, 1, tp_count), along_z(own, -1, tp_count)
    rows_there, weights = windows(bounds, chosen, affinity, block, slots)
    rows_here = lax.all_to_all(rows_there, "ep", split_axis=0, concat_axis=0, tiled=True)
    mid = block // 2
    lows = [low, left, over_plane(left[:mid], 0, 1), over_plane(right[mid:], 0, -1), right]
    highs = [high, down, over_plane(down[:mid], 1, 0), over_plane(up[mid:], -1, 0), up]
    ahead2, behind2 = along_z(ahead, 1, tp_count), along_z(behind, -1, tp_count)
    picked_low = pick(True, place, rows_here, lows)
    arrived_low = [picked_low[0]] + [over_plane(picked_low[d], d, 0) for d in range(1, SIDE)]
    picked_high = pick(False, place, rows_here, highs)
    arrived_high = [picked_high[0]] + [over_plane(picked_high[d], 0, d) for d in range(1, SIDE)]
    cut = own.shape[1] // 2
    far = [
        along_z(ahead2[:, :cut], 2, tp_count),
        along_z(behind2[:, cut:], -2, tp_count),
        along_z(ahead2, 1, tp_count),
        along_z(behind2, -1, tp_count),
    ]
    early = stack([own, ahead, behind, ahead2, behind2])
    late = stack(far)
    pieces = [early, late, other_core(early, tp_count), other_core(late, tp_count)]
    projections = assemble(pieces)
    made, back = {}, {}
    for number in range(len(STEPS)):
        finished = expert(number, place, weights, projections, arrived_low, arrived_high, made)
        for (half, by), piece in finished.items():
            if by == 0:
                back[half, by] = piece
            elif half == "low":
                back[half, by] = over_plane(piece, -by, 0)
            else:
                back[half, by] = over_plane(piece, 0, -by)
    sums_low = relay(True, place, rows_here, [back["low", d] for d in range(SIDE)], block)
    sums_low = [sums_low[0]] + [over_plane(sums_low[t], 0, -t) for t in range(1, SIDE)]
    sums_high = relay(False, place, rows_here, [back["high", d] for d in range(SIDE)], block)
    sums_high = [sums_high[0]] + [over_plane(sums_high[t], -t, 0) for t in range(1, SIDE)]
    return add(sums_low, sums_high)


def solution(mesh):
    return jax.shard_map(
        layer,
        mesh=mesh,
        in_specs=(
            P(("ep", "tp"), None),
            P(),
            P("ep", "tp", None),
            P("ep", "tp", None),
            P("ep", "tp", None),
            P("ep", None),
            P("ep", None),
        ),
        out_specs=P(("ep", "tp"), None),
        check_vma=False,
    )
```

```python
import functools

import jax
import jax.numpy as jnp
from jax import lax
from jax.experimental import pallas as pl
from jax.experimental.pallas import tpu as pltpu
from jax.sharding import PartitionSpec as P

epsilon = 1e-06
SIDE = 4
SMEM = pl.BlockSpec(memory_space=pltpu.SMEM)
VMEM = pl.BlockSpec(memory_space=pltpu.VMEM)


def wrap(value):
    return lax.rem(value + SIDE, SIDE)


def windows_kernel(block, slots, bounds_ref, list_ref, affinity_ref, rows_ref, weights_ref):
    listed = list_ref[...]
    lines = listed.shape[0]
    lane = lax.broadcasted_iota(jnp.int32, (1, slots), 1)

    def cut(j, carry):
        y, x = j // SIDE, lax.rem(j, SIDE)
        bound = bounds_ref[j]
        start = jnp.sum((listed < bound).astype(jnp.int32))
        line, shift = start // slots, start % slots
        first = jnp.minimum(line, lines - 1)
        second = jnp.minimum(line + 1, lines - 1)
        back = lax.rem(slots - shift, slots)

        def window(ref):
            low = pltpu.roll(ref[pl.ds(first, 1), :], back, 1)
            high = pltpu.roll(ref[pl.ds(second, 1), :], back, 1)
            return jnp.where(lane < slots - shift, low, high)

        rows = window(list_ref) - bound
        rows = jnp.where((rows >= 0) & (rows < block), rows, -1)
        for t in range(SIDE):
            rows_ref[y * SIDE + wrap(x + t - SIDE), t : t + 1, :] = rows
            rows_ref[wrap(y + t - SIDE) * SIDE + x, SIDE + t : SIDE + t + 1, :] = rows
        weights_ref[pl.ds(j, 1), :] = window(affinity_ref)
        return carry

    lax.fori_loop(0, weights_ref.shape[0], cut, 0, unroll=4)


def windows(bounds, listed, affinity, block, slots):
    count = bounds.shape[0]
    return pl.pallas_call(
        functools.partial(windows_kernel, block, slots),
        in_specs=[SMEM, VMEM, VMEM],
        out_shape=(
            jax.ShapeDtypeStruct((count, 2 * SIDE, slots), jnp.int32),
            jax.ShapeDtypeStruct((count, slots), jnp.float32),
        ),
        cost_estimate=pl.CostEstimate(flops=8_000_000, bytes_accessed=150_000, transcendentals=0),
        name="windows",
    )(bounds, listed.reshape(-1, slots), affinity.reshape(-1, slots))


def prepare_kernel(stream_ref, gain_ref, gate_ref, up_ref, down_ref, low_ref, high_ref, piece_ref):
    values = stream_ref[...].astype(jnp.float32)
    inverse = lax.rsqrt(jnp.mean(values * values, axis=-1, keepdims=True) + epsilon)
    normed = (values * inverse * gain_ref[...]).astype(jnp.bfloat16)
    half = low_ref.shape[1]
    low_ref[...] = normed[:, :half]
    high_ref[...] = normed[:, half:]

    @pl.when(pl.program_id(0) == 0)
    def _():
        piece_ref[0:1] = gate_ref[...]
        piece_ref[1:2] = up_ref[...]
        piece_ref[2:3] = down_ref[...]


def prepare(stream, norm_gain, parts):
    rows, features = stream.shape
    step, half = rows // 2, features // 2
    part = pl.BlockSpec(parts[0].shape, lambda i: (0, 0, 0))
    piece = (3, *parts[0].shape[1:])
    return pl.pallas_call(
        prepare_kernel,
        grid=(2,),
        in_specs=[
            pl.BlockSpec((step, features), lambda i: (i, 0)),
            pl.BlockSpec((1, features), lambda i: (0, 0)),
            part,
            part,
            part,
        ],
        out_specs=(
            pl.BlockSpec((step, half), lambda i: (i, 0)),
            pl.BlockSpec((step, half), lambda i: (i, 0)),
            pl.BlockSpec(piece, lambda i: (0, 0, 0)),
        ),
        out_shape=(
            jax.ShapeDtypeStruct((rows, half), jnp.bfloat16),
            jax.ShapeDtypeStruct((rows, half), jnp.bfloat16),
            jax.ShapeDtypeStruct(piece, jnp.bfloat16),
        ),
        cost_estimate=pl.CostEstimate(flops=3_000_000, bytes_accessed=3 << 20, transcendentals=512),
        name="prepare",
    )(stream, norm_gain.reshape(1, features), *parts)


def pick_kernel(place_ref, rows_ref, *refs):
    count = SIDE + 1
    across_ref, chosen_ref = refs[-2:]
    y, x = place_ref[0], place_ref[1]
    slots = rows_ref.shape[2]
    for along_y in (True, False):
        own_ref, after_ref, top_ref, bottom_ref, before_ref = refs[:count] if along_y else refs[count : 2 * count]
        outs = refs[2 * count :][:SIDE] if along_y else refs[2 * count + SIDE :][:SIDE]
        tokens, half = own_ref.shape
        across_ref[: tokens // 2, :] = top_ref[...]
        across_ref[tokens // 2 :, :] = bottom_ref[...]
        token = lax.broadcasted_iota(jnp.int32, (slots, tokens), 1).astype(jnp.float32)
        for d in range(SIDE):
            e = wrap(y + d) * SIDE + x if along_y else y * SIDE + wrap(x + d)
            column = rows_ref[e].astype(jnp.float32).T
            for t in range(SIDE):
                k = t if along_y else SIDE + t
                chosen_ref[t, d * slots : (d + 1) * slots, :] = jnp.where(
                    column[:, k : k + 1] == token, 1.0, 0.0
                ).astype(jnp.bfloat16)
        step = half // 2

        def work(i, carry, outs=outs, sources=(own_ref, after_ref, across_ref, before_ref), step=step):
            at = pl.ds(pl.multiple_of(i * step, step), step)
            for t, source in enumerate(sources):
                rows = jnp.dot(chosen_ref[t], source[:, at], preferred_element_type=jnp.float32).astype(jnp.bfloat16)
                for d in range(SIDE):
                    outs[d][t * slots : (t + 1) * slots, at] = rows[d * slots : (d + 1) * slots, :]
            return carry

        lax.fori_loop(0, 2, work, 0)


def pick(place, rows, lows, highs):
    tokens, half = lows[0].shape
    slots = rows.shape[2]
    return pl.pallas_call(
        pick_kernel,
        in_specs=[SMEM] + [VMEM] * (1 + len(lows) + len(highs)),
        out_shape=[jax.ShapeDtypeStruct((SIDE * slots, half), jnp.bfloat16)] * (2 * SIDE),
        scratch_shapes=[
            pltpu.VMEM((tokens, half), jnp.bfloat16),
            pltpu.VMEM((SIDE, SIDE * slots, tokens), jnp.bfloat16),
        ],
        cost_estimate=pl.CostEstimate(
            flops=4 * SIDE * SIDE * slots * tokens * half, bytes_accessed=8 << 20, transcendentals=0
        ),
        compiler_params=pltpu.CompilerParams(vmem_limit_bytes=20 << 20),
        name="pick",
    )(place, rows, *lows, *highs)


def stack_kernel(*refs):
    out_ref, at = refs[-1], 0
    for piece in refs[:-1]:
        width = piece.shape[1]
        out_ref[:, at : at + width, :] = piece[...]
        at += width


def stack(pieces):
    return pl.pallas_call(
        stack_kernel,
        in_specs=[VMEM] * len(pieces),
        out_shape=jax.ShapeDtypeStruct(
            (3, sum(piece.shape[1] for piece in pieces), pieces[0].shape[2]), jnp.bfloat16
        ),
        cost_estimate=pl.CostEstimate(flops=1_000_000, bytes_accessed=4 << 20, transcendentals=0),
        compiler_params=pltpu.CompilerParams(vmem_limit_bytes=8 << 20),
    )(*pieces)


def assemble_kernel(*refs):
    pieces, outs = refs[:-3], refs[-3:]
    step = 64
    at = 0
    for piece in pieces:
        width = piece.shape[1]
        for j, out in enumerate(outs):

            def move(i, carry, piece=piece, out=out, j=j, at=at):
                rows = pl.multiple_of(i * step, step)
                out[pl.ds(at + rows, step), :] = piece[j, pl.ds(rows, step), :]
                return carry

            lax.fori_loop(0, width // step, move, 0)
        at += width


def assemble(pieces):
    shape = jax.ShapeDtypeStruct((sum(piece.shape[1] for piece in pieces), pieces[0].shape[2]), jnp.bfloat16)
    return pl.pallas_call(
        assemble_kernel,
        in_specs=[VMEM] * len(pieces),
        out_shape=[shape] * 3,
        cost_estimate=pl.CostEstimate(flops=1_000_000, bytes_accessed=12 << 20, transcendentals=0),
        compiler_params=pltpu.CompilerParams(vmem_limit_bytes=16 << 20),
        name="assemble",
    )(*pieces)


STEPS = (
    ((2, 0), (2, 1), (2, 2), (2, 3), (0, 2), (1, 2), (3, 2), (1, 1)),
    ((1, 0), (1, 3), (0, 1), (3, 1), (3, 0), (3, 3), (0, 3), (0, 0)),
)
FINISHED = (
    (("low", 2), ("high", 2)),
    (("low", 1), ("high", 1), ("low", 3), ("high", 3), ("low", 0), ("high", 0)),
)


def members(piece):
    half, fixed = piece
    return [(fixed, k) if half == "low" else (k, fixed) for k in range(SIDE)]


def expert_kernel(number, names, place_ref, weights_ref, gate_ref, up_ref, down_ref, *refs):
    inputs_ref, result_ref, columns_ref = refs[-3:]
    ref = dict(zip(names, refs))
    blocks = STEPS[number]
    y, x = place_ref[0], place_ref[1]
    slots, half = weights_ref.shape[1], ref["in", "low", blocks[0][0]].shape[1]
    for k, (a, b) in enumerate(blocks):
        at = slice(k * slots, (k + 1) * slots)
        inputs_ref[at, :half] = ref["in", "low", a][b * slots : (b + 1) * slots, :]
        inputs_ref[at, half:] = ref["in", "high", b][a * slots : (a + 1) * slots, :]
        line = weights_ref[pl.ds(wrap(y - a) * SIDE + wrap(x - b), 1), :]
        columns_ref[at, :] = jnp.broadcast_to(line, (slots, slots)).T
    last = (((1,), (1,)), ((), ()))
    units = gate_ref.shape[0]
    width, rows = units // 4, SIDE * slots

    def work(i, carry):
        at = pl.ds(pl.multiple_of(i * rows, rows), rows)
        inputs = inputs_ref[at, :]
        hidden = []
        for f in range(0, units, width):
            gate_sum = lax.dot_general(inputs, gate_ref[f : f + width, :], last, preferred_element_type=jnp.float32)
            up_sum = lax.dot_general(inputs, up_ref[f : f + width, :], last, preferred_element_type=jnp.float32)
            hidden.append((gate_sum / (1.0 + jnp.exp(-gate_sum)) * up_sum).astype(jnp.bfloat16))
        result = jnp.dot(jnp.concatenate(hidden, 1), down_ref[...], preferred_element_type=jnp.float32)
        result_ref[at, :] = (result * columns_ref[at, :][:, :1]).astype(jnp.bfloat16)
        return carry

    lax.fori_loop(0, len(blocks) // SIDE, work, 0)

    def part(block, which):
        if block in blocks:
            k = blocks.index(block)
            cut = slice(0, half) if which == "low" else slice(half, 2 * half)
            return result_ref[k * slots : (k + 1) * slots, cut]
        step = next(n for n in range(number) if block in STEPS[n])
        k = STEPS[step].index(block)
        return ref["made", which, step][k * slots : (k + 1) * slots, :]

    for name in names:
        if name[0] == "out":
            for k, block in enumerate(members(name[1:])):
                ref[name][k * slots : (k + 1) * slots, :] = part(block, name[1])
        if name == ("made", name[1], number):
            for k, block in enumerate(blocks):
                ref[name][k * slots : (k + 1) * slots, :] = part(block, name[1])


def expert(number, place, weights, projections, low, high, made):
    slots, half = weights.shape[1], low[0].shape[1]
    features, units = 2 * half, projections[0].shape[0]
    piece_rows = SIDE * slots
    blocks = STEPS[number]
    total = len(blocks) * slots
    inputs = {("in", "low", a): low[a] for a, _ in blocks}
    inputs.update({("in", "high", b): high[b] for _, b in blocks})
    for piece in FINISHED[number]:
        for block in members(piece):
            step = next(n for n in range(len(STEPS)) if block in STEPS[n])
            if step < number:
                inputs["made", piece[0], step] = made[piece[0], step]
    outs = [("out", *piece) for piece in FINISHED[number]]
    for which in ("low", "high"):
        later = [
            piece
            for done in FINISHED[number + 1 :]
            for piece in done
            if piece[0] == which and any(block in blocks for block in members(piece))
        ]
        if later:
            outs.append(("made", which, number))
    shapes = [(piece_rows if name[0] == "out" else total, half) for name in outs]
    results = pl.pallas_call(
        functools.partial(expert_kernel, number, [*inputs, *outs]),
        in_specs=[SMEM] + [VMEM] * (4 + len(inputs)),
        out_shape=[jax.ShapeDtypeStruct(shape, jnp.bfloat16) for shape in shapes],
        scratch_shapes=[
            pltpu.VMEM((total, features), jnp.bfloat16),
            pltpu.VMEM((total, features), jnp.bfloat16),
            pltpu.VMEM((total, slots), jnp.float32),
        ],
        cost_estimate=pl.CostEstimate(
            flops=6 * total * units * features, bytes_accessed=4 * total * features, transcendentals=2 * total * units
        ),
        compiler_params=pltpu.CompilerParams(vmem_limit_bytes=28 << 20),
    )(place, weights, *projections, *inputs.values())
    results = dict(zip(outs, results))
    made.update({name[1:]: array for name, array in results.items() if name[0] == "made"})
    return {name[1:]: array for name, array in results.items() if name[0] == "out"}


def relay_kernel(place_ref, rows_ref, *refs):
    y, x = place_ref[0], place_ref[1]
    tokens, slots = refs[-1].shape[0], rows_ref.shape[2]
    step = tokens // 2
    token = lax.broadcasted_iota(jnp.int32, (step, slots), 0)
    for along_y in (True, False):
        first = 0 if along_y else SIDE
        pieces, outs = refs[first : first + SIDE], refs[first + 2 * SIDE : first + 3 * SIDE]
        lists = [rows_ref[wrap(y + d) * SIDE + x if along_y else y * SIDE + wrap(x + d)] for d in range(SIDE)]

        def work(i, carry, first=first, pieces=pieces, outs=outs, lists=lists):
            for t in range(SIDE):
                k = first + t
                chosen = jnp.concatenate(
                    [
                        jnp.where(token + i * step == rows[k : k + 1, :], 1.0, 0.0).astype(jnp.bfloat16)
                        for rows in lists
                    ],
                    1,
                )
                rows = jnp.concatenate([piece[t * slots : (t + 1) * slots, :] for piece in pieces])
                total = jnp.dot(chosen, rows, preferred_element_type=jnp.float32)
                outs[t][pl.ds(pl.multiple_of(i * step, step), step), :] = total.astype(jnp.bfloat16)
            return carry

        lax.fori_loop(0, 2, work, 0)


def relay(place, rows, lows, highs, tokens):
    total, half = lows[0].shape
    return pl.pallas_call(
        relay_kernel,
        in_specs=[SMEM] + [VMEM] * (1 + len(lows) + len(highs)),
        out_shape=[jax.ShapeDtypeStruct((tokens, half), jnp.bfloat16)] * (2 * SIDE),
        cost_estimate=pl.CostEstimate(
            flops=4 * SIDE * total * tokens * half, bytes_accessed=8 << 20, transcendentals=0
        ),
        compiler_params=pltpu.CompilerParams(vmem_limit_bytes=16 << 20),
        name="relay",
    )(place, rows, *lows, *highs)


def add_kernel(*refs):
    out_ref = refs[-1]
    half = refs[0].shape[1]
    for n, parts in enumerate((refs[:SIDE], refs[SIDE : 2 * SIDE])):
        total = parts[0][...].astype(jnp.float32)
        for part in parts[1:]:
            total = total + part[...].astype(jnp.float32)
        out_ref[:, n * half : (n + 1) * half] = total.astype(jnp.bfloat16)


def add(lows, highs):
    tokens, half = lows[0].shape
    step = tokens // 4
    return pl.pallas_call(
        add_kernel,
        grid=(4,),
        in_specs=[pl.BlockSpec((step, half), lambda i: (i, 0))] * (2 * SIDE),
        out_specs=pl.BlockSpec((step, 2 * half), lambda i: (i, 0)),
        out_shape=jax.ShapeDtypeStruct((tokens, 2 * half), jnp.bfloat16),
        cost_estimate=pl.CostEstimate(flops=4_000_000, bytes_accessed=5 << 20, transcendentals=0),
        compiler_params=pltpu.CompilerParams(vmem_limit_bytes=12 << 20),
        name="add",
    )(*lows, *highs)


def over_plane(array, by_y, by_x):
    places = [(y, x) for y in range(SIDE) for x in range(SIDE)]
    return lax.ppermute(
        array, "ep", [(y * SIDE + x, (y + by_y) % SIDE * SIDE + (x + by_x) % SIDE) for y, x in places]
    )


def along_z(array, by, tp_count):
    chips = tp_count // 2
    return lax.ppermute(array, "tp", [(z * 2 + c, (z + by) % chips * 2 + c) for z in range(chips) for c in range(2)])


def other_core(array, tp_count):
    return lax.ppermute(array, "tp", [(j, j ^ 1) for j in range(tp_count)])


def layer(stream, norm_gain, gate_rows, up_rows, down_rows, chosen, affinity):
    ep_count = lax.axis_size("ep")
    tp_count = lax.axis_size("tp")
    block, _ = stream.shape
    slots = 4 * block // ep_count
    ep_index = lax.axis_index("ep").astype(jnp.int32)
    place = jnp.stack([ep_index // SIDE, ep_index % SIDE])
    bounds = (jnp.arange(ep_count, dtype=jnp.int32) * tp_count + lax.axis_index("tp")) * block
    low, high, own = prepare(stream, norm_gain, (gate_rows, up_rows, down_rows))
    left, right = over_plane(low, 0, 1), over_plane(low, 0, -1)
    down, up = over_plane(high, 1, 0), over_plane(high, -1, 0)
    ahead, behind = along_z(own, 1, tp_count), along_z(own, -1, tp_count)
    rows_there, weights = windows(bounds, chosen, affinity, block, slots)
    rows_here = lax.all_to_all(rows_there, "ep", split_axis=0, concat_axis=0, tiled=True)
    mid = block // 2
    lows = [low, left, over_plane(left[:mid], 0, 1), over_plane(right[mid:], 0, -1), right]
    highs = [high, down, over_plane(down[:mid], 1, 0), over_plane(up[mid:], -1, 0), up]
    ahead2, behind2 = along_z(ahead, 1, tp_count), along_z(behind, -1, tp_count)
    picked = pick(place, rows_here, lows, highs)
    arrived_low, arrived_high = [picked[0]] + [None] * (SIDE - 1), [picked[SIDE]] + [None] * (SIDE - 1)
    for d in (1, 3, 2):
        arrived_low[d] = over_plane(picked[d], d, 0)
        arrived_high[d] = over_plane(picked[SIDE + d], 0, d)
    cut = own.shape[1] // 2
    far = [
        along_z(ahead2[:, :cut], 2, tp_count),
        along_z(behind2[:, cut:], -2, tp_count),
        along_z(ahead2, 1, tp_count),
        along_z(behind2, -1, tp_count),
    ]
    early = stack([own, ahead, behind, ahead2, behind2])
    late = stack(far)
    pieces = [early, late, other_core(early, tp_count), other_core(late, tp_count)]
    projections = assemble(pieces)
    made, back = {}, {}
    for number in range(len(STEPS)):
        finished = expert(number, place, weights, projections, arrived_low, arrived_high, made)
        for (half, by), piece in finished.items():
            if by == 0:
                back[half, by] = piece
            elif half == "low":
                back[half, by] = over_plane(piece, -by, 0)
            else:
                back[half, by] = over_plane(piece, 0, -by)
    lows, highs = [back["low", d] for d in range(SIDE)], [back["high", d] for d in range(SIDE)]
    sums = relay(place, rows_here, lows, highs, block)
    lows, highs = [sums[0]], [sums[SIDE]]
    for t in (1, 3, 2):
        lows.append(over_plane(sums[t], 0, -t))
        highs.append(over_plane(sums[SIDE + t], -t, 0))
    return add(lows, highs)


def solution(mesh):
    return jax.shard_map(
        layer,
        mesh=mesh,
        in_specs=(
            P(("ep", "tp"), None),
            P(),
            P("ep", "tp", None),
            P("ep", "tp", None),
            P("ep", "tp", None),
            P("ep", None),
            P("ep", None),
        ),
        out_specs=P(("ep", "tp"), None),
        check_vma=False,
    )
```

```python
import functools

import jax
import jax.numpy as jnp
from jax import lax
from jax.experimental import pallas as pl
from jax.experimental.pallas import tpu as pltpu
from jax.sharding import PartitionSpec as P

epsilon = 1e-06
SIDE = 4
SMEM = pl.BlockSpec(memory_space=pltpu.SMEM)
VMEM = pl.BlockSpec(memory_space=pltpu.VMEM)


def wrap(value):
    return lax.rem(value + SIDE, SIDE)


def windows_kernel(block, slots, bounds_ref, list_ref, affinity_ref, rows_ref, weights_ref):
    listed = list_ref[...]
    lines = listed.shape[0]
    lane = lax.broadcasted_iota(jnp.int32, (1, slots), 1)

    def cut(j, carry):
        y, x = j // SIDE, lax.rem(j, SIDE)
        bound = bounds_ref[j]
        start = jnp.sum((listed < bound).astype(jnp.int32))
        line, shift = start // slots, start % slots
        first = jnp.minimum(line, lines - 1)
        second = jnp.minimum(line + 1, lines - 1)
        back = lax.rem(slots - shift, slots)

        def window(ref):
            low = pltpu.roll(ref[pl.ds(first, 1), :], back, 1)
            high = pltpu.roll(ref[pl.ds(second, 1), :], back, 1)
            return jnp.where(lane < slots - shift, low, high)

        rows = window(list_ref) - bound
        rows = jnp.where((rows >= 0) & (rows < block), rows, -1)
        for t in range(SIDE):
            rows_ref[y * SIDE + wrap(x + t - SIDE), t : t + 1, :] = rows
            rows_ref[wrap(y + t - SIDE) * SIDE + x, SIDE + t : SIDE + t + 1, :] = rows
        weights_ref[pl.ds(j, 1), :] = window(affinity_ref)
        return carry

    lax.fori_loop(0, weights_ref.shape[0], cut, 0, unroll=4)


def windows(bounds, listed, affinity, block, slots):
    count = bounds.shape[0]
    return pl.pallas_call(
        functools.partial(windows_kernel, block, slots),
        in_specs=[SMEM, VMEM, VMEM],
        out_shape=(
            jax.ShapeDtypeStruct((count, 2 * SIDE, slots), jnp.int32),
            jax.ShapeDtypeStruct((count, slots), jnp.float32),
        ),
        cost_estimate=pl.CostEstimate(flops=8_000_000, bytes_accessed=150_000, transcendentals=0),
        name="windows",
    )(bounds, listed.reshape(-1, slots), affinity.reshape(-1, slots))


def prepare_kernel(stream_ref, gain_ref, gate_ref, up_ref, down_ref, low_ref, high_ref, piece_ref):
    values = stream_ref[...].astype(jnp.float32)
    inverse = lax.rsqrt(jnp.mean(values * values, axis=-1, keepdims=True) + epsilon)
    normed = (values * inverse * gain_ref[...]).astype(jnp.bfloat16)
    half = low_ref.shape[1]
    low_ref[...] = normed[:, :half]
    high_ref[...] = normed[:, half:]

    @pl.when(pl.program_id(0) == 0)
    def _():
        piece_ref[0:1] = gate_ref[...]
        piece_ref[1:2] = up_ref[...]
        piece_ref[2:3] = down_ref[...]


def prepare(stream, norm_gain, parts):
    rows, features = stream.shape
    step, half = rows // 2, features // 2
    part = pl.BlockSpec(parts[0].shape, lambda i: (0, 0, 0))
    piece = (3, *parts[0].shape[1:])
    return pl.pallas_call(
        prepare_kernel,
        grid=(2,),
        in_specs=[
            pl.BlockSpec((step, features), lambda i: (i, 0)),
            pl.BlockSpec((1, features), lambda i: (0, 0)),
            part,
            part,
            part,
        ],
        out_specs=(
            pl.BlockSpec((step, half), lambda i: (i, 0)),
            pl.BlockSpec((step, half), lambda i: (i, 0)),
            pl.BlockSpec(piece, lambda i: (0, 0, 0)),
        ),
        out_shape=(
            jax.ShapeDtypeStruct((rows, half), jnp.bfloat16),
            jax.ShapeDtypeStruct((rows, half), jnp.bfloat16),
            jax.ShapeDtypeStruct(piece, jnp.bfloat16),
        ),
        cost_estimate=pl.CostEstimate(flops=3_000_000, bytes_accessed=3 << 20, transcendentals=512),
        name="prepare",
    )(stream, norm_gain.reshape(1, features), *parts)


def pick_kernel(along_y, place_ref, rows_ref, own_ref, after_ref, top_ref, bottom_ref, before_ref, *refs):
    outs = refs[:SIDE]
    across_ref, chosen_ref = refs[SIDE:]
    y, x = place_ref[0], place_ref[1]
    tokens, half = own_ref.shape
    slots = rows_ref.shape[2]
    across_ref[: tokens // 2, :] = top_ref[...]
    across_ref[tokens // 2 :, :] = bottom_ref[...]
    token = lax.broadcasted_iota(jnp.int32, (slots, tokens), 1).astype(jnp.float32)
    for d in range(SIDE):
        e = wrap(y + d) * SIDE + x if along_y else y * SIDE + wrap(x + d)
        column = rows_ref[e].astype(jnp.float32).T
        for t in range(SIDE):
            k = t if along_y else SIDE + t
            chosen_ref[t, d * slots : (d + 1) * slots, :] = jnp.where(column[:, k : k + 1] == token, 1.0, 0.0).astype(
                jnp.bfloat16
            )
    step = half // 2

    def work(i, carry):
        at = pl.ds(pl.multiple_of(i * step, step), step)
        for t, source in enumerate((own_ref, after_ref, across_ref, before_ref)):
            rows = jnp.dot(chosen_ref[t], source[:, at], preferred_element_type=jnp.float32).astype(jnp.bfloat16)
            for d in range(SIDE):
                outs[d][t * slots : (t + 1) * slots, at] = rows[d * slots : (d + 1) * slots, :]
        return carry

    lax.fori_loop(0, 2, work, 0)


def pick(along_y, place, rows, sources):
    tokens, half = sources[0].shape
    slots = rows.shape[2]
    return pl.pallas_call(
        functools.partial(pick_kernel, along_y),
        in_specs=[SMEM] + [VMEM] * 6,
        out_shape=[jax.ShapeDtypeStruct((SIDE * slots, half), jnp.bfloat16)] * SIDE,
        scratch_shapes=[
            pltpu.VMEM((tokens, half), jnp.bfloat16),
            pltpu.VMEM((SIDE, SIDE * slots, tokens), jnp.bfloat16),
        ],
        cost_estimate=pl.CostEstimate(
            flops=2 * SIDE * SIDE * slots * tokens * half, bytes_accessed=4 << 20, transcendentals=0
        ),
        compiler_params=pltpu.CompilerParams(vmem_limit_bytes=14 << 20),
        name="pick_y" if along_y else "pick_x",
    )(place, rows, *sources)


def stack_kernel(*refs):
    out_ref, at = refs[-1], 0
    for piece in refs[:-1]:
        width = piece.shape[1]
        out_ref[:, at : at + width, :] = piece[...]
        at += width


def stack(pieces):
    return pl.pallas_call(
        stack_kernel,
        in_specs=[VMEM] * len(pieces),
        out_shape=jax.ShapeDtypeStruct(
            (3, sum(piece.shape[1] for piece in pieces), pieces[0].shape[2]), jnp.bfloat16
        ),
        cost_estimate=pl.CostEstimate(flops=1_000_000, bytes_accessed=4 << 20, transcendentals=0),
        compiler_params=pltpu.CompilerParams(vmem_limit_bytes=8 << 20),
    )(*pieces)


def assemble_kernel(*refs):
    pieces, outs = refs[:-3], refs[-3:]
    step = 64
    at = 0
    for piece in pieces:
        width = piece.shape[1]
        for j, out in enumerate(outs):

            def move(i, carry, piece=piece, out=out, j=j, at=at):
                rows = pl.multiple_of(i * step, step)
                out[pl.ds(at + rows, step), :] = piece[j, pl.ds(rows, step), :]
                return carry

            lax.fori_loop(0, width // step, move, 0)
        at += width


def assemble(pieces):
    shape = jax.ShapeDtypeStruct((sum(piece.shape[1] for piece in pieces), pieces[0].shape[2]), jnp.bfloat16)
    return pl.pallas_call(
        assemble_kernel,
        in_specs=[VMEM] * len(pieces),
        out_shape=[shape] * 3,
        cost_estimate=pl.CostEstimate(flops=1_000_000, bytes_accessed=12 << 20, transcendentals=0),
        compiler_params=pltpu.CompilerParams(vmem_limit_bytes=16 << 20),
        name="assemble",
    )(*pieces)


STEPS = (
    ((2, 0), (2, 1), (2, 2), (2, 3), (0, 2), (1, 2), (3, 2), (1, 1)),
    ((1, 0), (1, 3), (0, 1), (3, 1), (3, 0), (3, 3), (0, 3), (0, 0)),
)
FINISHED = (
    (("low", 2), ("high", 2)),
    (("low", 1), ("high", 1), ("low", 3), ("high", 3), ("low", 0), ("high", 0)),
)


def members(piece):
    half, fixed = piece
    return [(fixed, k) if half == "low" else (k, fixed) for k in range(SIDE)]


def expert_kernel(number, names, place_ref, weights_ref, gate_ref, up_ref, down_ref, *refs):
    inputs_ref, result_ref, columns_ref = refs[-3:]
    ref = dict(zip(names, refs))
    blocks = STEPS[number]
    y, x = place_ref[0], place_ref[1]
    slots, half = weights_ref.shape[1], ref["in", "low", blocks[0][0]].shape[1]
    for k, (a, b) in enumerate(blocks):
        at = slice(k * slots, (k + 1) * slots)
        inputs_ref[at, :half] = ref["in", "low", a][b * slots : (b + 1) * slots, :]
        inputs_ref[at, half:] = ref["in", "high", b][a * slots : (a + 1) * slots, :]
        line = weights_ref[pl.ds(wrap(y - a) * SIDE + wrap(x - b), 1), :]
        columns_ref[at, :] = jnp.broadcast_to(line, (slots, slots)).T
    last = (((1,), (1,)), ((), ()))
    units = gate_ref.shape[0]
    width, rows = units // 4, SIDE * slots

    def work(i, carry):
        at = pl.ds(pl.multiple_of(i * rows, rows), rows)
        inputs = inputs_ref[at, :]
        hidden = []
        for f in range(0, units, width):
            gate_sum = lax.dot_general(inputs, gate_ref[f : f + width, :], last, preferred_element_type=jnp.float32)
            up_sum = lax.dot_general(inputs, up_ref[f : f + width, :], last, preferred_element_type=jnp.float32)
            hidden.append((gate_sum / (1.0 + jnp.exp(-gate_sum)) * up_sum).astype(jnp.bfloat16))
        result = jnp.dot(jnp.concatenate(hidden, 1), down_ref[...], preferred_element_type=jnp.float32)
        result_ref[at, :] = (result * columns_ref[at, :][:, :1]).astype(jnp.bfloat16)
        return carry

    lax.fori_loop(0, len(blocks) // SIDE, work, 0)

    def part(block, which):
        if block in blocks:
            k = blocks.index(block)
            cut = slice(0, half) if which == "low" else slice(half, 2 * half)
            return result_ref[k * slots : (k + 1) * slots, cut]
        step = next(n for n in range(number) if block in STEPS[n])
        k = STEPS[step].index(block)
        return ref["made", which, step][k * slots : (k + 1) * slots, :]

    for name in names:
        if name[0] == "out":
            for k, block in enumerate(members(name[1:])):
                ref[name][k * slots : (k + 1) * slots, :] = part(block, name[1])
        if name == ("made", name[1], number):
            for k, block in enumerate(blocks):
                ref[name][k * slots : (k + 1) * slots, :] = part(block, name[1])


def expert(number, place, weights, projections, low, high, made):
    slots, half = weights.shape[1], low[0].shape[1]
    features, units = 2 * half, projections[0].shape[0]
    piece_rows = SIDE * slots
    blocks = STEPS[number]
    total = len(blocks) * slots
    inputs = {("in", "low", a): low[a] for a, _ in blocks}
    inputs.update({("in", "high", b): high[b] for _, b in blocks})
    for piece in FINISHED[number]:
        for block in members(piece):
            step = next(n for n in range(len(STEPS)) if block in STEPS[n])
            if step < number:
                inputs["made", piece[0], step] = made[piece[0], step]
    outs = [("out", *piece) for piece in FINISHED[number]]
    for which in ("low", "high"):
        later = [
            piece
            for done in FINISHED[number + 1 :]
            for piece in done
            if piece[0] == which and any(block in blocks for block in members(piece))
        ]
        if later:
            outs.append(("made", which, number))
    shapes = [(piece_rows if name[0] == "out" else total, half) for name in outs]
    results = pl.pallas_call(
        functools.partial(expert_kernel, number, [*inputs, *outs]),
        in_specs=[SMEM] + [VMEM] * (4 + len(inputs)),
        out_shape=[jax.ShapeDtypeStruct(shape, jnp.bfloat16) for shape in shapes],
        scratch_shapes=[
            pltpu.VMEM((total, features), jnp.bfloat16),
            pltpu.VMEM((total, features), jnp.bfloat16),
            pltpu.VMEM((total, slots), jnp.float32),
        ],
        cost_estimate=pl.CostEstimate(
            flops=6 * total * units * features, bytes_accessed=4 * total * features, transcendentals=2 * total * units
        ),
        compiler_params=pltpu.CompilerParams(vmem_limit_bytes=28 << 20),
    )(place, weights, *projections, *inputs.values())
    results = dict(zip(outs, results))
    made.update({name[1:]: array for name, array in results.items() if name[0] == "made"})
    return {name[1:]: array for name, array in results.items() if name[0] == "out"}


def relay_kernel(place_ref, rows_ref, *refs):
    y, x = place_ref[0], place_ref[1]
    tokens, slots = refs[-1].shape[0], rows_ref.shape[2]
    step = tokens // 2
    token = lax.broadcasted_iota(jnp.int32, (step, slots), 0)
    for along_y in (True, False):
        first = 0 if along_y else SIDE
        pieces, outs = refs[first : first + SIDE], refs[first + 2 * SIDE : first + 3 * SIDE]
        lists = [rows_ref[wrap(y + d) * SIDE + x if along_y else y * SIDE + wrap(x + d)] for d in range(SIDE)]

        def work(i, carry, first=first, pieces=pieces, outs=outs, lists=lists):
            for t in range(SIDE):
                k = first + t
                chosen = jnp.concatenate(
                    [
                        jnp.where(token + i * step == rows[k : k + 1, :], 1.0, 0.0).astype(jnp.bfloat16)
                        for rows in lists
                    ],
                    1,
                )
                rows = jnp.concatenate([piece[t * slots : (t + 1) * slots, :] for piece in pieces])
                total = jnp.dot(chosen, rows, preferred_element_type=jnp.float32)
                outs[t][pl.ds(pl.multiple_of(i * step, step), step), :] = total.astype(jnp.bfloat16)
            return carry

        lax.fori_loop(0, 2, work, 0)


def relay(place, rows, lows, highs, tokens):
    total, half = lows[0].shape
    return pl.pallas_call(
        relay_kernel,
        in_specs=[SMEM] + [VMEM] * (1 + len(lows) + len(highs)),
        out_shape=[jax.ShapeDtypeStruct((tokens, half), jnp.bfloat16)] * (2 * SIDE),
        cost_estimate=pl.CostEstimate(
            flops=4 * SIDE * total * tokens * half, bytes_accessed=8 << 20, transcendentals=0
        ),
        compiler_params=pltpu.CompilerParams(vmem_limit_bytes=16 << 20),
        name="relay",
    )(place, rows, *lows, *highs)


def add_kernel(*refs):
    out_ref = refs[-1]
    half = refs[0].shape[1]
    for n, parts in enumerate((refs[:SIDE], refs[SIDE : 2 * SIDE])):
        total = parts[0][...].astype(jnp.float32)
        for part in parts[1:]:
            total = total + part[...].astype(jnp.float32)
        out_ref[:, n * half : (n + 1) * half] = total.astype(jnp.bfloat16)


def add(lows, highs):
    tokens, half = lows[0].shape
    step = tokens // 4
    return pl.pallas_call(
        add_kernel,
        grid=(4,),
        in_specs=[pl.BlockSpec((step, half), lambda i: (i, 0))] * (2 * SIDE),
        out_specs=pl.BlockSpec((step, 2 * half), lambda i: (i, 0)),
        out_shape=jax.ShapeDtypeStruct((tokens, 2 * half), jnp.bfloat16),
        cost_estimate=pl.CostEstimate(flops=4_000_000, bytes_accessed=5 << 20, transcendentals=0),
        compiler_params=pltpu.CompilerParams(vmem_limit_bytes=12 << 20),
        name="add",
    )(*lows, *highs)


def over_plane(array, by_y, by_x):
    places = [(y, x) for y in range(SIDE) for x in range(SIDE)]
    return lax.ppermute(
        array, "ep", [(y * SIDE + x, (y + by_y) % SIDE * SIDE + (x + by_x) % SIDE) for y, x in places]
    )


def along_z(array, by, tp_count):
    chips = tp_count // 2
    pairs = [(z, c, (z + (-by if c else by)) % chips) for z in range(chips) for c in range(2)]
    return lax.ppermute(array, "tp", [(z * 2 + c, to * 2 + c) for z, c, to in pairs])


def other_core(array, tp_count):
    return lax.ppermute(array, "tp", [(j, j ^ 1) for j in range(tp_count)])


def layer(stream, norm_gain, gate_rows, up_rows, down_rows, chosen, affinity):
    ep_count = lax.axis_size("ep")
    tp_count = lax.axis_size("tp")
    block, _ = stream.shape
    slots = 4 * block // ep_count
    ep_index = lax.axis_index("ep").astype(jnp.int32)
    place = jnp.stack([ep_index // SIDE, ep_index % SIDE])
    bounds = (jnp.arange(ep_count, dtype=jnp.int32) * tp_count + lax.axis_index("tp")) * block
    low, high, own = prepare(stream, norm_gain, (gate_rows, up_rows, down_rows))
    left, right = over_plane(low, 0, 1), over_plane(low, 0, -1)
    down, up = over_plane(high, 1, 0), over_plane(high, -1, 0)
    both = stack([own, other_core(own, tp_count)])
    next1 = along_z(both, 1, tp_count)
    rows_there, weights = windows(bounds, chosen, affinity, block, slots)
    rows_here = lax.all_to_all(rows_there, "ep", split_axis=0, concat_axis=0, tiled=True)
    mid = block // 2
    lows = [low, left, over_plane(left[:mid], 0, 1), over_plane(right[mid:], 0, -1), right]
    highs = [high, down, over_plane(down[:mid], 1, 0), over_plane(up[mid:], -1, 0), up]
    next2 = along_z(next1, 1, tp_count)
    picked_low = pick(True, place, rows_here, lows)
    arrived_low = [picked_low[0]] + [over_plane(picked_low[d], d, 0) for d in range(1, SIDE)]
    next3 = along_z(next2, 1, tp_count)
    picked_high = pick(False, place, rows_here, highs)
    arrived_high = [picked_high[0]] + [over_plane(picked_high[d], 0, d) for d in range(1, SIDE)]
    across = along_z(next2[:, : own.shape[1]], 2, tp_count)
    held = [next1, next2, next3, across]
    pieces = [both, *held, *(other_core(piece, tp_count) for piece in held)]
    projections = assemble(pieces)
    made, back = {}, {}
    for number in range(len(STEPS)):
        finished = expert(number, place, weights, projections, arrived_low, arrived_high, made)
        for (half, by), piece in finished.items():
            if by == 0:
                back[half, by] = piece
            elif half == "low":
                back[half, by] = over_plane(piece, -by, 0)
            else:
                back[half, by] = over_plane(piece, 0, -by)
    lows, highs = [back["low", d] for d in range(SIDE)], [back["high", d] for d in range(SIDE)]
    sums = relay(place, rows_here, lows, highs, block)
    lows, highs = [sums[0]], [sums[SIDE]]
    for t in (1, 3, 2):
        lows.append(over_plane(sums[t], 0, -t))
        highs.append(over_plane(sums[SIDE + t], -t, 0))
    return add(lows, highs)


def solution(mesh):
    return jax.shard_map(
        layer,
        mesh=mesh,
        in_specs=(
            P(("ep", "tp"), None),
            P(),
            P("ep", "tp", None),
            P("ep", "tp", None),
            P("ep", "tp", None),
            P("ep", None),
            P("ep", None),
        ),
        out_specs=P(("ep", "tp"), None),
        check_vma=False,
    )
```

```python
import functools

import jax
import jax.numpy as jnp
from jax import lax
from jax.experimental import pallas as pl
from jax.experimental.pallas import tpu as pltpu
from jax.sharding import PartitionSpec as P

epsilon = 1e-06
SIDE = 4
SMEM = pl.BlockSpec(memory_space=pltpu.SMEM)
VMEM = pl.BlockSpec(memory_space=pltpu.VMEM)


def wrap(value):
    return lax.rem(value + SIDE, SIDE)


def windows_kernel(block, slots, bounds_ref, list_ref, affinity_ref, rows_ref, weights_ref):
    listed = list_ref[...]
    lines = listed.shape[0]
    lane = lax.broadcasted_iota(jnp.int32, (1, slots), 1)

    def cut(j, carry):
        y, x = j // SIDE, lax.rem(j, SIDE)
        bound = bounds_ref[j]
        start = jnp.sum((listed < bound).astype(jnp.int32))
        line, shift = start // slots, start % slots
        first = jnp.minimum(line, lines - 1)
        second = jnp.minimum(line + 1, lines - 1)
        back = lax.rem(slots - shift, slots)

        def window(ref):
            low = pltpu.roll(ref[pl.ds(first, 1), :], back, 1)
            high = pltpu.roll(ref[pl.ds(second, 1), :], back, 1)
            return jnp.where(lane < slots - shift, low, high)

        rows = window(list_ref) - bound
        rows = jnp.where((rows >= 0) & (rows < block), rows, -1)
        for t in range(SIDE):
            rows_ref[y * SIDE + wrap(x + t - SIDE), t : t + 1, :] = rows
            rows_ref[wrap(y + t - SIDE) * SIDE + x, SIDE + t : SIDE + t + 1, :] = rows
        weights_ref[pl.ds(j, 1), :] = window(affinity_ref)
        return carry

    lax.fori_loop(0, weights_ref.shape[0], cut, 0, unroll=4)


def windows(bounds, listed, affinity, block, slots):
    count = bounds.shape[0]
    return pl.pallas_call(
        functools.partial(windows_kernel, block, slots),
        in_specs=[SMEM, VMEM, VMEM],
        out_shape=(
            jax.ShapeDtypeStruct((count, 2 * SIDE, slots), jnp.int32),
            jax.ShapeDtypeStruct((count, slots), jnp.float32),
        ),
        cost_estimate=pl.CostEstimate(flops=8_000_000, bytes_accessed=150_000, transcendentals=0),
        name="windows",
    )(bounds, listed.reshape(-1, slots), affinity.reshape(-1, slots))


def prepare_kernel(stream_ref, gain_ref, gate_ref, up_ref, down_ref, low_ref, high_ref, piece_ref):
    values = stream_ref[...].astype(jnp.float32)
    inverse = lax.rsqrt(jnp.mean(values * values, axis=-1, keepdims=True) + epsilon)
    normed = (values * inverse * gain_ref[...]).astype(jnp.bfloat16)
    half = low_ref.shape[1]
    low_ref[...] = normed[:, :half]
    high_ref[...] = normed[:, half:]

    @pl.when(pl.program_id(0) == 0)
    def _():
        piece_ref[0:1] = gate_ref[...]
        piece_ref[1:2] = up_ref[...]
        piece_ref[2:3] = down_ref[...]


def prepare(stream, norm_gain, parts):
    rows, features = stream.shape
    step, half = rows // 2, features // 2
    part = pl.BlockSpec(parts[0].shape, lambda i: (0, 0, 0))
    piece = (3, *parts[0].shape[1:])
    return pl.pallas_call(
        prepare_kernel,
        grid=(2,),
        in_specs=[
            pl.BlockSpec((step, features), lambda i: (i, 0)),
            pl.BlockSpec((1, features), lambda i: (0, 0)),
            part,
            part,
            part,
        ],
        out_specs=(
            pl.BlockSpec((step, half), lambda i: (i, 0)),
            pl.BlockSpec((step, half), lambda i: (i, 0)),
            pl.BlockSpec(piece, lambda i: (0, 0, 0)),
        ),
        out_shape=(
            jax.ShapeDtypeStruct((rows, half), jnp.bfloat16),
            jax.ShapeDtypeStruct((rows, half), jnp.bfloat16),
            jax.ShapeDtypeStruct(piece, jnp.bfloat16),
        ),
        cost_estimate=pl.CostEstimate(flops=3_000_000, bytes_accessed=3 << 20, transcendentals=512),
        name="prepare",
    )(stream, norm_gain.reshape(1, features), *parts)


def pick_kernel(along_y, place_ref, rows_ref, own_ref, after_ref, top_ref, bottom_ref, before_ref, *refs):
    outs = refs[:SIDE]
    across_ref, chosen_ref = refs[SIDE:]
    y, x = place_ref[0], place_ref[1]
    tokens, half = own_ref.shape
    slots = rows_ref.shape[2]
    across_ref[: tokens // 2, :] = top_ref[...]
    across_ref[tokens // 2 :, :] = bottom_ref[...]
    token = lax.broadcasted_iota(jnp.int32, (slots, tokens), 1).astype(jnp.float32)
    for d in range(SIDE):
        e = wrap(y + d) * SIDE + x if along_y else y * SIDE + wrap(x + d)
        column = rows_ref[e].astype(jnp.float32).T
        for t in range(SIDE):
            k = t if along_y else SIDE + t
            chosen_ref[t, d * slots : (d + 1) * slots, :] = jnp.where(column[:, k : k + 1] == token, 1.0, 0.0).astype(
                jnp.bfloat16
            )
    step = half // 2

    def work(i, carry):
        at = pl.ds(pl.multiple_of(i * step, step), step)
        for t, source in enumerate((own_ref, after_ref, across_ref, before_ref)):
            rows = jnp.dot(chosen_ref[t], source[:, at], preferred_element_type=jnp.float32).astype(jnp.bfloat16)
            for d in range(SIDE):
                outs[d][t * slots : (t + 1) * slots, at] = rows[d * slots : (d + 1) * slots, :]
        return carry

    lax.fori_loop(0, 2, work, 0)


def pick(along_y, place, rows, sources):
    tokens, half = sources[0].shape
    slots = rows.shape[2]
    return pl.pallas_call(
        functools.partial(pick_kernel, along_y),
        in_specs=[SMEM] + [VMEM] * 6,
        out_shape=[jax.ShapeDtypeStruct((SIDE * slots, half), jnp.bfloat16)] * SIDE,
        scratch_shapes=[
            pltpu.VMEM((tokens, half), jnp.bfloat16),
            pltpu.VMEM((SIDE, SIDE * slots, tokens), jnp.bfloat16),
        ],
        cost_estimate=pl.CostEstimate(
            flops=2 * SIDE * SIDE * slots * tokens * half, bytes_accessed=4 << 20, transcendentals=0
        ),
        compiler_params=pltpu.CompilerParams(vmem_limit_bytes=14 << 20),
        name="pick_y" if along_y else "pick_x",
    )(place, rows, *sources)


def stack_kernel(*refs):
    out_ref, at = refs[-1], 0
    for piece in refs[:-1]:
        width = piece.shape[1]
        out_ref[:, at : at + width, :] = piece[...]
        at += width


def stack(pieces):
    return pl.pallas_call(
        stack_kernel,
        in_specs=[VMEM] * len(pieces),
        out_shape=jax.ShapeDtypeStruct(
            (3, sum(piece.shape[1] for piece in pieces), pieces[0].shape[2]), jnp.bfloat16
        ),
        cost_estimate=pl.CostEstimate(flops=1_000_000, bytes_accessed=4 << 20, transcendentals=0),
        compiler_params=pltpu.CompilerParams(vmem_limit_bytes=8 << 20),
    )(*pieces)


def assemble_kernel(*refs):
    pieces, outs = refs[:-3], refs[-3:]
    step = 64
    at = 0
    for piece in pieces:
        width = piece.shape[1]
        for j, out in enumerate(outs):

            def move(i, carry, piece=piece, out=out, j=j, at=at):
                rows = pl.multiple_of(i * step, step)
                out[pl.ds(at + rows, step), :] = piece[j, pl.ds(rows, step), :]
                return carry

            lax.fori_loop(0, width // step, move, 0)
        at += width


def assemble(pieces):
    shape = jax.ShapeDtypeStruct((sum(piece.shape[1] for piece in pieces), pieces[0].shape[2]), jnp.bfloat16)
    return pl.pallas_call(
        assemble_kernel,
        in_specs=[VMEM] * len(pieces),
        out_shape=[shape] * 3,
        cost_estimate=pl.CostEstimate(flops=1_000_000, bytes_accessed=12 << 20, transcendentals=0),
        compiler_params=pltpu.CompilerParams(vmem_limit_bytes=16 << 20),
        name="assemble",
    )(*pieces)


STEPS = (
    ((2, 0), (2, 1), (2, 2), (2, 3), (0, 2), (1, 2), (3, 2), (1, 1)),
    ((1, 0), (1, 3), (0, 1), (3, 1), (3, 0), (3, 3), (0, 3), (0, 0)),
)
FINISHED = (
    (("low", 2), ("high", 2)),
    (("low", 1), ("high", 1), ("low", 3), ("high", 3), ("low", 0), ("high", 0)),
)


def members(piece):
    half, fixed = piece
    return [(fixed, k) if half == "low" else (k, fixed) for k in range(SIDE)]


def expert_kernel(number, names, place_ref, weights_ref, gate_ref, up_ref, down_ref, *refs):
    inputs_ref, result_ref, columns_ref = refs[-3:]
    ref = dict(zip(names, refs))
    blocks = STEPS[number]
    y, x = place_ref[0], place_ref[1]
    slots, half = weights_ref.shape[1], ref["in", "low", blocks[0][0]].shape[1]
    for k, (a, b) in enumerate(blocks):
        at = slice(k * slots, (k + 1) * slots)
        inputs_ref[at, :half] = ref["in", "low", a][b * slots : (b + 1) * slots, :]
        inputs_ref[at, half:] = ref["in", "high", b][a * slots : (a + 1) * slots, :]
        line = weights_ref[pl.ds(wrap(y - a) * SIDE + wrap(x - b), 1), :]
        columns_ref[at, :] = jnp.broadcast_to(line, (slots, slots)).T
    last = (((1,), (1,)), ((), ()))
    units = gate_ref.shape[0]
    width, rows = units // 4, SIDE * slots

    def work(i, carry):
        at = pl.ds(pl.multiple_of(i * rows, rows), rows)
        inputs = inputs_ref[at, :]
        hidden = []
        for f in range(0, units, width):
            gate_sum = lax.dot_general(inputs, gate_ref[f : f + width, :], last, preferred_element_type=jnp.float32)
            up_sum = lax.dot_general(inputs, up_ref[f : f + width, :], last, preferred_element_type=jnp.float32)
            hidden.append((gate_sum / (1.0 + jnp.exp(-gate_sum)) * up_sum).astype(jnp.bfloat16))
        result = jnp.dot(jnp.concatenate(hidden, 1), down_ref[...], preferred_element_type=jnp.float32)
        result_ref[at, :] = (result * columns_ref[at, :][:, :1]).astype(jnp.bfloat16)
        return carry

    lax.fori_loop(0, len(blocks) // SIDE, work, 0)

    def part(block, which):
        if block in blocks:
            k = blocks.index(block)
            cut = slice(0, half) if which == "low" else slice(half, 2 * half)
            return result_ref[k * slots : (k + 1) * slots, cut]
        step = next(n for n in range(number) if block in STEPS[n])
        k = STEPS[step].index(block)
        return ref["made", which, step][k * slots : (k + 1) * slots, :]

    for name in names:
        if name[0] == "out":
            for k, block in enumerate(members(name[1:])):
                ref[name][k * slots : (k + 1) * slots, :] = part(block, name[1])
        if name == ("made", name[1], number):
            for k, block in enumerate(blocks):
                ref[name][k * slots : (k + 1) * slots, :] = part(block, name[1])


def expert(number, place, weights, projections, low, high, made):
    slots, half = weights.shape[1], low[0].shape[1]
    features, units = 2 * half, projections[0].shape[0]
    piece_rows = SIDE * slots
    blocks = STEPS[number]
    total = len(blocks) * slots
    inputs = {("in", "low", a): low[a] for a, _ in blocks}
    inputs.update({("in", "high", b): high[b] for _, b in blocks})
    for piece in FINISHED[number]:
        for block in members(piece):
            step = next(n for n in range(len(STEPS)) if block in STEPS[n])
            if step < number:
                inputs["made", piece[0], step] = made[piece[0], step]
    outs = [("out", *piece) for piece in FINISHED[number]]
    for which in ("low", "high"):
        later = [
            piece
            for done in FINISHED[number + 1 :]
            for piece in done
            if piece[0] == which and any(block in blocks for block in members(piece))
        ]
        if later:
            outs.append(("made", which, number))
    shapes = [(piece_rows if name[0] == "out" else total, half) for name in outs]
    results = pl.pallas_call(
        functools.partial(expert_kernel, number, [*inputs, *outs]),
        in_specs=[SMEM] + [VMEM] * (4 + len(inputs)),
        out_shape=[jax.ShapeDtypeStruct(shape, jnp.bfloat16) for shape in shapes],
        scratch_shapes=[
            pltpu.VMEM((total, features), jnp.bfloat16),
            pltpu.VMEM((total, features), jnp.bfloat16),
            pltpu.VMEM((total, slots), jnp.float32),
        ],
        cost_estimate=pl.CostEstimate(
            flops=6 * total * units * features, bytes_accessed=4 * total * features, transcendentals=2 * total * units
        ),
        compiler_params=pltpu.CompilerParams(vmem_limit_bytes=28 << 20),
    )(place, weights, *projections, *inputs.values())
    results = dict(zip(outs, results))
    made.update({name[1:]: array for name, array in results.items() if name[0] == "made"})
    return {name[1:]: array for name, array in results.items() if name[0] == "out"}


def relay_kernel(place_ref, rows_ref, *refs):
    y, x = place_ref[0], place_ref[1]
    tokens, slots = refs[-1].shape[0], rows_ref.shape[2]
    step = tokens // 2
    token = lax.broadcasted_iota(jnp.int32, (step, slots), 0)
    for along_y in (True, False):
        first = 0 if along_y else SIDE
        pieces, outs = refs[first : first + SIDE], refs[first + 2 * SIDE : first + 3 * SIDE]
        lists = [rows_ref[wrap(y + d) * SIDE + x if along_y else y * SIDE + wrap(x + d)] for d in range(SIDE)]

        def work(i, carry, first=first, pieces=pieces, outs=outs, lists=lists):
            for t in range(SIDE):
                k = first + t
                chosen = jnp.concatenate(
                    [
                        jnp.where(token + i * step == rows[k : k + 1, :], 1.0, 0.0).astype(jnp.bfloat16)
                        for rows in lists
                    ],
                    1,
                )
                rows = jnp.concatenate([piece[t * slots : (t + 1) * slots, :] for piece in pieces])
                total = jnp.dot(chosen, rows, preferred_element_type=jnp.float32)
                outs[t][pl.ds(pl.multiple_of(i * step, step), step), :] = total.astype(jnp.bfloat16)
            return carry

        lax.fori_loop(0, 2, work, 0)


def relay(place, rows, lows, highs, tokens):
    total, half = lows[0].shape
    return pl.pallas_call(
        relay_kernel,
        in_specs=[SMEM] + [VMEM] * (1 + len(lows) + len(highs)),
        out_shape=[jax.ShapeDtypeStruct((tokens, half), jnp.bfloat16)] * (2 * SIDE),
        cost_estimate=pl.CostEstimate(
            flops=4 * SIDE * total * tokens * half, bytes_accessed=8 << 20, transcendentals=0
        ),
        compiler_params=pltpu.CompilerParams(vmem_limit_bytes=16 << 20),
        name="relay",
    )(place, rows, *lows, *highs)


def add_kernel(*refs):
    out_ref = refs[-1]
    half = refs[0].shape[1]
    for n, parts in enumerate((refs[:SIDE], refs[SIDE : 2 * SIDE])):
        total = parts[0][...].astype(jnp.float32)
        for part in parts[1:]:
            total = total + part[...].astype(jnp.float32)
        out_ref[:, n * half : (n + 1) * half] = total.astype(jnp.bfloat16)


def add(lows, highs):
    tokens, half = lows[0].shape
    step = tokens // 4
    return pl.pallas_call(
        add_kernel,
        grid=(4,),
        in_specs=[pl.BlockSpec((step, half), lambda i: (i, 0))] * (2 * SIDE),
        out_specs=pl.BlockSpec((step, 2 * half), lambda i: (i, 0)),
        out_shape=jax.ShapeDtypeStruct((tokens, 2 * half), jnp.bfloat16),
        cost_estimate=pl.CostEstimate(flops=4_000_000, bytes_accessed=5 << 20, transcendentals=0),
        compiler_params=pltpu.CompilerParams(vmem_limit_bytes=12 << 20),
        name="add",
    )(*lows, *highs)


def over_plane(array, by_y, by_x):
    places = [(y, x) for y in range(SIDE) for x in range(SIDE)]
    return lax.ppermute(
        array, "ep", [(y * SIDE + x, (y + by_y) % SIDE * SIDE + (x + by_x) % SIDE) for y, x in places]
    )


def along_z(array, by, tp_count):
    chips = tp_count // 2
    pairs = [(z, c, (z + (-by if c else by)) % chips) for z in range(chips) for c in range(2)]
    return lax.ppermute(array, "tp", [(z * 2 + c, to * 2 + c) for z, c, to in pairs])


def other_core(array, tp_count):
    return lax.ppermute(array, "tp", [(j, j ^ 1) for j in range(tp_count)])


def layer(stream, norm_gain, gate_rows, up_rows, down_rows, chosen, affinity):
    ep_count = lax.axis_size("ep")
    tp_count = lax.axis_size("tp")
    block, _ = stream.shape
    slots = 4 * block // ep_count
    ep_index = lax.axis_index("ep").astype(jnp.int32)
    place = jnp.stack([ep_index // SIDE, ep_index % SIDE])
    bounds = (jnp.arange(ep_count, dtype=jnp.int32) * tp_count + lax.axis_index("tp")) * block
    low, high, own = prepare(stream, norm_gain, (gate_rows, up_rows, down_rows))
    left, right = over_plane(low, 0, 1), over_plane(low, 0, -1)
    down, up = over_plane(high, 1, 0), over_plane(high, -1, 0)
    both = stack([own, other_core(own, tp_count)])
    next1 = along_z(both, 1, tp_count)
    rows_there, weights = windows(bounds, chosen, affinity, block, slots)
    rows_here = lax.all_to_all(rows_there, "ep", split_axis=0, concat_axis=0, tiled=True)
    mid = block // 2
    lows = [low, left, over_plane(left[:mid], 0, 1), over_plane(right[mid:], 0, -1), right]
    highs = [high, down, over_plane(down[:mid], 1, 0), over_plane(up[mid:], -1, 0), up]
    next2 = along_z(next1, 1, tp_count)
    picked_low = pick(True, place, rows_here, lows)
    arrived_low = [picked_low[0]] + [None] * (SIDE - 1)
    arrived_low[1], arrived_low[3] = over_plane(picked_low[1], 1, 0), over_plane(picked_low[3], 3, 0)
    arrived_low[2] = over_plane(picked_low[2], 2, 0)
    next3 = along_z(next2, 1, tp_count)
    picked_high = pick(False, place, rows_here, highs)
    arrived_high = [picked_high[0]] + [None] * (SIDE - 1)
    arrived_high[1], arrived_high[3] = over_plane(picked_high[1], 0, 1), over_plane(picked_high[3], 0, 3)
    arrived_high[2] = over_plane(picked_high[2], 0, 2)
    across = along_z(next2[:, : own.shape[1]], 2, tp_count)
    held = [next1, next2, next3, across]
    pieces = [both, *held, *(other_core(piece, tp_count) for piece in held)]
    projections = assemble(pieces)
    made, back = {}, {}
    for number in range(len(STEPS)):
        finished = expert(number, place, weights, projections, arrived_low, arrived_high, made)
        for (half, by), piece in finished.items():
            if by == 0:
                back[half, by] = piece
            elif half == "low":
                back[half, by] = over_plane(piece, -by, 0)
            else:
                back[half, by] = over_plane(piece, 0, -by)
    lows, highs = [back["low", d] for d in range(SIDE)], [back["high", d] for d in range(SIDE)]
    sums = relay(place, rows_here, lows, highs, block)
    lows, highs = [sums[0]], [sums[SIDE]]
    for t in (1, 3, 2):
        lows.append(over_plane(sums[t], 0, -t))
        highs.append(over_plane(sums[SIDE + t], -t, 0))
    return add(lows, highs)


def solution(mesh):
    return jax.shard_map(
        layer,
        mesh=mesh,
        in_specs=(
            P(("ep", "tp"), None),
            P(),
            P("ep", "tp", None),
            P("ep", "tp", None),
            P("ep", "tp", None),
            P("ep", None),
            P("ep", None),
        ),
        out_specs=P(("ep", "tp"), None),
        check_vma=False,
    )
```

```python
import functools

import jax
import jax.numpy as jnp
from jax import lax
from jax.experimental import pallas as pl
from jax.experimental.pallas import tpu as pltpu
from jax.sharding import PartitionSpec as P

epsilon = 1e-06
SIDE = 4
SMEM = pl.BlockSpec(memory_space=pltpu.SMEM)
VMEM = pl.BlockSpec(memory_space=pltpu.VMEM)


def wrap(value):
    return lax.rem(value + SIDE, SIDE)


def windows_kernel(block, slots, bounds_ref, list_ref, affinity_ref, rows_ref, weights_ref):
    listed = list_ref[...]
    lines = listed.shape[0]
    lane = lax.broadcasted_iota(jnp.int32, (1, slots), 1)

    def cut(j, carry):
        y, x = j // SIDE, lax.rem(j, SIDE)
        bound = bounds_ref[j]
        start = jnp.sum((listed < bound).astype(jnp.int32))
        line, shift = start // slots, start % slots
        first = jnp.minimum(line, lines - 1)
        second = jnp.minimum(line + 1, lines - 1)
        back = lax.rem(slots - shift, slots)

        def window(ref):
            low = pltpu.roll(ref[pl.ds(first, 1), :], back, 1)
            high = pltpu.roll(ref[pl.ds(second, 1), :], back, 1)
            return jnp.where(lane < slots - shift, low, high)

        rows = window(list_ref) - bound
        rows = jnp.where((rows >= 0) & (rows < block), rows, -1)
        for t in range(SIDE):
            rows_ref[y * SIDE + wrap(x + t - SIDE), t : t + 1, :] = rows
            rows_ref[wrap(y + t - SIDE) * SIDE + x, SIDE + t : SIDE + t + 1, :] = rows
        weights_ref[pl.ds(j, 1), :] = window(affinity_ref)
        return carry

    lax.fori_loop(0, weights_ref.shape[0], cut, 0, unroll=4)


def windows(bounds, listed, affinity, block, slots):
    count = bounds.shape[0]
    return pl.pallas_call(
        functools.partial(windows_kernel, block, slots),
        in_specs=[SMEM, VMEM, VMEM],
        out_shape=(
            jax.ShapeDtypeStruct((count, 2 * SIDE, slots), jnp.int32),
            jax.ShapeDtypeStruct((count, slots), jnp.float32),
        ),
        cost_estimate=pl.CostEstimate(flops=8_000_000, bytes_accessed=150_000, transcendentals=0),
        name="windows",
    )(bounds, listed.reshape(-1, slots), affinity.reshape(-1, slots))


def prepare_kernel(stream_ref, gain_ref, gate_ref, up_ref, down_ref, low_ref, high_ref, piece_ref):
    values = stream_ref[...].astype(jnp.float32)
    inverse = lax.rsqrt(jnp.mean(values * values, axis=-1, keepdims=True) + epsilon)
    normed = (values * inverse * gain_ref[...]).astype(jnp.bfloat16)
    half = low_ref.shape[1]
    low_ref[...] = normed[:, :half]
    high_ref[...] = normed[:, half:]

    @pl.when(pl.program_id(0) == 0)
    def _():
        piece_ref[0:1] = gate_ref[...]
        piece_ref[1:2] = up_ref[...]
        piece_ref[2:3] = down_ref[...]


def prepare(stream, norm_gain, parts):
    rows, features = stream.shape
    step, half = rows // 2, features // 2
    part = pl.BlockSpec(parts[0].shape, lambda i: (0, 0, 0))
    piece = (3, *parts[0].shape[1:])
    return pl.pallas_call(
        prepare_kernel,
        grid=(2,),
        in_specs=[
            pl.BlockSpec((step, features), lambda i: (i, 0)),
            pl.BlockSpec((1, features), lambda i: (0, 0)),
            part,
            part,
            part,
        ],
        out_specs=(
            pl.BlockSpec((step, half), lambda i: (i, 0)),
            pl.BlockSpec((step, half), lambda i: (i, 0)),
            pl.BlockSpec(piece, lambda i: (0, 0, 0)),
        ),
        out_shape=(
            jax.ShapeDtypeStruct((rows, half), jnp.bfloat16),
            jax.ShapeDtypeStruct((rows, half), jnp.bfloat16),
            jax.ShapeDtypeStruct(piece, jnp.bfloat16),
        ),
        cost_estimate=pl.CostEstimate(flops=3_000_000, bytes_accessed=3 << 20, transcendentals=512),
        name="prepare",
    )(stream, norm_gain.reshape(1, features), *parts)


def pick_kernel(along_y, place_ref, rows_ref, own_ref, after_ref, top_ref, bottom_ref, before_ref, *refs):
    outs = refs[:SIDE]
    across_ref, chosen_ref = refs[SIDE:]
    y, x = place_ref[0], place_ref[1]
    tokens, half = own_ref.shape
    slots = rows_ref.shape[2]
    across_ref[: tokens // 2, :] = top_ref[...]
    across_ref[tokens // 2 :, :] = bottom_ref[...]
    token = lax.broadcasted_iota(jnp.int32, (slots, tokens), 1).astype(jnp.float32)
    for d in range(SIDE):
        e = wrap(y + d) * SIDE + x if along_y else y * SIDE + wrap(x + d)
        column = rows_ref[e].astype(jnp.float32).T
        for t in range(SIDE):
            k = t if along_y else SIDE + t
            chosen_ref[t, d * slots : (d + 1) * slots, :] = jnp.where(column[:, k : k + 1] == token, 1.0, 0.0).astype(
                jnp.bfloat16
            )
    step = half // 2

    def work(i, carry):
        at = pl.ds(pl.multiple_of(i * step, step), step)
        for t, source in enumerate((own_ref, after_ref, across_ref, before_ref)):
            rows = jnp.dot(chosen_ref[t], source[:, at], preferred_element_type=jnp.float32).astype(jnp.bfloat16)
            for d in range(SIDE):
                outs[d][t * slots : (t + 1) * slots, at] = rows[d * slots : (d + 1) * slots, :]
        return carry

    lax.fori_loop(0, 2, work, 0)


def pick(along_y, place, rows, sources):
    tokens, half = sources[0].shape
    slots = rows.shape[2]
    return pl.pallas_call(
        functools.partial(pick_kernel, along_y),
        in_specs=[SMEM] + [VMEM] * 6,
        out_shape=[jax.ShapeDtypeStruct((SIDE * slots, half), jnp.bfloat16)] * SIDE,
        scratch_shapes=[
            pltpu.VMEM((tokens, half), jnp.bfloat16),
            pltpu.VMEM((SIDE, SIDE * slots, tokens), jnp.bfloat16),
        ],
        cost_estimate=pl.CostEstimate(
            flops=2 * SIDE * SIDE * slots * tokens * half, bytes_accessed=4 << 20, transcendentals=0
        ),
        compiler_params=pltpu.CompilerParams(vmem_limit_bytes=14 << 20),
        name="pick_y" if along_y else "pick_x",
    )(place, rows, *sources)


def stack_kernel(*refs):
    out_ref, at = refs[-1], 0
    for piece in refs[:-1]:
        width = piece.shape[1]
        out_ref[:, at : at + width, :] = piece[...]
        at += width


def stack(pieces):
    return pl.pallas_call(
        stack_kernel,
        in_specs=[VMEM] * len(pieces),
        out_shape=jax.ShapeDtypeStruct(
            (3, sum(piece.shape[1] for piece in pieces), pieces[0].shape[2]), jnp.bfloat16
        ),
        cost_estimate=pl.CostEstimate(flops=1_000_000, bytes_accessed=4 << 20, transcendentals=0),
        compiler_params=pltpu.CompilerParams(vmem_limit_bytes=8 << 20),
    )(*pieces)


def assemble_kernel(*refs):
    pieces, outs = refs[:-3], refs[-3:]
    step = 64
    at = 0
    for piece in pieces:
        width = piece.shape[1]
        for j, out in enumerate(outs):

            def move(i, carry, piece=piece, out=out, j=j, at=at):
                rows = pl.multiple_of(i * step, step)
                out[pl.ds(at + rows, step), :] = piece[j, pl.ds(rows, step), :]
                return carry

            lax.fori_loop(0, width // step, move, 0)
        at += width


def assemble(pieces):
    shape = jax.ShapeDtypeStruct((sum(piece.shape[1] for piece in pieces), pieces[0].shape[2]), jnp.bfloat16)
    return pl.pallas_call(
        assemble_kernel,
        in_specs=[VMEM] * len(pieces),
        out_shape=[shape] * 3,
        cost_estimate=pl.CostEstimate(flops=1_000_000, bytes_accessed=12 << 20, transcendentals=0),
        compiler_params=pltpu.CompilerParams(vmem_limit_bytes=16 << 20),
        name="assemble",
    )(*pieces)


STEPS = (
    ((0, 0), (1, 0), (2, 0), (3, 0)),
    ((2, 1), (2, 2), (2, 3), (0, 2), (1, 2), (3, 2)),
    ((0, 1), (1, 1), (3, 1), (0, 3), (1, 3), (3, 3)),
)
FINISHED = (
    (("high", 0),),
    (("low", 2), ("high", 2)),
    (("low", 1), ("high", 1), ("low", 3), ("high", 3), ("low", 0)),
)


def members(piece):
    half, fixed = piece
    return [(fixed, k) if half == "low" else (k, fixed) for k in range(SIDE)]


def expert_kernel(number, names, place_ref, weights_ref, gate_ref, up_ref, down_ref, *refs):
    inputs_ref, result_ref, columns_ref = refs[-3:]
    ref = dict(zip(names, refs))
    blocks = STEPS[number]
    y, x = place_ref[0], place_ref[1]
    slots, half = weights_ref.shape[1], ref["in", "low", blocks[0][0]].shape[1]
    for k, (a, b) in enumerate(blocks):
        at = slice(k * slots, (k + 1) * slots)
        inputs_ref[at, :half] = ref["in", "low", a][b * slots : (b + 1) * slots, :]
        inputs_ref[at, half:] = ref["in", "high", b][a * slots : (a + 1) * slots, :]
        line = weights_ref[pl.ds(wrap(y - a) * SIDE + wrap(x - b), 1), :]
        columns_ref[at, :] = jnp.broadcast_to(line, (slots, slots)).T
    last = (((1,), (1,)), ((), ()))
    units = gate_ref.shape[0]
    width, rows = units // 4, 2 * slots

    def work(i, carry):
        at = pl.ds(pl.multiple_of(i * rows, rows), rows)
        inputs = inputs_ref[at, :]
        hidden = []
        for f in range(0, units, width):
            gate_sum = lax.dot_general(inputs, gate_ref[f : f + width, :], last, preferred_element_type=jnp.float32)
            up_sum = lax.dot_general(inputs, up_ref[f : f + width, :], last, preferred_element_type=jnp.float32)
            hidden.append((gate_sum / (1.0 + jnp.exp(-gate_sum)) * up_sum).astype(jnp.bfloat16))
        result = jnp.dot(jnp.concatenate(hidden, 1), down_ref[...], preferred_element_type=jnp.float32)
        result_ref[at, :] = (result * columns_ref[at, :][:, :1]).astype(jnp.bfloat16)
        return carry

    lax.fori_loop(0, len(blocks) // 2, work, 0)

    def part(block, which):
        if block in blocks:
            k = blocks.index(block)
            cut = slice(0, half) if which == "low" else slice(half, 2 * half)
            return result_ref[k * slots : (k + 1) * slots, cut]
        step = next(n for n in range(number) if block in STEPS[n])
        k = STEPS[step].index(block)
        return ref["made", which, step][k * slots : (k + 1) * slots, :]

    for name in names:
        if name[0] == "out":
            for k, block in enumerate(members(name[1:])):
                ref[name][k * slots : (k + 1) * slots, :] = part(block, name[1])
        if name == ("made", name[1], number):
            for k, block in enumerate(blocks):
                ref[name][k * slots : (k + 1) * slots, :] = part(block, name[1])


def expert(number, place, weights, projections, low, high, made):
    slots, half = weights.shape[1], low[0].shape[1]
    features, units = 2 * half, projections[0].shape[0]
    piece_rows = SIDE * slots
    blocks = STEPS[number]
    total = len(blocks) * slots
    inputs = {("in", "low", a): low[a] for a, _ in blocks}
    inputs.update({("in", "high", b): high[b] for _, b in blocks})
    for piece in FINISHED[number]:
        for block in members(piece):
            step = next(n for n in range(len(STEPS)) if block in STEPS[n])
            if step < number:
                inputs["made", piece[0], step] = made[piece[0], step]
    outs = [("out", *piece) for piece in FINISHED[number]]
    for which in ("low", "high"):
        later = [
            piece
            for done in FINISHED[number + 1 :]
            for piece in done
            if piece[0] == which and any(block in blocks for block in members(piece))
        ]
        if later:
            outs.append(("made", which, number))
    shapes = [(piece_rows if name[0] == "out" else total, half) for name in outs]
    results = pl.pallas_call(
        functools.partial(expert_kernel, number, [*inputs, *outs]),
        in_specs=[SMEM] + [VMEM] * (4 + len(inputs)),
        out_shape=[jax.ShapeDtypeStruct(shape, jnp.bfloat16) for shape in shapes],
        scratch_shapes=[
            pltpu.VMEM((total, features), jnp.bfloat16),
            pltpu.VMEM((total, features), jnp.bfloat16),
            pltpu.VMEM((total, slots), jnp.float32),
        ],
        cost_estimate=pl.CostEstimate(
            flops=6 * total * units * features, bytes_accessed=4 * total * features, transcendentals=2 * total * units
        ),
        compiler_params=pltpu.CompilerParams(vmem_limit_bytes=28 << 20),
    )(place, weights, *projections, *inputs.values())
    results = dict(zip(outs, results))
    made.update({name[1:]: array for name, array in results.items() if name[0] == "made"})
    return {name[1:]: array for name, array in results.items() if name[0] == "out"}


def relay_kernel(place_ref, rows_ref, *refs):
    y, x = place_ref[0], place_ref[1]
    tokens, slots = refs[-1].shape[0], rows_ref.shape[2]
    step = tokens // 2
    token = lax.broadcasted_iota(jnp.int32, (step, slots), 0)
    for along_y in (True, False):
        first = 0 if along_y else SIDE
        pieces, outs = refs[first : first + SIDE], refs[first + 2 * SIDE : first + 3 * SIDE]
        lists = [rows_ref[wrap(y + d) * SIDE + x if along_y else y * SIDE + wrap(x + d)] for d in range(SIDE)]

        def work(i, carry, first=first, pieces=pieces, outs=outs, lists=lists):
            for t in range(SIDE):
                k = first + t
                chosen = jnp.concatenate(
                    [
                        jnp.where(token + i * step == rows[k : k + 1, :], 1.0, 0.0).astype(jnp.bfloat16)
                        for rows in lists
                    ],
                    1,
                )
                rows = jnp.concatenate([piece[t * slots : (t + 1) * slots, :] for piece in pieces])
                total = jnp.dot(chosen, rows, preferred_element_type=jnp.float32)
                outs[t][pl.ds(pl.multiple_of(i * step, step), step), :] = total.astype(jnp.bfloat16)
            return carry

        lax.fori_loop(0, 2, work, 0)


def relay(place, rows, lows, highs, tokens):
    total, half = lows[0].shape
    return pl.pallas_call(
        relay_kernel,
        in_specs=[SMEM] + [VMEM] * (1 + len(lows) + len(highs)),
        out_shape=[jax.ShapeDtypeStruct((tokens, half), jnp.bfloat16)] * (2 * SIDE),
        cost_estimate=pl.CostEstimate(
            flops=4 * SIDE * total * tokens * half, bytes_accessed=8 << 20, transcendentals=0
        ),
        compiler_params=pltpu.CompilerParams(vmem_limit_bytes=16 << 20),
        name="relay",
    )(place, rows, *lows, *highs)


def add_kernel(*refs):
    out_ref = refs[-1]
    half = refs[0].shape[1]
    for n, parts in enumerate((refs[:SIDE], refs[SIDE : 2 * SIDE])):
        total = parts[0][...].astype(jnp.float32)
        for part in parts[1:]:
            total = total + part[...].astype(jnp.float32)
        out_ref[:, n * half : (n + 1) * half] = total.astype(jnp.bfloat16)


def add(lows, highs):
    tokens, half = lows[0].shape
    step = tokens // 4
    return pl.pallas_call(
        add_kernel,
        grid=(4,),
        in_specs=[pl.BlockSpec((step, half), lambda i: (i, 0))] * (2 * SIDE),
        out_specs=pl.BlockSpec((step, 2 * half), lambda i: (i, 0)),
        out_shape=jax.ShapeDtypeStruct((tokens, 2 * half), jnp.bfloat16),
        cost_estimate=pl.CostEstimate(flops=4_000_000, bytes_accessed=5 << 20, transcendentals=0),
        compiler_params=pltpu.CompilerParams(vmem_limit_bytes=12 << 20),
        name="add",
    )(*lows, *highs)


def over_plane(array, by_y, by_x):
    places = [(y, x) for y in range(SIDE) for x in range(SIDE)]
    return lax.ppermute(
        array, "ep", [(y * SIDE + x, (y + by_y) % SIDE * SIDE + (x + by_x) % SIDE) for y, x in places]
    )


def along_z(array, by, tp_count):
    chips = tp_count // 2
    pairs = [(z, c, (z + (-by if c else by)) % chips) for z in range(chips) for c in range(2)]
    return lax.ppermute(array, "tp", [(z * 2 + c, to * 2 + c) for z, c, to in pairs])


def other_core(array, tp_count):
    return lax.ppermute(array, "tp", [(j, j ^ 1) for j in range(tp_count)])


def layer(stream, norm_gain, gate_rows, up_rows, down_rows, chosen, affinity):
    ep_count = lax.axis_size("ep")
    tp_count = lax.axis_size("tp")
    block, _ = stream.shape
    slots = 4 * block // ep_count
    ep_index = lax.axis_index("ep").astype(jnp.int32)
    place = jnp.stack([ep_index // SIDE, ep_index % SIDE])
    bounds = (jnp.arange(ep_count, dtype=jnp.int32) * tp_count + lax.axis_index("tp")) * block
    low, high, own = prepare(stream, norm_gain, (gate_rows, up_rows, down_rows))
    left, right = over_plane(low, 0, 1), over_plane(low, 0, -1)
    down, up = over_plane(high, 1, 0), over_plane(high, -1, 0)
    both = stack([own, other_core(own, tp_count)])
    next1 = along_z(both, 1, tp_count)
    rows_there, weights = windows(bounds, chosen, affinity, block, slots)
    rows_here = lax.all_to_all(rows_there, "ep", split_axis=0, concat_axis=0, tiled=True)
    mid = block // 2
    lows = [low, left, over_plane(left[:mid], 0, 1), over_plane(right[mid:], 0, -1), right]
    highs = [high, down, over_plane(down[:mid], 1, 0), over_plane(up[mid:], -1, 0), up]
    next2 = along_z(next1, 1, tp_count)
    picked_low = pick(True, place, rows_here, lows)
    arrived_low = [picked_low[0]] + [None] * (SIDE - 1)
    arrived_low[1], arrived_low[3] = over_plane(picked_low[1], 1, 0), over_plane(picked_low[3], 3, 0)
    arrived_low[2] = over_plane(picked_low[2], 2, 0)
    next3 = along_z(next2, 1, tp_count)
    picked_high = pick(False, place, rows_here, highs)
    arrived_high = [picked_high[0]] + [None] * (SIDE - 1)
    arrived_high[1], arrived_high[3] = over_plane(picked_high[1], 0, 1), over_plane(picked_high[3], 0, 3)
    arrived_high[2] = over_plane(picked_high[2], 0, 2)
    across = along_z(next2[:, : own.shape[1]], 2, tp_count)
    held = [next1, next2, next3, across]
    pieces = [both, *held, *(other_core(piece, tp_count) for piece in held)]
    projections = assemble(pieces)
    made, back = {}, {}
    for number in range(len(STEPS)):
        finished = expert(number, place, weights, projections, arrived_low, arrived_high, made)
        for (half, by), piece in finished.items():
            if by == 0:
                back[half, by] = piece
            elif half == "low":
                back[half, by] = over_plane(piece, -by, 0)
            else:
                back[half, by] = over_plane(piece, 0, -by)
    lows, highs = [back["low", d] for d in range(SIDE)], [back["high", d] for d in range(SIDE)]
    sums = relay(place, rows_here, lows, highs, block)
    lows, highs = [sums[0]], [sums[SIDE]]
    for t in (1, 3, 2):
        lows.append(over_plane(sums[t], 0, -t))
        highs.append(over_plane(sums[SIDE + t], -t, 0))
    return add(lows, highs)


def solution(mesh):
    return jax.shard_map(
        layer,
        mesh=mesh,
        in_specs=(
            P(("ep", "tp"), None),
            P(),
            P("ep", "tp", None),
            P("ep", "tp", None),
            P("ep", "tp", None),
            P("ep", None),
            P("ep", None),
        ),
        out_specs=P(("ep", "tp"), None),
        check_vma=False,
    )
```

```python
import functools

import jax
import jax.numpy as jnp
from jax import lax
from jax.experimental import pallas as pl
from jax.experimental.pallas import tpu as pltpu
from jax.sharding import PartitionSpec as P

epsilon = 1e-06
SIDE = 4
SMEM = pl.BlockSpec(memory_space=pltpu.SMEM)
VMEM = pl.BlockSpec(memory_space=pltpu.VMEM)


def wrap(value):
    return lax.rem(value + SIDE, SIDE)


def windows_kernel(block, slots, bounds_ref, list_ref, affinity_ref, rows_ref, weights_ref):
    listed = list_ref[...]
    lines = listed.shape[0]
    lane = lax.broadcasted_iota(jnp.int32, (1, slots), 1)

    def cut(j, carry):
        y, x = j // SIDE, lax.rem(j, SIDE)
        bound = bounds_ref[j]
        start = jnp.sum((listed < bound).astype(jnp.int32))
        line, shift = start // slots, start % slots
        first = jnp.minimum(line, lines - 1)
        second = jnp.minimum(line + 1, lines - 1)
        back = lax.rem(slots - shift, slots)

        def window(ref):
            low = pltpu.roll(ref[pl.ds(first, 1), :], back, 1)
            high = pltpu.roll(ref[pl.ds(second, 1), :], back, 1)
            return jnp.where(lane < slots - shift, low, high)

        rows = window(list_ref) - bound
        rows = jnp.where((rows >= 0) & (rows < block), rows, -1)
        for t in range(SIDE):
            rows_ref[y * SIDE + wrap(x + t - SIDE), t : t + 1, :] = rows
            rows_ref[wrap(y + t - SIDE) * SIDE + x, SIDE + t : SIDE + t + 1, :] = rows
        weights_ref[pl.ds(j, 1), :] = window(affinity_ref)
        return carry

    lax.fori_loop(0, weights_ref.shape[0], cut, 0, unroll=4)


def windows(bounds, listed, affinity, block, slots):
    count = bounds.shape[0]
    return pl.pallas_call(
        functools.partial(windows_kernel, block, slots),
        in_specs=[SMEM, VMEM, VMEM],
        out_shape=(
            jax.ShapeDtypeStruct((count, 2 * SIDE, slots), jnp.int32),
            jax.ShapeDtypeStruct((count, slots), jnp.float32),
        ),
        cost_estimate=pl.CostEstimate(flops=8_000_000, bytes_accessed=150_000, transcendentals=0),
        name="windows",
    )(bounds, listed.reshape(-1, slots), affinity.reshape(-1, slots))


def prepare_kernel(stream_ref, gain_ref, gate_ref, up_ref, down_ref, *refs):
    values = stream_ref[...].astype(jnp.float32)
    inverse = lax.rsqrt(jnp.mean(values * values, axis=-1, keepdims=True) + epsilon)
    normed = (values * inverse * gain_ref[...]).astype(jnp.bfloat16)
    high_ref, piece_ref = refs[2:]
    half = high_ref.shape[1]
    high_ref[...] = normed[:, half:]
    for part in range(2):

        @pl.when(pl.program_id(0) == part)
        def _():
            refs[part][...] = normed[:, :half]

    @pl.when(pl.program_id(0) == 0)
    def _():
        piece_ref[0:1] = gate_ref[...]
        piece_ref[1:2] = up_ref[...]
        piece_ref[2:3] = down_ref[...]


def prepare(stream, norm_gain, parts):
    rows, features = stream.shape
    step, half = rows // 2, features // 2
    part = pl.BlockSpec(parts[0].shape, lambda i: (0, 0, 0))
    piece = (3, *parts[0].shape[1:])
    return pl.pallas_call(
        prepare_kernel,
        grid=(2,),
        in_specs=[
            pl.BlockSpec((step, features), lambda i: (i, 0)),
            pl.BlockSpec((1, features), lambda i: (0, 0)),
            part,
            part,
            part,
        ],
        out_specs=(
            *[pl.BlockSpec((step, half), lambda i: (0, 0))] * 2,
            pl.BlockSpec((step, half), lambda i: (i, 0)),
            pl.BlockSpec(piece, lambda i: (0, 0, 0)),
        ),
        out_shape=(
            *[jax.ShapeDtypeStruct((step, half), jnp.bfloat16)] * 2,
            jax.ShapeDtypeStruct((rows, half), jnp.bfloat16),
            jax.ShapeDtypeStruct(piece, jnp.bfloat16),
        ),
        cost_estimate=pl.CostEstimate(flops=3_000_000, bytes_accessed=3 << 20, transcendentals=512),
        name="prepare",
    )(stream, norm_gain.reshape(1, features), *parts)


def pick_kernel(along_y, place_ref, rows_ref, *refs):
    sources, outs = refs[: -SIDE - 2], refs[-SIDE - 2 : -2]
    sources_ref, chosen_ref = refs[-2:]
    y, x = place_ref[0], place_ref[1]
    _, tokens, half = sources_ref.shape
    slots = rows_ref.shape[2]
    at = 0
    for source in sources:
        sources_ref[at // tokens, at % tokens : at % tokens + source.shape[0], :] = source[...]
        at += source.shape[0]
    token = lax.broadcasted_iota(jnp.int32, (slots, tokens), 1).astype(jnp.float32)
    for d in range(SIDE):
        e = wrap(y + d) * SIDE + x if along_y else y * SIDE + wrap(x + d)
        column = rows_ref[e].astype(jnp.float32).T
        for t in range(SIDE):
            k = t if along_y else SIDE + t
            chosen_ref[t, d * slots : (d + 1) * slots, :] = jnp.where(column[:, k : k + 1] == token, 1.0, 0.0).astype(
                jnp.bfloat16
            )
    step = half // 2

    def work(i, carry):
        at = pl.ds(pl.multiple_of(i * step, step), step)
        for t in range(SIDE):
            rows = jnp.dot(chosen_ref[t], sources_ref[t, :, at], preferred_element_type=jnp.float32).astype(jnp.bfloat16)
            for d in range(SIDE):
                outs[d][t * slots : (t + 1) * slots, at] = rows[d * slots : (d + 1) * slots, :]
        return carry

    lax.fori_loop(0, 2, work, 0)


def pick(along_y, place, rows, sources):
    tokens, half = sum(source.shape[0] for source in sources) // SIDE, sources[0].shape[1]
    slots = rows.shape[2]
    return pl.pallas_call(
        functools.partial(pick_kernel, along_y),
        in_specs=[SMEM] + [VMEM] * (1 + len(sources)),
        out_shape=[jax.ShapeDtypeStruct((SIDE * slots, half), jnp.bfloat16)] * SIDE,
        scratch_shapes=[
            pltpu.VMEM((SIDE, tokens, half), jnp.bfloat16),
            pltpu.VMEM((SIDE, SIDE * slots, tokens), jnp.bfloat16),
        ],
        cost_estimate=pl.CostEstimate(
            flops=2 * SIDE * SIDE * slots * tokens * half, bytes_accessed=4 << 20, transcendentals=0
        ),
        compiler_params=pltpu.CompilerParams(vmem_limit_bytes=14 << 20),
        name="pick_y" if along_y else "pick_x",
    )(place, rows, *sources)


def stack_kernel(*refs):
    out_ref, at = refs[-1], 0
    for piece in refs[:-1]:
        width = piece.shape[1]
        out_ref[:, at : at + width, :] = piece[...]
        at += width


def stack(pieces):
    return pl.pallas_call(
        stack_kernel,
        in_specs=[VMEM] * len(pieces),
        out_shape=jax.ShapeDtypeStruct(
            (3, sum(piece.shape[1] for piece in pieces), pieces[0].shape[2]), jnp.bfloat16
        ),
        cost_estimate=pl.CostEstimate(flops=1_000_000, bytes_accessed=4 << 20, transcendentals=0),
        compiler_params=pltpu.CompilerParams(vmem_limit_bytes=8 << 20),
    )(*pieces)


def assemble_kernel(*refs):
    pieces, outs = refs[:-3], refs[-3:]
    step = 64
    at = 0
    for piece in pieces:
        width = piece.shape[1]
        for j, out in enumerate(outs):

            def move(i, carry, piece=piece, out=out, j=j, at=at):
                rows = pl.multiple_of(i * step, step)
                out[pl.ds(at + rows, step), :] = piece[j, pl.ds(rows, step), :]
                return carry

            lax.fori_loop(0, width // step, move, 0)
        at += width


def assemble(pieces):
    shape = jax.ShapeDtypeStruct((sum(piece.shape[1] for piece in pieces), pieces[0].shape[2]), jnp.bfloat16)
    return pl.pallas_call(
        assemble_kernel,
        in_specs=[VMEM] * len(pieces),
        out_shape=[shape] * 3,
        cost_estimate=pl.CostEstimate(flops=1_000_000, bytes_accessed=12 << 20, transcendentals=0),
        compiler_params=pltpu.CompilerParams(vmem_limit_bytes=16 << 20),
        name="assemble",
    )(*pieces)


STEPS = (
    ((0, 0), (1, 0), (2, 0), (3, 0)),
    ((2, 1), (2, 2), (2, 3), (0, 2), (1, 2), (3, 2)),
    ((0, 1), (1, 1), (3, 1), (0, 3), (1, 3), (3, 3)),
)
FINISHED = (
    (("high", 0),),
    (("low", 2), ("high", 2)),
    (("low", 1), ("high", 1), ("low", 3), ("high", 3), ("low", 0)),
)


def members(piece):
    half, fixed = piece
    return [(fixed, k) if half == "low" else (k, fixed) for k in range(SIDE)]


def expert_kernel(number, names, place_ref, weights_ref, gate_ref, up_ref, down_ref, *refs):
    inputs_ref, result_ref, columns_ref = refs[-3:]
    ref = dict(zip(names, refs))
    blocks = STEPS[number]
    y, x = place_ref[0], place_ref[1]
    slots, half = weights_ref.shape[1], ref["in", "low", blocks[0][0]].shape[1]
    for k, (a, b) in enumerate(blocks):
        at = slice(k * slots, (k + 1) * slots)
        inputs_ref[at, :half] = ref["in", "low", a][b * slots : (b + 1) * slots, :]
        inputs_ref[at, half:] = ref["in", "high", b][a * slots : (a + 1) * slots, :]
        line = weights_ref[pl.ds(wrap(y - a) * SIDE + wrap(x - b), 1), :]
        columns_ref[at, :] = jnp.broadcast_to(line, (slots, slots)).T
    last = (((1,), (1,)), ((), ()))
    units = gate_ref.shape[0]
    width, rows = units // 4, 2 * slots

    def work(i, carry):
        at = pl.ds(pl.multiple_of(i * rows, rows), rows)
        inputs = inputs_ref[at, :]
        hidden = []
        for f in range(0, units, width):
            gate_sum = lax.dot_general(inputs, gate_ref[f : f + width, :], last, preferred_element_type=jnp.float32)
            up_sum = lax.dot_general(inputs, up_ref[f : f + width, :], last, preferred_element_type=jnp.float32)
            hidden.append((gate_sum / (1.0 + jnp.exp(-gate_sum)) * up_sum).astype(jnp.bfloat16))
        result = jnp.dot(jnp.concatenate(hidden, 1), down_ref[...], preferred_element_type=jnp.float32)
        result_ref[at, :] = (result * columns_ref[at, :][:, :1]).astype(jnp.bfloat16)
        return carry

    lax.fori_loop(0, len(blocks) // 2, work, 0)

    def part(block, which):
        if block in blocks:
            k = blocks.index(block)
            cut = slice(0, half) if which == "low" else slice(half, 2 * half)
            return result_ref[k * slots : (k + 1) * slots, cut]
        step = next(n for n in range(number) if block in STEPS[n])
        k = STEPS[step].index(block)
        return ref["made", which, step][k * slots : (k + 1) * slots, :]

    for name in names:
        if name[0] == "out":
            for k, block in enumerate(members(name[1:])):
                ref[name][k * slots : (k + 1) * slots, :] = part(block, name[1])
        if name == ("made", name[1], number):
            for k, block in enumerate(blocks):
                ref[name][k * slots : (k + 1) * slots, :] = part(block, name[1])


def expert(number, place, weights, projections, low, high, made):
    slots, half = weights.shape[1], low[0].shape[1]
    features, units = 2 * half, projections[0].shape[0]
    piece_rows = SIDE * slots
    blocks = STEPS[number]
    total = len(blocks) * slots
    inputs = {("in", "low", a): low[a] for a, _ in blocks}
    inputs.update({("in", "high", b): high[b] for _, b in blocks})
    for piece in FINISHED[number]:
        for block in members(piece):
            step = next(n for n in range(len(STEPS)) if block in STEPS[n])
            if step < number:
                inputs["made", piece[0], step] = made[piece[0], step]
    outs = [("out", *piece) for piece in FINISHED[number]]
    for which in ("low", "high"):
        later = [
            piece
            for done in FINISHED[number + 1 :]
            for piece in done
            if piece[0] == which and any(block in blocks for block in members(piece))
        ]
        if later:
            outs.append(("made", which, number))
    shapes = [(piece_rows if name[0] == "out" else total, half) for name in outs]
    results = pl.pallas_call(
        functools.partial(expert_kernel, number, [*inputs, *outs]),
        in_specs=[SMEM] + [VMEM] * (4 + len(inputs)),
        out_shape=[jax.ShapeDtypeStruct(shape, jnp.bfloat16) for shape in shapes],
        scratch_shapes=[
            pltpu.VMEM((total, features), jnp.bfloat16),
            pltpu.VMEM((total, features), jnp.bfloat16),
            pltpu.VMEM((total, slots), jnp.float32),
        ],
        cost_estimate=pl.CostEstimate(
            flops=6 * total * units * features, bytes_accessed=4 * total * features, transcendentals=2 * total * units
        ),
        compiler_params=pltpu.CompilerParams(vmem_limit_bytes=28 << 20),
    )(place, weights, *projections, *inputs.values())
    results = dict(zip(outs, results))
    made.update({name[1:]: array for name, array in results.items() if name[0] == "made"})
    return {name[1:]: array for name, array in results.items() if name[0] == "out"}


def relay_kernel(place_ref, rows_ref, *refs):
    y, x = place_ref[0], place_ref[1]
    tokens, slots = refs[-1].shape[0], rows_ref.shape[2]
    step = tokens // 2
    token = lax.broadcasted_iota(jnp.int32, (step, slots), 0)
    for along_y in (True, False):
        first = 0 if along_y else SIDE
        pieces, outs = refs[first : first + SIDE], refs[first + 2 * SIDE : first + 3 * SIDE]
        lists = [rows_ref[wrap(y + d) * SIDE + x if along_y else y * SIDE + wrap(x + d)] for d in range(SIDE)]

        def work(i, carry, first=first, pieces=pieces, outs=outs, lists=lists):
            for t in range(SIDE):
                k = first + t
                chosen = jnp.concatenate(
                    [
                        jnp.where(token + i * step == rows[k : k + 1, :], 1.0, 0.0).astype(jnp.bfloat16)
                        for rows in lists
                    ],
                    1,
                )
                rows = jnp.concatenate([piece[t * slots : (t + 1) * slots, :] for piece in pieces])
                total = jnp.dot(chosen, rows, preferred_element_type=jnp.float32)
                outs[t][pl.ds(pl.multiple_of(i * step, step), step), :] = total.astype(jnp.bfloat16)
            return carry

        lax.fori_loop(0, 2, work, 0)


def relay(place, rows, lows, highs, tokens):
    total, half = lows[0].shape
    return pl.pallas_call(
        relay_kernel,
        in_specs=[SMEM] + [VMEM] * (1 + len(lows) + len(highs)),
        out_shape=[jax.ShapeDtypeStruct((tokens, half), jnp.bfloat16)] * (2 * SIDE),
        cost_estimate=pl.CostEstimate(
            flops=4 * SIDE * total * tokens * half, bytes_accessed=8 << 20, transcendentals=0
        ),
        compiler_params=pltpu.CompilerParams(vmem_limit_bytes=16 << 20),
        name="relay",
    )(place, rows, *lows, *highs)


def add_kernel(*refs):
    out_ref = refs[-1]
    half = refs[0].shape[1]
    for n, parts in enumerate((refs[:SIDE], refs[SIDE : 2 * SIDE])):
        total = parts[0][...].astype(jnp.float32)
        for part in parts[1:]:
            total = total + part[...].astype(jnp.float32)
        out_ref[:, n * half : (n + 1) * half] = total.astype(jnp.bfloat16)


def add(lows, highs):
    tokens, half = lows[0].shape
    step = tokens // 4
    return pl.pallas_call(
        add_kernel,
        grid=(4,),
        in_specs=[pl.BlockSpec((step, half), lambda i: (i, 0))] * (2 * SIDE),
        out_specs=pl.BlockSpec((step, 2 * half), lambda i: (i, 0)),
        out_shape=jax.ShapeDtypeStruct((tokens, 2 * half), jnp.bfloat16),
        cost_estimate=pl.CostEstimate(flops=4_000_000, bytes_accessed=5 << 20, transcendentals=0),
        compiler_params=pltpu.CompilerParams(vmem_limit_bytes=12 << 20),
        name="add",
    )(*lows, *highs)


def over_plane(array, by_y, by_x):
    places = [(y, x) for y in range(SIDE) for x in range(SIDE)]
    return lax.ppermute(
        array, "ep", [(y * SIDE + x, (y + by_y) % SIDE * SIDE + (x + by_x) % SIDE) for y, x in places]
    )


def along_z(array, by, tp_count):
    chips = tp_count // 2
    pairs = [(z, c, (z + (-by if c else by)) % chips) for z in range(chips) for c in range(2)]
    return lax.ppermute(array, "tp", [(z * 2 + c, to * 2 + c) for z, c, to in pairs])


def other_core(array, tp_count):
    return lax.ppermute(array, "tp", [(j, j ^ 1) for j in range(tp_count)])


def layer(stream, norm_gain, gate_rows, up_rows, down_rows, chosen, affinity):
    ep_count = lax.axis_size("ep")
    tp_count = lax.axis_size("tp")
    block, _ = stream.shape
    slots = 4 * block // ep_count
    ep_index = lax.axis_index("ep").astype(jnp.int32)
    place = jnp.stack([ep_index // SIDE, ep_index % SIDE])
    bounds = (jnp.arange(ep_count, dtype=jnp.int32) * tp_count + lax.axis_index("tp")) * block
    *low, high, own = prepare(stream, norm_gain, (gate_rows, up_rows, down_rows))
    left, right = [over_plane(part, 0, 1) for part in low], [over_plane(part, 0, -1) for part in low]
    down, up = over_plane(high, 1, 0), over_plane(high, -1, 0)
    both = stack([own, other_core(own, tp_count)])
    next1 = along_z(both, 1, tp_count)
    rows_there, weights = windows(bounds, chosen, affinity, block, slots)
    rows_here = lax.all_to_all(rows_there, "ep", split_axis=0, concat_axis=0, tiled=True)
    lows = [*low, *left, over_plane(left[0], 0, 1), over_plane(right[1], 0, -1), *right]
    mid = block // 2
    highs = [high, down, over_plane(down[:mid], 1, 0), over_plane(up[mid:], -1, 0), up]
    next2 = along_z(next1, 1, tp_count)
    picked_low = pick(True, place, rows_here, lows)
    arrived_low = [picked_low[0]] + [None] * (SIDE - 1)
    arrived_low[1], arrived_low[3] = over_plane(picked_low[1], 1, 0), over_plane(picked_low[3], 3, 0)
    arrived_low[2] = over_plane(picked_low[2], 2, 0)
    next3 = along_z(next2, 1, tp_count)
    picked_high = pick(False, place, rows_here, highs)
    arrived_high = [picked_high[0]] + [None] * (SIDE - 1)
    arrived_high[1], arrived_high[3] = over_plane(picked_high[1], 0, 1), over_plane(picked_high[3], 0, 3)
    arrived_high[2] = over_plane(picked_high[2], 0, 2)
    across = along_z(next2[:, : own.shape[1]], 2, tp_count)
    held = [next1, next2, next3, across]
    pieces = [both, *held, *(other_core(piece, tp_count) for piece in held)]
    projections = assemble(pieces)
    made, back = {}, {}
    for number in range(len(STEPS)):
        finished = expert(number, place, weights, projections, arrived_low, arrived_high, made)
        for (half, by), piece in finished.items():
            if by == 0:
                back[half, by] = piece
            elif half == "low":
                back[half, by] = over_plane(piece, -by, 0)
            else:
                back[half, by] = over_plane(piece, 0, -by)
    lows, highs = [back["low", d] for d in range(SIDE)], [back["high", d] for d in range(SIDE)]
    sums = relay(place, rows_here, lows, highs, block)
    lows, highs = [sums[0]], [sums[SIDE]]
    for t in (1, 3, 2):
        lows.append(over_plane(sums[t], 0, -t))
        highs.append(over_plane(sums[SIDE + t], -t, 0))
    return add(lows, highs)


def solution(mesh):
    return jax.shard_map(
        layer,
        mesh=mesh,
        in_specs=(
            P(("ep", "tp"), None),
            P(),
            P("ep", "tp", None),
            P("ep", "tp", None),
            P("ep", "tp", None),
            P("ep", None),
            P("ep", None),
        ),
        out_specs=P(("ep", "tp"), None),
        check_vma=False,
    )
```

```python
import functools

import jax
import jax.numpy as jnp
from jax import lax
from jax.experimental import pallas as pl
from jax.experimental.pallas import tpu as pltpu
from jax.sharding import PartitionSpec as P

epsilon = 1e-06
SIDE = 4
SMEM = pl.BlockSpec(memory_space=pltpu.SMEM)
VMEM = pl.BlockSpec(memory_space=pltpu.VMEM)


def wrap(value):
    return lax.rem(value + SIDE, SIDE)


def windows_kernel(block, slots, bounds_ref, list_ref, affinity_ref, rows_ref, weights_ref):
    listed = list_ref[...]
    lines = listed.shape[0]
    lane = lax.broadcasted_iota(jnp.int32, (1, slots), 1)

    def cut(j, carry):
        y, x = j // SIDE, lax.rem(j, SIDE)
        bound = bounds_ref[j]
        start = jnp.sum((listed < bound).astype(jnp.int32))
        line, shift = start // slots, start % slots
        first = jnp.minimum(line, lines - 1)
        second = jnp.minimum(line + 1, lines - 1)
        back = lax.rem(slots - shift, slots)

        def window(ref):
            low = pltpu.roll(ref[pl.ds(first, 1), :], back, 1)
            high = pltpu.roll(ref[pl.ds(second, 1), :], back, 1)
            return jnp.where(lane < slots - shift, low, high)

        rows = window(list_ref) - bound
        rows = jnp.where((rows >= 0) & (rows < block), rows, -1)
        for t in range(SIDE):
            rows_ref[y * SIDE + wrap(x + t - SIDE), t : t + 1, :] = rows
            rows_ref[wrap(y + t - SIDE) * SIDE + x, SIDE + t : SIDE + t + 1, :] = rows
        weights_ref[pl.ds(j, 1), :] = window(affinity_ref)
        return carry

    lax.fori_loop(0, weights_ref.shape[0], cut, 0, unroll=4)


def windows(bounds, listed, affinity, block, slots):
    count = bounds.shape[0]
    return pl.pallas_call(
        functools.partial(windows_kernel, block, slots),
        in_specs=[SMEM, VMEM, VMEM],
        out_shape=(
            jax.ShapeDtypeStruct((count, 2 * SIDE, slots), jnp.int32),
            jax.ShapeDtypeStruct((count, slots), jnp.float32),
        ),
        cost_estimate=pl.CostEstimate(flops=8_000_000, bytes_accessed=150_000, transcendentals=0),
        name="windows",
    )(bounds, listed.reshape(-1, slots), affinity.reshape(-1, slots))


def prepare_kernel(stream_ref, gain_ref, gate_ref, up_ref, down_ref, low_ref, high_ref, piece_ref):
    values = stream_ref[...].astype(jnp.float32)
    inverse = lax.rsqrt(jnp.mean(values * values, axis=-1, keepdims=True) + epsilon)
    normed = (values * inverse * gain_ref[...]).astype(jnp.bfloat16)
    half = low_ref.shape[1]
    low_ref[...] = normed[:, :half]
    high_ref[...] = normed[:, half:]

    @pl.when(pl.program_id(0) == 0)
    def _():
        piece_ref[0:1] = gate_ref[...]
        piece_ref[1:2] = up_ref[...]
        piece_ref[2:3] = down_ref[...]


def prepare(stream, norm_gain, parts):
    rows, features = stream.shape
    step, half = rows // 2, features // 2
    part = pl.BlockSpec(parts[0].shape, lambda i: (0, 0, 0))
    piece = (3, *parts[0].shape[1:])
    return pl.pallas_call(
        prepare_kernel,
        grid=(2,),
        in_specs=[
            pl.BlockSpec((step, features), lambda i: (i, 0)),
            pl.BlockSpec((1, features), lambda i: (0, 0)),
            part,
            part,
            part,
        ],
        out_specs=(
            pl.BlockSpec((step, half), lambda i: (i, 0)),
            pl.BlockSpec((step, half), lambda i: (i, 0)),
            pl.BlockSpec(piece, lambda i: (0, 0, 0)),
        ),
        out_shape=(
            jax.ShapeDtypeStruct((rows, half), jnp.bfloat16),
            jax.ShapeDtypeStruct((rows, half), jnp.bfloat16),
            jax.ShapeDtypeStruct(piece, jnp.bfloat16),
        ),
        cost_estimate=pl.CostEstimate(flops=3_000_000, bytes_accessed=3 << 20, transcendentals=512),
        name="prepare",
    )(stream, norm_gain.reshape(1, features), *parts)


def pick_kernel(along_y, place_ref, rows_ref, own_ref, after_ref, top_ref, bottom_ref, before_ref, *refs):
    outs = refs[:SIDE]
    across_ref, chosen_ref = refs[SIDE:]
    y, x = place_ref[0], place_ref[1]
    tokens, half = own_ref.shape
    slots = rows_ref.shape[2]
    across_ref[: tokens // 2, :] = top_ref[...]
    across_ref[tokens // 2 :, :] = bottom_ref[...]
    token = lax.broadcasted_iota(jnp.int32, (slots, tokens), 1).astype(jnp.float32)
    for d in range(SIDE):
        e = wrap(y + d) * SIDE + x if along_y else y * SIDE + wrap(x + d)
        column = rows_ref[e].astype(jnp.float32).T
        for t in range(SIDE):
            k = t if along_y else SIDE + t
            chosen_ref[t, d * slots : (d + 1) * slots, :] = jnp.where(column[:, k : k + 1] == token, 1.0, 0.0).astype(
                jnp.bfloat16
            )
    step = half // 2

    def work(i, carry):
        at = pl.ds(pl.multiple_of(i * step, step), step)
        for t, source in enumerate((own_ref, after_ref, across_ref, before_ref)):
            rows = jnp.dot(chosen_ref[t], source[:, at], preferred_element_type=jnp.float32).astype(jnp.bfloat16)
            for d in range(SIDE):
                outs[d][t * slots : (t + 1) * slots, at] = rows[d * slots : (d + 1) * slots, :]
        return carry

    lax.fori_loop(0, 2, work, 0)


def pick(along_y, place, rows, sources):
    tokens, half = sources[0].shape
    slots = rows.shape[2]
    return pl.pallas_call(
        functools.partial(pick_kernel, along_y),
        in_specs=[SMEM] + [VMEM] * 6,
        out_shape=[jax.ShapeDtypeStruct((SIDE * slots, half), jnp.bfloat16)] * SIDE,
        scratch_shapes=[
            pltpu.VMEM((tokens, half), jnp.bfloat16),
            pltpu.VMEM((SIDE, SIDE * slots, tokens), jnp.bfloat16),
        ],
        cost_estimate=pl.CostEstimate(
            flops=2 * SIDE * SIDE * slots * tokens * half, bytes_accessed=4 << 20, transcendentals=0
        ),
        compiler_params=pltpu.CompilerParams(vmem_limit_bytes=14 << 20),
        name="pick_y" if along_y else "pick_x",
    )(place, rows, *sources)


def stack_kernel(*refs):
    out_ref, at = refs[-1], 0
    for piece in refs[:-1]:
        width = piece.shape[1]
        out_ref[:, at : at + width, :] = piece[...]
        at += width


def stack(pieces):
    return pl.pallas_call(
        stack_kernel,
        in_specs=[VMEM] * len(pieces),
        out_shape=jax.ShapeDtypeStruct(
            (3, sum(piece.shape[1] for piece in pieces), pieces[0].shape[2]), jnp.bfloat16
        ),
        cost_estimate=pl.CostEstimate(flops=1_000_000, bytes_accessed=4 << 20, transcendentals=0),
        compiler_params=pltpu.CompilerParams(vmem_limit_bytes=8 << 20),
    )(*pieces)


def assemble_kernel(*refs):
    pieces, outs = refs[:-3], refs[-3:]
    step = 64
    at = 0
    for piece in pieces:
        width = piece.shape[1]
        for j, out in enumerate(outs):

            def move(i, carry, piece=piece, out=out, j=j, at=at):
                rows = pl.multiple_of(i * step, step)
                out[pl.ds(at + rows, step), :] = piece[j, pl.ds(rows, step), :]
                return carry

            lax.fori_loop(0, width // step, move, 0)
        at += width


def assemble(pieces):
    shape = jax.ShapeDtypeStruct((sum(piece.shape[1] for piece in pieces), pieces[0].shape[2]), jnp.bfloat16)
    return pl.pallas_call(
        assemble_kernel,
        in_specs=[VMEM] * len(pieces),
        out_shape=[shape] * 3,
        cost_estimate=pl.CostEstimate(flops=1_000_000, bytes_accessed=12 << 20, transcendentals=0),
        compiler_params=pltpu.CompilerParams(vmem_limit_bytes=16 << 20),
        name="assemble",
    )(*pieces)


STEPS = (
    ((0, 0), (1, 0), (2, 0), (3, 0)),
    ((2, 1), (2, 2), (2, 3), (0, 2), (1, 2), (3, 2)),
    ((0, 1), (1, 1), (3, 1), (0, 3), (1, 3), (3, 3)),
)
FINISHED = (
    (("high", 0),),
    (("low", 2), ("high", 2)),
    (("low", 1), ("high", 1), ("low", 3), ("high", 3), ("low", 0)),
)


def members(piece):
    half, fixed = piece
    return [(fixed, k) if half == "low" else (k, fixed) for k in range(SIDE)]


def expert_kernel(number, names, place_ref, weights_ref, gate_ref, up_ref, down_ref, *refs):
    inputs_ref, result_ref, columns_ref = refs[-3:]
    ref = dict(zip(names, refs))
    blocks = STEPS[number]
    y, x = place_ref[0], place_ref[1]
    slots, half = weights_ref.shape[1], ref["in", "low", blocks[0][0]].shape[1]
    for k, (a, b) in enumerate(blocks):
        at = slice(k * slots, (k + 1) * slots)
        inputs_ref[at, :half] = ref["in", "low", a][b * slots : (b + 1) * slots, :]
        inputs_ref[at, half:] = ref["in", "high", b][a * slots : (a + 1) * slots, :]
        line = weights_ref[pl.ds(wrap(y - a) * SIDE + wrap(x - b), 1), :]
        columns_ref[at, :] = jnp.broadcast_to(line, (slots, slots)).T
    last = (((1,), (1,)), ((), ()))
    units = gate_ref.shape[0]
    width, rows = units // 4, (4 if len(blocks) % 4 == 0 else number + 1) * slots

    def work(i, carry):
        at = pl.ds(pl.multiple_of(i * rows, rows), rows)
        inputs = inputs_ref[at, :]
        hidden = []
        for f in range(0, units, width):
            gate_sum = lax.dot_general(inputs, gate_ref[f : f + width, :], last, preferred_element_type=jnp.float32)
            up_sum = lax.dot_general(inputs, up_ref[f : f + width, :], last, preferred_element_type=jnp.float32)
            hidden.append((gate_sum / (1.0 + jnp.exp(-gate_sum)) * up_sum).astype(jnp.bfloat16))
        result = jnp.dot(jnp.concatenate(hidden, 1), down_ref[...], preferred_element_type=jnp.float32)
        result_ref[at, :] = (result * columns_ref[at, :][:, :1]).astype(jnp.bfloat16)
        return carry

    lax.fori_loop(0, len(blocks) * slots // rows, work, 0)

    def part(block, which):
        if block in blocks:
            k = blocks.index(block)
            cut = slice(0, half) if which == "low" else slice(half, 2 * half)
            return result_ref[k * slots : (k + 1) * slots, cut]
        step = next(n for n in range(number) if block in STEPS[n])
        k = STEPS[step].index(block)
        return ref["made", which, step][k * slots : (k + 1) * slots, :]

    for name in names:
        if name[0] == "out":
            for k, block in enumerate(members(name[1:])):
                ref[name][k * slots : (k + 1) * slots, :] = part(block, name[1])
        if name == ("made", name[1], number):
            for k, block in enumerate(blocks):
                ref[name][k * slots : (k + 1) * slots, :] = part(block, name[1])


def expert(number, place, weights, projections, low, high, made):
    slots, half = weights.shape[1], low[0].shape[1]
    features, units = 2 * half, projections[0].shape[0]
    piece_rows = SIDE * slots
    blocks = STEPS[number]
    total = len(blocks) * slots
    inputs = {("in", "low", a): low[a] for a, _ in blocks}
    inputs.update({("in", "high", b): high[b] for _, b in blocks})
    for piece in FINISHED[number]:
        for block in members(piece):
            step = next(n for n in range(len(STEPS)) if block in STEPS[n])
            if step < number:
                inputs["made", piece[0], step] = made[piece[0], step]
    outs = [("out", *piece) for piece in FINISHED[number]]
    for which in ("low", "high"):
        later = [
            piece
            for done in FINISHED[number + 1 :]
            for piece in done
            if piece[0] == which and any(block in blocks for block in members(piece))
        ]
        if later:
            outs.append(("made", which, number))
    shapes = [(piece_rows if name[0] == "out" else total, half) for name in outs]
    results = pl.pallas_call(
        functools.partial(expert_kernel, number, [*inputs, *outs]),
        in_specs=[SMEM] + [VMEM] * (4 + len(inputs)),
        out_shape=[jax.ShapeDtypeStruct(shape, jnp.bfloat16) for shape in shapes],
        scratch_shapes=[
            pltpu.VMEM((total, features), jnp.bfloat16),
            pltpu.VMEM((total, features), jnp.bfloat16),
            pltpu.VMEM((total, slots), jnp.float32),
        ],
        cost_estimate=pl.CostEstimate(
            flops=6 * total * units * features, bytes_accessed=4 * total * features, transcendentals=2 * total * units
        ),
        compiler_params=pltpu.CompilerParams(vmem_limit_bytes=28 << 20),
    )(place, weights, *projections, *inputs.values())
    results = dict(zip(outs, results))
    made.update({name[1:]: array for name, array in results.items() if name[0] == "made"})
    return {name[1:]: array for name, array in results.items() if name[0] == "out"}


def relay_kernel(place_ref, rows_ref, *refs):
    y, x = place_ref[0], place_ref[1]
    tokens, slots = refs[-1].shape[0], rows_ref.shape[2]
    step = tokens // 2
    token = lax.broadcasted_iota(jnp.int32, (step, slots), 0)
    for along_y in (True, False):
        first = 0 if along_y else SIDE
        pieces, outs = refs[first : first + SIDE], refs[first + 2 * SIDE : first + 3 * SIDE]
        lists = [rows_ref[wrap(y + d) * SIDE + x if along_y else y * SIDE + wrap(x + d)] for d in range(SIDE)]

        def work(i, carry, first=first, pieces=pieces, outs=outs, lists=lists):
            for t in range(SIDE):
                k = first + t
                chosen = jnp.concatenate(
                    [
                        jnp.where(token + i * step == rows[k : k + 1, :], 1.0, 0.0).astype(jnp.bfloat16)
                        for rows in lists
                    ],
                    1,
                )
                rows = jnp.concatenate([piece[t * slots : (t + 1) * slots, :] for piece in pieces])
                total = jnp.dot(chosen, rows, preferred_element_type=jnp.float32)
                outs[t][pl.ds(pl.multiple_of(i * step, step), step), :] = total.astype(jnp.bfloat16)
            return carry

        lax.fori_loop(0, 2, work, 0)


def relay(place, rows, lows, highs, tokens):
    total, half = lows[0].shape
    return pl.pallas_call(
        relay_kernel,
        in_specs=[SMEM] + [VMEM] * (1 + len(lows) + len(highs)),
        out_shape=[jax.ShapeDtypeStruct((tokens, half), jnp.bfloat16)] * (2 * SIDE),
        cost_estimate=pl.CostEstimate(
            flops=4 * SIDE * total * tokens * half, bytes_accessed=8 << 20, transcendentals=0
        ),
        compiler_params=pltpu.CompilerParams(vmem_limit_bytes=16 << 20),
        name="relay",
    )(place, rows, *lows, *highs)


def add_kernel(*refs):
    out_ref = refs[-1]
    half = refs[0].shape[1]
    for n, parts in enumerate((refs[:SIDE], refs[SIDE : 2 * SIDE])):
        total = parts[0][...].astype(jnp.float32)
        for part in parts[1:]:
            total = total + part[...].astype(jnp.float32)
        out_ref[:, n * half : (n + 1) * half] = total.astype(jnp.bfloat16)


def add(lows, highs):
    tokens, half = lows[0].shape
    step = tokens // 2
    return pl.pallas_call(
        add_kernel,
        grid=(2,),
        in_specs=[pl.BlockSpec((step, half), lambda i: (i, 0))] * (2 * SIDE),
        out_specs=pl.BlockSpec((step, 2 * half), lambda i: (i, 0)),
        out_shape=jax.ShapeDtypeStruct((tokens, 2 * half), jnp.bfloat16),
        cost_estimate=pl.CostEstimate(flops=4_000_000, bytes_accessed=5 << 20, transcendentals=0),
        compiler_params=pltpu.CompilerParams(vmem_limit_bytes=12 << 20),
        name="add",
    )(*lows, *highs)


def over_plane(array, by_y, by_x):
    places = [(y, x) for y in range(SIDE) for x in range(SIDE)]
    return lax.ppermute(
        array, "ep", [(y * SIDE + x, (y + by_y) % SIDE * SIDE + (x + by_x) % SIDE) for y, x in places]
    )


def along_z(array, by, tp_count):
    chips = tp_count // 2
    pairs = [(z, c, (z + (-by if c else by)) % chips) for z in range(chips) for c in range(2)]
    return lax.ppermute(array, "tp", [(z * 2 + c, to * 2 + c) for z, c, to in pairs])


def other_core(array, tp_count):
    return lax.ppermute(array, "tp", [(j, j ^ 1) for j in range(tp_count)])


def layer(stream, norm_gain, gate_rows, up_rows, down_rows, chosen, affinity):
    ep_count = lax.axis_size("ep")
    tp_count = lax.axis_size("tp")
    block, _ = stream.shape
    slots = 4 * block // ep_count
    ep_index = lax.axis_index("ep").astype(jnp.int32)
    place = jnp.stack([ep_index // SIDE, ep_index % SIDE])
    bounds = (jnp.arange(ep_count, dtype=jnp.int32) * tp_count + lax.axis_index("tp")) * block
    low, high, own = prepare(stream, norm_gain, (gate_rows, up_rows, down_rows))
    left, right = over_plane(low, 0, 1), over_plane(low, 0, -1)
    down, up = over_plane(high, 1, 0), over_plane(high, -1, 0)
    both = stack([own, other_core(own, tp_count)])
    next1 = along_z(both, 1, tp_count)
    rows_there, weights = windows(bounds, chosen, affinity, block, slots)
    rows_here = lax.all_to_all(rows_there, "ep", split_axis=0, concat_axis=0, tiled=True)
    mid = block // 2
    lows = [low, left, over_plane(left[:mid], 0, 1), over_plane(right[mid:], 0, -1), right]
    highs = [high, down, over_plane(down[:mid], 1, 0), over_plane(up[mid:], -1, 0), up]
    next2 = along_z(next1, 1, tp_count)
    picked_low = pick(True, place, rows_here, lows)
    arrived_low = [picked_low[0]] + [None] * (SIDE - 1)
    arrived_low[1], arrived_low[3] = over_plane(picked_low[1], 1, 0), over_plane(picked_low[3], 3, 0)
    arrived_low[2] = over_plane(picked_low[2], 2, 0)
    next3 = along_z(next2, 1, tp_count)
    picked_high = pick(False, place, rows_here, highs)
    arrived_high = [picked_high[0]] + [None] * (SIDE - 1)
    arrived_high[1], arrived_high[3] = over_plane(picked_high[1], 0, 1), over_plane(picked_high[3], 0, 3)
    arrived_high[2] = over_plane(picked_high[2], 0, 2)
    across = along_z(next2[:, : own.shape[1]], 2, tp_count)
    held = [next1, next2, next3, across]
    pieces = [both, *held, *(other_core(piece, tp_count) for piece in held)]
    projections = assemble(pieces)
    made, back = {}, {}
    for number in range(len(STEPS)):
        finished = expert(number, place, weights, projections, arrived_low, arrived_high, made)
        for (half, by), piece in finished.items():
            if by == 0:
                back[half, by] = piece
            elif half == "low":
                back[half, by] = over_plane(piece, -by, 0)
            else:
                back[half, by] = over_plane(piece, 0, -by)
    lows, highs = [back["low", d] for d in range(SIDE)], [back["high", d] for d in range(SIDE)]
    sums = relay(place, rows_here, lows, highs, block)
    lows, highs = [sums[0]], [sums[SIDE]]
    for t in (1, 3, 2):
        lows.append(over_plane(sums[t], 0, -t))
        highs.append(over_plane(sums[SIDE + t], -t, 0))
    return add(lows, highs)


def solution(mesh):
    return jax.shard_map(
        layer,
        mesh=mesh,
        in_specs=(
            P(("ep", "tp"), None),
            P(),
            P("ep", "tp", None),
            P("ep", "tp", None),
            P("ep", "tp", None),
            P("ep", None),
            P("ep", None),
        ),
        out_specs=P(("ep", "tp"), None),
        check_vma=False,
    )
```
